256 devices in a mesh: sp: 64 (over z, x, core), tp: 4 (over y).
Axes of the slice: x: 4, y: 4, z: 8, core: 2. Of those that a mesh axis runs over, the one named last changes fastest.
Arguments:
- tokens: bfloat16 [16384, 1024], P(('sp', 'tp')), may hold values from -6 to 6
- norm_gain: float32 [1024], replicated, may hold values from 0.1 to 1.9
- w_query: bfloat16 [1024, 1024], P('sp', 'tp'), may hold values from -0.1875 to 0.1875
- w_key: bfloat16 [1024, 1024], P('sp', 'tp'), may hold values from -0.1875 to 0.1875
- w_value: bfloat16 [1024, 1024], P('sp', 'tp'), may hold values from -0.1875 to 0.1875
- w_forget: bfloat16 [1024, 16], P('sp', 'tp'), may hold values from -0.375 to 0.375
- forget_offset: float32 [16], P('tp'), may hold values from 1 to 3.5
- w_out_t: bfloat16 [1024, 1024], P('sp', 'tp'), may hold values from -0.1875 to 0.1875
- out_gain: float32 [1024], replicated, may hold values from 0.1 to 1.9
Outputs:
- mixed: bfloat16 [16384, 1024], P(('sp', 'tp'))
The draws below stay inside these ranges and needn't reach their ends.
All inputs are finite; a program needn't handle non-finite values.
Results may differ from the reference program's by a relative error of at most 0.015.
Values may be sent and summed in bfloat16 or wider, within the bound.
A program may use at most 192 MiB of HBM per device.

```python
import jax
import jax.numpy as jnp
from jax import lax

D = 1024
HEADS = 16
HEAD_DIM = 64
TOK_DEV = 256
TOKENS = 16384
N_SP = 64


def block_scale(key, dims, split, smallest, top_value):
    def one(axis_at, blocks):
        draws = jax.random.uniform(jax.random.fold_in(jax.random.fold_in(key, 6), axis_at), (blocks,), jnp.float32, smallest / len(split), top_value / len(split))
        return jnp.repeat(jnp.exp(draws), dims[axis_at] // blocks).reshape((-1,) + (1,) * (len(dims) - axis_at - 1))

    loudness = one(*split[0])
    for cut in split[1:]:
        loudness = loudness * one(*cut)
    return loudness


def gaussian(rng, shape, spread, limit, shards=(), kind=jnp.bfloat16):
    drawn = jax.random.normal(rng, shape, jnp.float32) * spread
    if len(shards) > 0:
        drawn = block_scale(rng, shape, shards, -0.22, 0.18) * drawn
    return jnp.clip(drawn, min=-limit, max=limit).astype(kind)


def setup_inputs(seed: int = 0) -> dict:
    streams_of = jax.random.split(jax.random.key(seed), 10)
    tokens = gaussian(streams_of[0], (TOKENS, D), 1.0, 6.0, ((0, 256),))
    norm_gain = jnp.clip(1.0 + 0.18 * jax.random.normal(streams_of[1], (D,), jnp.float32), 0.1, 1.9)
    w_query = gaussian(streams_of[2], (D, HEADS * HEAD_DIM), D ** -0.5, 0.1875, ((0, 64), (1, 4)))
    w_key = gaussian(streams_of[3], (D, HEADS * HEAD_DIM), D ** -0.5, 0.1875, ((0, 64), (1, 4)))
    w_value = gaussian(streams_of[4], (D, HEADS * HEAD_DIM), D ** -0.5, 0.1875, ((0, 64), (1, 4)))
    w_forget = gaussian(streams_of[5], (D, HEADS), (D // 4) ** -0.5, 0.375, ((0, 64), (1, 4)))
    forget_offset = jnp.clip(1.0 + 2.5 * jax.random.uniform(streams_of[6], (HEADS,), jnp.float32) ** block_scale(streams_of[6], (HEADS,), ((0, 4),), -0.2, 0.2), 1.0, 3.5)
    w_out_t = gaussian(streams_of[7], (D, HEADS * HEAD_DIM), (HEADS * HEAD_DIM) ** -0.5, 0.1875, ((0, 64), (1, 4)))
    out_gain = jnp.clip(1.0 + 0.18 * jax.random.normal(streams_of[8], (D,), jnp.float32), 0.1, 1.9)
    return {"tokens": tokens, "norm_gain": norm_gain, "w_query": w_query, "w_key": w_key, "w_value": w_value, "w_forget": w_forget, "forget_offset": forget_offset, "w_out_t": w_out_t, "out_gain": out_gain}


norm_eps = 1e-06

def rms_norm(values_in, gain_row):
    floats = values_in.astype(jnp.float32)
    scale_row = lax.rsqrt(lax.optimization_barrier(jnp.mean(floats * floats, axis=-1, keepdims=True)) + norm_eps)
    return (floats * scale_row * gain_row).astype(jnp.bfloat16)

def reference(tokens, norm_gain, w_query, w_key, w_value, w_forget, forget_offset, w_out_t, out_gain):
    normed = rms_norm(tokens, norm_gain)
    queries = jnp.dot(normed, w_query, preferred_element_type=jnp.float32).astype(jnp.bfloat16)
    keys_all = jnp.dot(normed, w_key, preferred_element_type=jnp.float32).astype(jnp.bfloat16)
    values_all = jnp.dot(normed, w_value, preferred_element_type=jnp.float32).astype(jnp.bfloat16)
    logits = jnp.dot(normed, w_forget, preferred_element_type=jnp.float32) + forget_offset + jnp.log(jnp.float32(TOKENS))
    log_gates = jax.nn.log_sigmoid(logits)
    cumulative = jnp.cumsum(log_gates, axis=0)
    head_shape = (TOKENS, HEADS, HEAD_DIM)
    key_heads = keys_all.reshape(head_shape).astype(jnp.float32)
    value_heads = values_all.reshape(head_shape).astype(jnp.float32)
    query_blocks = queries.reshape(N_SP, TOK_DEV, HEADS, HEAD_DIM).astype(jnp.float32)
    cum_blocks = cumulative.reshape(N_SP, TOK_DEV, HEADS)
    key_pos = jnp.arange(TOKENS, dtype=jnp.int32)

    def attend(block_args):
        query_block, cum_block, block_index = block_args
        scores = jnp.einsum('qhd,khd->hqk', query_block, key_heads, precision=lax.Precision.HIGHEST) * HEAD_DIM ** (-0.5)
        scores = scores + cum_block.T[:, :, None] - cumulative.T[:, None, :]
        query_pos = block_index * TOK_DEV + jnp.arange(TOK_DEV, dtype=jnp.int32)
        allowed = key_pos[None, :] <= query_pos[:, None]
        scores = jnp.where(allowed[None], scores, -jnp.inf)
        attn_probs = jax.nn.softmax(scores, axis=-1)
        return jnp.einsum('hqk,khd->qhd', attn_probs, value_heads, precision=lax.Precision.HIGHEST)
    attended = lax.map(attend, (query_blocks, cum_blocks, jnp.arange(N_SP, dtype=jnp.int32)))
    attended = attended.reshape(TOKENS, HEADS * HEAD_DIM).astype(jnp.bfloat16)
    projected = lax.dot_general(attended, w_out_t, (((1,), (1,)), ((), ())), preferred_element_type=jnp.float32)
    return rms_norm(projected, out_gain)
```

```python
import functools

import jax
import jax.numpy as jnp
from jax import lax
from jax.experimental import pallas as pl
from jax.experimental.pallas import tpu as pltpu
from jax.sharding import PartitionSpec as P

HEAD_DIM = 64
LANES = 128
NORM_EPS = 1e-06
NX, NC = 4, 2
MESH = pl.DeviceIdType.MESH
F32 = jnp.float32
BF16 = jnp.bfloat16
CONTRACT_LAST = (((1,), (1,)), ((), ()))


def rms_norm(floats, gain_row):
    scale_col = lax.rsqrt(jnp.mean(floats * floats, axis=-1, keepdims=True) + NORM_EPS)
    return (floats * scale_col * gain_row).astype(BF16)


def layer_kernel(
    nz, n_tp,
    tokens_ref, gain_ref, wq_ref, wk_ref, wv_ref, wf_ref, offset_ref, wo_ref, out_gain_ref,
    out_ref,
    normed, w_all, wo_all, forget_all, gates_send, gates_all, bias_all,
    kv_send, kv_all, q_send, q_recv, q_rhs, scores, run_max, run_acc, att_send, att_recv,
    local_sem, tok_send, tok_recv, wx_send, wx_recv, wz_send, wz_recv, wd_send, wd_recv,
    fx_send, fx_recv, fz_send, fz_recv, fd_send, fd_recv,
    oz_send, oz_recv, ox_send, ox_recv, oy_send, oy_recv, od_send, od_recv,
    gx_send, gx_recv, gz_send, gz_recv, kx_send, kx_recv, qx_send, qx_recv,
    kz_send, kz_recv, kd_send, kd_recv, at_send, at_recv,
):
    sp, tp = lax.axis_index("sp"), lax.axis_index("tp")
    z = lax.div(sp, NX * NC)
    x = lax.rem(lax.div(sp, NC), NX)
    c = lax.rem(sp, NC)
    rows = tokens_ref.shape[0]
    block = rows * n_tp
    half = block // 2
    model = tokens_ref.shape[1]
    width = wq_ref.shape[1]
    heads = NX
    plane_blocks = NX * NC
    far = nz // 2

    def wrap(value, size):
        return lax.rem(value + size, size)

    def at(zz, xx, cc):
        return (zz * NX + xx) * NC + cc

    def remote(src, dst, send, recv, zz, xx, cc, yy):
        return pltpu.make_async_remote_copy(
            src_ref=src, dst_ref=dst, send_sem=send, recv_sem=recv,
            device_id=(at(zz, xx, cc), yy), device_id_type=MESH,
        )

    up, down = wrap(z + 1, nz), wrap(z - 1, nz)
    other = 1 - c

    local = [
        pltpu.make_async_copy(
            ref, w_all.at[z, x, c, :, pl.ds(i * width, width)], local_sem.at[i]
        )
        for i, ref in enumerate((wq_ref, wk_ref, wv_ref))
    ]
    local.append(pltpu.make_async_copy(wo_ref, wo_all.at[tp, z, x, c], local_sem.at[3]))
    for copy in local:
        copy.start()

    barrier = pltpu.get_barrier_semaphore()
    for k in range(1, NX * n_tp):
        pl.semaphore_signal(
            barrier, inc=1, device_id_type=MESH,
            device_id=(at(z, wrap(x + k // n_tp, NX), c), wrap(tp + k % n_tp, n_tp)),
        )
    for k in range(1, nz * NC):
        cc = c if k % NC == 0 else other
        pl.semaphore_signal(
            barrier, inc=1, device_id_type=MESH,
            device_id=(at(wrap(z + k // NC, nz), x, cc), tp),
        )

    forget_all[z, x, c] = jnp.concatenate(
        [wf_ref[...].astype(F32), jnp.zeros((8 - heads, wf_ref.shape[1]), F32)], axis=0
    )
    normed[tp] = rms_norm(tokens_ref[...].astype(F32), gain_ref[...])
    for copy in local:
        copy.wait()
    pl.semaphore_wait(barrier, NX * n_tp - 1 + nz * NC - 1)

    def x_copy(ref, send, recv, dx):
        return remote(
            ref.at[z, x, c], ref.at[z, x, c], send.at[dx - 1], recv.at[dx - 1],
            z, wrap(x + dx, NX), c, tp,
        )

    def ring_subs(way, step):
        if step < far:
            return (0, 1, 2, 3)
        return (0, 1) if way == 0 else (2, 3)

    def plane_at(way, step):
        return wrap(z - step, nz) if way == 0 else wrap(z + step, nz)

    def ring_hop(ref, send, recv, way, step, sub):
        place = ref.at[plane_at(way, step - 1), wrap(x + sub, NX), c]
        return remote(
            place, place, send.at[way, step - 1, sub], recv.at[way, step - 1, sub],
            (up, down)[way], x, c, tp,
        )

    def ring_wait(ref, send, recv, way, step, sub):
        place = ref.at[plane_at(way, step), wrap(x + sub, NX), c]
        remote(
            place, place, send.at[way, step - 1, sub], recv.at[way, step - 1, sub],
            (up, down)[way], x, c, tp,
        ).wait_recv()

    def twin(ref, send, recv, way, step, sub, core):
        place = ref.at[plane_at(way, step), wrap(x + sub, NX), core]
        return remote(
            place, place, send.at[way, step, sub], recv.at[way, step, sub], z, x, other, tp
        )

    def tok_copy(dy):
        return remote(
            normed.at[tp], normed.at[tp], tok_send.at[dy - 1], tok_recv.at[dy - 1],
            z, x, c, wrap(tp + dy, n_tp),
        )

    def wo_hop(way, step):
        place = wo_all.at[tp, plane_at(way, step - 1), x, c]
        return remote(
            place, place, oz_send.at[way, step - 1], oz_recv.at[way, step - 1],
            (up, down)[way], x, c, tp,
        )

    def wo_wait(way, step):
        place = wo_all.at[tp, plane_at(way, step), x, c]
        remote(
            place, place, oz_send.at[way, step - 1], oz_recv.at[way, step - 1],
            (up, down)[way], x, c, tp,
        ).wait_recv()

    def forget_hop(way, step):
        place = forget_all.at[plane_at(way, step - 1), :, c]
        return remote(
            place, place, fz_send.at[way, step - 1], fz_recv.at[way, step - 1],
            (up, down)[way], x, c, tp,
        )

    def forget_wait(way, step):
        place = forget_all.at[plane_at(way, step), :, c]
        remote(
            place, place, fz_send.at[way, step - 1], fz_recv.at[way, step - 1],
            (up, down)[way], x, c, tp,
        ).wait_recv()

    def forget_twin(way, step, core):
        place = forget_all.at[plane_at(way, step), :, core]
        return remote(
            place, place, fd_send.at[way, step], fd_recv.at[way, step], z, x, other, tp
        )

    for dx in range(1, NX):
        x_copy(w_all, wx_send, wx_recv, dx).start()
        x_copy(forget_all, fx_send, fx_recv, dx).start()
    for way in (0, 1):
        ring_hop(w_all, wz_send, wz_recv, way, 1, 0).start()
    for dy in range(1, n_tp):
        tok_copy(dy).start()
    twin(w_all, wd_send, wd_recv, 0, 0, 0, c).start()

    for sub in range(1, NX):
        dx = NX - sub
        place = w_all.at[z, wrap(x + sub, NX), c]
        remote(
            place, place, wx_send.at[dx - 1], wx_recv.at[dx - 1], z, x, c, tp
        ).wait_recv()
        for way in (0, 1):
            ring_hop(w_all, wz_send, wz_recv, way, 1, sub).start()
        twin(w_all, wd_send, wd_recv, 0, 0, sub, c).start()
        place = forget_all.at[z, wrap(x + sub, NX), c]
        remote(
            place, place, fx_send.at[dx - 1], fx_recv.at[dx - 1], z, x, c, tp
        ).wait_recv()
    for way in (0, 1):
        forget_hop(way, 1).start()
        wo_hop(way, 1).start()
    forget_twin(0, 0, c).start()

    both = (0, 1)
    for step in range(1, far + 1):
        for sub in range(NX):
            for way in both:
                if sub not in ring_subs(way, step):
                    continue
                ring_wait(w_all, wz_send, wz_recv, way, step, sub)
                if step < far and sub in ring_subs(way, step + 1):
                    ring_hop(w_all, wz_send, wz_recv, way, step + 1, sub).start()
                twin(w_all, wd_send, wd_recv, way, step, sub, c).start()
        for way in both if step < far else (0,):
            forget_wait(way, step)
            wo_wait(way, step)
            if step + 1 < far or (step + 1 == far and way == 0):
                forget_hop(way, step + 1).start()
                wo_hop(way, step + 1).start()
            forget_twin(way, step, c).start()

    def wo_x(dx):
        place = wo_all.at[tp, :, x, c]
        return remote(
            place, place, ox_send.at[dx - 1], ox_recv.at[dx - 1], z, wrap(x + dx, NX), c, tp
        )

    def wo_y(dy):
        place = wo_all.at[tp, :, :, c]
        return remote(
            place, place, oy_send.at[dy - 1], oy_recv.at[dy - 1], z, x, c, wrap(tp + dy, n_tp)
        )

    def wo_twin(dy, core):
        place = wo_all.at[wrap(tp + dy, n_tp), :, :, core]
        return remote(place, place, od_send.at[dy], od_recv.at[dy], z, x, other, tp)

    for dy in range(1, n_tp):
        place = normed.at[wrap(tp - dy, n_tp)]
        remote(
            place, place, tok_send.at[dy - 1], tok_recv.at[dy - 1], z, x, c, tp
        ).wait_recv()
    forget_twin(0, 0, other).wait_recv()
    for step in range(1, far + 1):
        for way in both if step < far else (0,):
            forget_twin(way, step, other).wait_recv()

    tokens_here = normed[...].reshape(block, model)
    forget_rows = jnp.concatenate(
        [
            forget_all[i // plane_blocks, (i // NC) % NX, i % NC]
            for i in range(nz * plane_blocks)
        ],
        axis=1,
    ).astype(BF16)
    logits = lax.dot_general(
        forget_rows, tokens_here, CONTRACT_LAST, preferred_element_type=F32
    )
    head_row = lax.broadcasted_iota(jnp.int32, (8, block), 0)
    offsets = jnp.zeros((8, block), F32)
    for h in range(heads):
        offsets = jnp.where(head_row == h, offset_ref[h], offsets)
    n_tokens = nz * plane_blocks * block
    logits = logits + offsets + jnp.log(jnp.full((8, block), n_tokens, F32))
    log_gates = jnp.minimum(logits, 0.0) - jnp.log1p(jnp.exp(-jnp.abs(logits)))
    row_at = lax.broadcasted_iota(jnp.int32, (block, block), 0)
    col_at = lax.broadcasted_iota(jnp.int32, (block, block), 1)
    cum_here = jnp.dot(
        log_gates, jnp.where(row_at <= col_at, 1.0, 0.0).astype(F32),
        precision=lax.Precision.HIGHEST, preferred_element_type=F32,
    )
    for h in range(heads):
        gates_send[h] = cum_here[h : h + 1, :]
    gates_all[z, x, c] = gates_send[x]

    def gate_x(dx):
        hx = wrap(x + dx, NX)
        return remote(
            gates_send.at[hx], gates_all.at[z, x, c], gx_send.at[dx - 1], gx_recv.at[dx - 1],
            z, hx, c, tp,
        )

    for dx in range(1, NX):
        gate_x(dx).start()

    for step in range(0, far + 1):
        for way in both:
            if step == 0 and way == 1:
                continue
            for sub in range(NX) if step == 0 else ring_subs(way, step):
                twin(w_all, wd_send, wd_recv, way, step, sub, other).wait_recv()
    for dx in range(1, NX):
        wo_x(dx).start()

    def project(i):
        weights = w_all[:, :, :, :, i * width : (i + 1) * width].reshape(model, width)
        return jnp.dot(tokens_here, weights, preferred_element_type=F32)

    lane_at = lax.broadcasted_iota(jnp.int32, (half, LANES), 1)
    keys = project(1)
    values_t = project(2).T.astype(BF16)
    for h in range(heads):
        tile = keys[:, (h // 2) * LANES : (h // 2 + 1) * LANES]
        first, second = tile[:half], tile[half:]
        if h % 2 == 0:
            second = pltpu.roll(second, HEAD_DIM, axis=1)
        else:
            first = pltpu.roll(first, HEAD_DIM, axis=1)
        kv_send[h, :half, :] = jnp.where(lane_at < HEAD_DIM, first, second).astype(BF16)
        value_rows = values_t[h * HEAD_DIM : (h + 1) * HEAD_DIM]
        kv_send[h, half : half + HEAD_DIM, :] = value_rows[:, :half]
        kv_send[h, half + HEAD_DIM :, :] = value_rows[:, half:]

    def kv_x(dx):
        hx = wrap(x + dx, NX)
        return remote(
            kv_send.at[hx], kv_all.at[z, x, c], kx_send.at[dx - 1], kx_recv.at[dx - 1],
            z, hx, c, tp,
        )

    for dx in range(1, NX):
        kv_x(dx).start()
    kv_all[z, x, c] = kv_send[x]
    for way in both:
        ring_hop(kv_all, kz_send, kz_recv, way, 1, 0).start()
    twin(kv_all, kd_send, kd_recv, 0, 0, 0, c).start()

    queries_t = (project(0).astype(BF16).astype(F32) * HEAD_DIM ** (-0.5)).T.astype(BF16)
    for h in range(heads):
        q_send[h] = queries_t[h * HEAD_DIM : (h + 1) * HEAD_DIM]

    def q_x(dx):
        hx = wrap(x + dx, NX)
        return remote(
            q_send.at[hx], q_recv.at[x], qx_send.at[dx - 1], qx_recv.at[dx - 1], z, hx, c, tp
        )

    for dx in range(1, NX):
        q_x(dx).start()
    q_recv[x] = q_send[x]

    for dx in range(1, NX):
        place = gates_all.at[z, wrap(x - dx, NX), c]
        remote(
            place, place, gx_send.at[dx - 1], gx_recv.at[dx - 1], z, x, c, tp
        ).wait_recv()

    def gate_z(k):
        cc = c if k % NC == 0 else other
        place = gates_all.at[z, :, c]
        return remote(
            place, place, gz_send.at[k - 1], gz_recv.at[k - 1],
            wrap(z + k // NC, nz), x, cc, tp,
        )

    for k in range(1, nz * NC):
        gate_z(k).start()

    for sub in range(1, NX):
        dx = NX - sub
        place = kv_all.at[z, wrap(x + sub, NX), c]
        remote(
            place, place, kx_send.at[dx - 1], kx_recv.at[dx - 1], z, x, c, tp
        ).wait_recv()
        for way in both:
            ring_hop(kv_all, kz_send, kz_recv, way, 1, sub).start()
        twin(kv_all, kd_send, kd_recv, 0, 0, sub, c).start()

    for dx in range(1, NX):
        place = q_recv.at[wrap(x - dx, NX)]
        remote(
            place, place, qx_send.at[dx - 1], qx_recv.at[dx - 1], z, x, c, tp
        ).wait_recv()

    ones_at = lax.broadcasted_iota(jnp.int32, (LANES, block), 0)
    no_rows = jnp.zeros((HEAD_DIM, block), BF16)
    for side in (0, 1):
        picks = ((ones_at // 8) % 2 == side) & (ones_at < 6 * 8)
        picks = jnp.where(picks, 1.0, 0.0).astype(BF16)
        for i in range(NX):
            parts = [q_recv[i], no_rows] if side == 0 else [no_rows, q_recv[i]]
            q_rhs[i, side] = jnp.concatenate(parts + [picks], axis=0)

    for k in range(1, nz * NC):
        cc = c if k % NC == 0 else other
        place = gates_all.at[wrap(z - k // NC, nz), :, cc]
        remote(
            place, place, gz_send.at[k - 1], gz_recv.at[k - 1], z, x, other, tp
        ).wait_recv()

    n_blocks = nz * plane_blocks
    gate_rows = gates_all[...].reshape(n_blocks, block)
    mine = z * plane_blocks
    row_block = lax.broadcasted_iota(jnp.int32, (n_blocks, n_blocks), 0)
    col_block = lax.broadcasted_iota(jnp.int32, (n_blocks, n_blocks), 1)
    behind = (col_block >= row_block) & (col_block < mine)
    ahead = (col_block < row_block) & (col_block >= mine)
    steps_between = jnp.where(ahead, 1.0, 0.0) - jnp.where(behind, 1.0, 0.0)
    starts = jnp.dot(
        steps_between, gate_rows[:, half:], precision=lax.Precision.HIGHEST,
        preferred_element_type=F32,
    )[:, half - 1 :]
    bias = -(starts + gate_rows)
    bias_high = bias.astype(BF16).astype(F32)
    bias_rest = bias - bias_high
    bias_mid = bias_rest.astype(BF16).astype(F32)
    bias_low = bias_rest - bias_mid
    no_bias = jnp.zeros((LANES - 6 * plane_blocks, LANES), F32)
    for zz in range(nz):
        here = slice(zz * plane_blocks, (zz + 1) * plane_blocks)
        stack = []
        for part in (bias_high, bias_mid, bias_low):
            stack += [part[here, :half], part[here, half:]]
        bias_all[zz] = jnp.concatenate(stack + [no_bias], axis=0).T.astype(BF16)

    lane_block = lax.broadcasted_iota(jnp.int32, (8, LANES), 1) % 8
    ones_rows = jnp.ones((16, plane_blocks * half), BF16)

    def attend(plane, own):
        key_rows = kv_all[plane, :, :, :half, :].reshape(plane_blocks * half, LANES)
        bias_cols = bias_all[plane]
        masks = [
            jnp.where(lane_block == b, 1.0, 0.0)[:1].astype(BF16) for b in range(plane_blocks)
        ]
        bias_tiles = jnp.concatenate([bias_cols * mask for mask in masks], axis=0)
        left = jnp.concatenate([key_rows, bias_tiles], axis=1)

        def score(i):
            tops = []
            for side in (0, 1):
                s = jnp.dot(left, q_rhs[i, side], preferred_element_type=F32)
                if own:
                    row = lax.broadcasted_iota(jnp.int32, s.shape, 0)
                    key_at = (row // half) * block + side * half + row % half
                    query_at = lax.broadcasted_iota(jnp.int32, s.shape, 1) + (
                        (i * NC + c) * block
                    )
                    s = jnp.where(key_at <= query_at, s, -1e30)
                scores[i, side] = s
                tops.append(jnp.max(s, axis=0, keepdims=True))
            return jnp.maximum(tops[0], tops[1])

        def absorb(i, top):
            if own:
                total = jnp.zeros((HEAD_DIM + 16, block), F32)
            else:
                old = run_max[i]
                top = jnp.maximum(old, top)
                total = run_acc[i] * jnp.exp(old - top)
            run_max[i] = top
            for side in (0, 1):
                weights = jnp.exp(scores[i, side] - top).astype(BF16)
                lo = half + side * HEAD_DIM
                value_cols = jnp.concatenate(
                    [
                        kv_all[plane, b // NC, b % NC, lo : lo + HEAD_DIM, :]
                        for b in range(plane_blocks)
                    ],
                    axis=1,
                )
                value_cols = jnp.concatenate([value_cols, ones_rows], axis=0)
                total = total + jnp.dot(value_cols, weights, preferred_element_type=F32)
            run_acc[i] = total

        tops = [score(0)]
        for i in range(NX):
            if i + 1 < NX:
                tops.append(score(i + 1))
            absorb(i, tops[i])

    for sub in range(NX):
        twin(kv_all, kd_send, kd_recv, 0, 0, sub, other).wait_recv()
    attend(z, True)

    for dx in range(1, NX):
        place = wo_all.at[tp, :, wrap(x - dx, NX), c]
        remote(
            place, place, ox_send.at[dx - 1], ox_recv.at[dx - 1], z, x, c, tp
        ).wait_recv()
    for dy in range(1, n_tp):
        wo_y(dy).start()
    wo_twin(0, c).start()

    def kv_step(step):
        last = step == far
        for sub in range(NX):
            for way in both:
                if sub not in ring_subs(way, step):
                    continue
                ring_wait(kv_all, kz_send, kz_recv, way, step, sub)
                if not last and sub in ring_subs(way, step + 1):
                    ring_hop(kv_all, kz_send, kz_recv, way, step + 1, sub).start()
                twin(kv_all, kd_send, kd_recv, way, step, sub, c).start()

    def maybe_attend(plane):
        @pl.when(plane < z)
        def _():
            attend(plane, False)

    for step in range(1, far + 1):
        kv_step(step)
        if step > 1:
            maybe_attend(plane_at(1, step - 1))
        for way in both:
            for sub in ring_subs(way, step):
                twin(kv_all, kd_send, kd_recv, way, step, sub, other).wait_recv()
        maybe_attend(plane_at(0, step))

    for dy in range(1, n_tp):
        place = wo_all.at[wrap(tp - dy, n_tp), :, :, c]
        remote(
            place, place, oy_send.at[dy - 1], oy_recv.at[dy - 1], z, x, c, tp
        ).wait_recv()
        wo_twin(n_tp - dy, c).start()

    my_head = tp * NX + x
    odd = lax.rem(x, 2)
    row_in = lax.broadcasted_iota(jnp.int32, (2 * HEAD_DIM, block), 0) // HEAD_DIM

    def att_copy(i, dy):
        yy = wrap(tp + dy, n_tp)
        return remote(
            att_send.at[i, pl.ds(pl.multiple_of(yy * rows, rows), rows), :],
            att_recv.at[my_head], at_send.at[i, dy], at_recv.at[my_head],
            z, i, c, yy,
        )

    for i in range(NX):
        acc = run_acc[i]
        att = acc[:HEAD_DIM] / acc[HEAD_DIM : HEAD_DIM + 1]
        att = jnp.where(row_in == odd, jnp.concatenate([att, att], axis=0), 0.0)
        att_send[i] = att.T.astype(BF16)
        for dy in range(n_tp):
            if dy == 0:

                @pl.when(x != i)
                def _():
                    att_copy(i, dy).start()
            else:
                att_copy(i, dy).start()
    att_recv[my_head] = att_send[x, pl.ds(pl.multiple_of(tp * rows, rows), rows), :]

    for dy in range(n_tp):
        wo_twin(dy, other).wait_recv()
    for k in range(1, NX * n_tp):
        source = wrap(my_head + k, NX * n_tp)
        place = att_recv.at[source]
        remote(place, place, at_send.at[0, 0], at_recv.at[source], z, x, c, tp).wait_recv()

    projected = jnp.zeros((rows, model), F32)
    for y in range(n_tp):
        pieces = []
        for pair in range(NX // 2):
            even = y * NX + 2 * pair
            pieces.append(att_recv[even] + att_recv[even + 1])
        columns = jnp.concatenate(pieces, axis=1)
        projected = projected + lax.dot_general(
            columns, wo_all[y].reshape(model, width), CONTRACT_LAST, preferred_element_type=F32
        )
    out_ref[...] = rms_norm(projected, out_gain_ref[...])

    for d in range(1, NX):
        x_copy(w_all, wx_send, wx_recv, d).wait_send()
        x_copy(forget_all, fx_send, fx_recv, d).wait_send()
        wo_x(d).wait_send()
        gate_x(d).wait_send()
        kv_x(d).wait_send()
        q_x(d).wait_send()
    for d in range(1, n_tp):
        tok_copy(d).wait_send()
        wo_y(d).wait_send()
    for d in range(n_tp):
        wo_twin(d, c).wait_send()
    for k in range(1, nz * NC):
        gate_z(k).wait_send()
    for step in range(0, far + 1):
        for way in both:
            if step == 0 and way == 1:
                continue
            for sub in range(NX) if step == 0 else ring_subs(way, step):
                twin(w_all, wd_send, wd_recv, way, step, sub, c).wait_send()
                twin(kv_all, kd_send, kd_recv, way, step, sub, c).wait_send()
                if step > 0:
                    ring_hop(w_all, wz_send, wz_recv, way, step, sub).wait_send()
                    ring_hop(kv_all, kz_send, kz_recv, way, step, sub).wait_send()
            if step < far or way == 0:
                forget_twin(way, step, c).wait_send()
                if step > 0:
                    forget_hop(way, step).wait_send()
                    wo_hop(way, step).wait_send()
    for i in range(NX):
        for dy in range(n_tp):
            if dy == 0:

                @pl.when(x != i)
                def _():
                    att_copy(i, dy).wait_send()
            else:
                att_copy(i, dy).wait_send()


def solution(mesh):
    n_sp, n_tp = mesh.shape["sp"], mesh.shape["tp"]
    nz = n_sp // (NX * NC)

    def on_device(
        tokens, norm_gain, w_query, w_key, w_value, w_forget, forget_offset, w_out_t, out_gain
    ):
        rows, model = tokens.shape
        w_rows, width = w_query.shape
        heads = w_forget.shape[1]
        block = rows * n_tp
        half = block // 2
        far = nz // 2
        vmem = pl.BlockSpec(memory_space=pltpu.VMEM)
        anywhere = pl.BlockSpec(memory_space=pl.ANY)
        dma = pltpu.SemaphoreType.DMA

        def pair(*shape):
            return [dma(shape), dma(shape)]

        return pl.pallas_call(
            functools.partial(layer_kernel, nz, n_tp),
            out_shape=jax.ShapeDtypeStruct((rows, model), BF16),
            in_specs=[
                vmem, vmem, anywhere, anywhere, anywhere, vmem,
                pl.BlockSpec(memory_space=pltpu.SMEM), anywhere, vmem,
            ],
            out_specs=vmem,
            scratch_shapes=[
                pltpu.VMEM((n_tp, rows, model), BF16),
                pltpu.VMEM((nz, NX, NC, w_rows, 3 * width), BF16),
                pltpu.VMEM((n_tp, nz, NX, NC, w_rows, width), BF16),
                pltpu.VMEM((nz, NX, NC, 8, w_rows), F32),
                pltpu.VMEM((heads, 1, block), F32),
                pltpu.VMEM((nz, NX, NC, 1, block), F32),
                pltpu.VMEM((nz, LANES, LANES), BF16),
                pltpu.VMEM((heads, block, LANES), BF16),
                pltpu.VMEM((nz, NX, NC, block, LANES), BF16),
                pltpu.VMEM((heads, HEAD_DIM, block), BF16),
                pltpu.VMEM((NX, HEAD_DIM, block), BF16),
                pltpu.VMEM((NX, 2, block, block), BF16),
                pltpu.VMEM((NX, 2, NX * NC * half, block), F32),
                pltpu.VMEM((NX, 1, block), F32),
                pltpu.VMEM((NX, HEAD_DIM + 16, block), F32),
                pltpu.VMEM((NX, block, LANES), BF16),
                pltpu.VMEM((NX * n_tp, rows, LANES), BF16),
                dma((4,)),
                *pair(n_tp - 1),
                *pair(NX - 1),
                *pair(2, far, NX),
                *pair(2, far + 1, NX),
                *pair(NX - 1),
                *pair(2, far),
                *pair(2, far + 1),
                *pair(2, far),
                *pair(NX - 1),
                *pair(n_tp - 1),
                *pair(n_tp),
                *pair(NX - 1),
                *pair(nz * NC - 1),
                *pair(NX - 1),
                *pair(NX - 1),
                *pair(2, far, NX),
                *pair(2, far + 1, NX),
                dma((NX, n_tp)),
                dma((NX * n_tp,)),
            ],
            compiler_params=pltpu.CompilerParams(collective_id=0, has_side_effects=True),
        )(
            tokens, norm_gain.reshape(1, model), w_query, w_key, w_value, w_forget.T,
            forget_offset, w_out_t, out_gain.reshape(1, model),
        )

    return jax.shard_map(
        on_device,
        mesh=mesh,
        in_specs=(
            P(("sp", "tp"), None),
            P(),
            P("sp", "tp"),
            P("sp", "tp"),
            P("sp", "tp"),
            P("sp", "tp"),
            P("tp"),
            P("sp", "tp"),
            P(),
        ),
        out_specs=P(("sp", "tp"), None),
        check_vma=False,
    )
```

```python
import functools

import jax
import jax.numpy as jnp
from jax import lax
from jax.experimental import pallas as pl
from jax.experimental.pallas import tpu as pltpu
from jax.sharding import PartitionSpec as P

HEAD_DIM = 64
LANES = 128
NORM_EPS = 1e-06
NX, NC = 4, 2
CHUNK, LAG = 4, 4
MESH = pl.DeviceIdType.MESH
F32 = jnp.float32
BF16 = jnp.bfloat16
CONTRACT_LAST = (((1,), (1,)), ((), ()))


def rms_norm(floats, gain_row):
    scale_col = lax.rsqrt(jnp.mean(floats * floats, axis=-1, keepdims=True) + NORM_EPS)
    return (floats * scale_col * gain_row).astype(BF16)


def layer_kernel(
    nz, n_tp,
    tokens_ref, gain_ref, wq_ref, wk_ref, wv_ref, wf_ref, offset_ref, wo_ref, out_gain_ref,
    out_ref,
    normed, w_kv, w_q, wo_all, forget_all, gates_send, gates_all, bias_all,
    kv_send, kv_all, q_send, q_recv, q_rhs, left, scores, run_max, run_acc, att_send, att_recv,
    local_sem, tok_send, tok_recv, wz_send, wz_recv, wx_send, wx_recv, wd_send, wd_recv,
    fz_send, fz_recv, fx_send, fx_recv, fd_send, fd_recv,
    oz_send, oz_recv, ox_send, ox_recv, oy_send, oy_recv, od_send, od_recv,
    gx_send, gx_recv, gz_send, gz_recv, kx_send, kx_recv, qx_send, qx_recv,
    kz_send, kz_recv, kd_send, kd_recv, at_send, at_recv,
):
    sp, tp = lax.axis_index("sp"), lax.axis_index("tp")
    z = lax.div(sp, NX * NC)
    x = lax.rem(lax.div(sp, NC), NX)
    c = lax.rem(sp, NC)
    rows = tokens_ref.shape[0]
    block = rows * n_tp
    half = block // 2
    model = tokens_ref.shape[1]
    width = wq_ref.shape[1]
    heads = NX
    plane_blocks = NX * NC
    far = nz // 2

    def wrap(value, size):
        return lax.rem(value + size, size)

    def at(zz, xx, cc):
        return (zz * NX + xx) * NC + cc

    def remote(src, dst, send, recv, zz, xx, cc, yy):
        return pltpu.make_async_remote_copy(
            src_ref=src, dst_ref=dst, send_sem=send, recv_sem=recv,
            device_id=(at(zz, xx, cc), yy), device_id_type=MESH,
        )

    up, down = wrap(z + 1, nz), wrap(z - 1, nz)
    other = 1 - c

    weights = (w_kv, w_q)
    local = [
        pltpu.make_async_copy(
            ref, place.at[z, x, c, :, pl.ds(i * width, width)], local_sem.at[n]
        )
        for n, (ref, place, i) in enumerate(
            ((wk_ref, w_kv, 0), (wv_ref, w_kv, 1), (wq_ref, w_q, 0))
        )
    ]
    local.append(pltpu.make_async_copy(wo_ref, wo_all.at[tp, z, x, c], local_sem.at[3]))
    for copy in local:
        copy.start()

    barrier = pltpu.get_barrier_semaphore()
    near = [(at(z, wrap(x + dx, NX), c), tp) for dx in range(1, NX)]
    near += [(sp, wrap(tp + dy, n_tp)) for dy in range(1, n_tp)]
    near += [(at(wrap(z + dz, nz), x, c), tp) for dz in range(1, nz)]
    near += [(at(z, x, other), tp)]
    for device in near:
        pl.semaphore_signal(barrier, inc=1, device_id_type=MESH, device_id=device)

    forget_all[z, x, c] = jnp.concatenate(
        [wf_ref[...].astype(F32), jnp.zeros((8 - heads, wf_ref.shape[1]), F32)], axis=0
    )
    normed[tp] = rms_norm(tokens_ref[...].astype(F32), gain_ref[...])
    for copy in local:
        copy.wait()
    pl.semaphore_wait(barrier, len(near))

    def w_place(a, k, dx, core):
        return weights[a].at[wrap(z - k, nz), wrap(x + dx, NX), core]

    def w_z(a, k):
        place = w_place(a, 0, 0, c)
        return remote(
            place, place, wz_send.at[a, k], wz_recv.at[a, k], wrap(z + k, nz), x, c, tp
        )

    def w_x(a, k, dx):
        place = w_place(a, k, 0, c)
        return remote(
            place, place, wx_send.at[a, k, dx], wx_recv.at[a, k, dx],
            z, wrap(x + dx, NX), c, tp,
        )

    def w_twin(a, k, dx, core):
        place = w_place(a, k, dx, core)
        return remote(
            place, place, wd_send.at[a, k, dx], wd_recv.at[a, k, dx], z, x, other, tp
        )

    def w_onward(a, k):
        for dx in (2, 1, 3):
            w_x(a, k, dx).start()
        w_twin(a, k, 0, c).start()

    def nearest(n):
        return jnp.where(lax.rem(n, 2) == 1, lax.div(n + 1, 2), nz - lax.div(n, 2))

    def w_from_z(a):
        w_onward(a, 0)

        @pl.loop(1, nz)
        def _(n):
            k = nearest(n)
            place = w_place(a, k, 0, c)
            remote(
                place, place, wz_send.at[a, k], wz_recv.at[a, k], up, x, c, tp
            ).wait_recv()
            w_onward(a, k)

    def w_from_x(a):
        @pl.loop(0, nz)
        def _(n):
            k = jnp.where(n == 0, 0, nearest(n))
            for dx in (1, 3, 2):
                place = w_place(a, k, NX - dx, c)
                remote(
                    place, place, wx_send.at[a, k, dx], wx_recv.at[a, k, dx],
                    z, wrap(x + 1, NX), c, tp,
                ).wait_recv()
                w_twin(a, k, NX - dx, c).start()

    def w_from_twin(a):
        @pl.loop(0, nz)
        def _(k):
            for dx in range(NX):
                w_twin(a, k, dx, other).wait_recv()

    def ring_subs(way, step):
        if step < far:
            return (0, 1, 2, 3)
        return (0, 1) if way == 0 else (2, 3)

    def plane_at(way, step):
        return wrap(z - step, nz) if way == 0 else wrap(z + step, nz)

    def ring_hop(ref, send, recv, way, step, sub):
        place = ref.at[plane_at(way, step - 1), wrap(x + sub, NX), c]
        return remote(
            place, place, send.at[way, step - 1, sub], recv.at[way, step - 1, sub],
            (up, down)[way], x, c, tp,
        )

    def ring_wait(ref, send, recv, way, step, sub):
        place = ref.at[plane_at(way, step), wrap(x + sub, NX), c]
        remote(
            place, place, send.at[way, step - 1, sub], recv.at[way, step - 1, sub],
            (up, down)[way], x, c, tp,
        ).wait_recv()

    def twin(ref, send, recv, way, step, sub, core):
        place = ref.at[plane_at(way, step), wrap(x + sub, NX), core]
        return remote(
            place, place, send.at[way, step, sub], recv.at[way, step, sub], z, x, other, tp
        )

    def tok_copy(dy):
        return remote(
            normed.at[tp], normed.at[tp], tok_send.at[dy - 1], tok_recv.at[dy - 1],
            z, x, c, wrap(tp + dy, n_tp),
        )

    def forget_z(k):
        place = forget_all.at[z, x, c]
        return remote(
            place, place, fz_send.at[k - 1], fz_recv.at[k - 1], wrap(z + k, nz), x, c, tp
        )

    def forget_x(dx):
        place = forget_all.at[:, x, c]
        return remote(
            place, place, fx_send.at[dx - 1], fx_recv.at[dx - 1], z, wrap(x + dx, NX), c, tp
        )

    def forget_twin(core):
        place = forget_all.at[:, :, core]
        return remote(place, place, fd_send.at[0], fd_recv.at[0], z, x, other, tp)

    def wo_z(k):
        place = wo_all.at[tp, z, x, c]
        return remote(
            place, place, oz_send.at[k - 1], oz_recv.at[k - 1], wrap(z + k, nz), x, c, tp
        )

    def wo_x(dx):
        place = wo_all.at[tp, :, x, c]
        return remote(
            place, place, ox_send.at[dx - 1], ox_recv.at[dx - 1], z, wrap(x + dx, NX), c, tp
        )

    def wo_y(dy):
        place = wo_all.at[tp, :, :, c]
        return remote(
            place, place, oy_send.at[dy - 1], oy_recv.at[dy - 1], z, x, c, wrap(tp + dy, n_tp)
        )

    def wo_twin(dy, core):
        place = wo_all.at[wrap(tp + dy, n_tp), :, :, core]
        return remote(place, place, od_send.at[dy], od_recv.at[dy], z, x, other, tp)

    both = (0, 1)
    far_first = sorted(range(1, nz), key=lambda k: -min(k, nz - k))
    for k in far_first:
        w_z(0, k).start()
    for dy in range(1, n_tp):
        tok_copy(dy).start()
    for k in far_first:
        forget_z(k).start()
    for k in far_first:
        w_z(1, k).start()
    for k in far_first:
        wo_z(k).start()

    w_from_z(0)
    for k in range(1, nz):
        place = forget_all.at[wrap(z - k, nz), x, c]
        remote(place, place, fz_send.at[k - 1], fz_recv.at[k - 1], up, x, c, tp).wait_recv()
    for dx in range(1, NX):
        forget_x(dx).start()
    w_from_z(1)
    w_from_x(0)
    for dx in range(1, NX):
        place = forget_all.at[:, wrap(x - dx, NX), c]
        remote(
            place, place, fx_send.at[dx - 1], fx_recv.at[dx - 1], z, x, c, tp
        ).wait_recv()
    forget_twin(c).start()
    for dy in range(1, n_tp):
        place = normed.at[wrap(tp - dy, n_tp)]
        remote(
            place, place, tok_send.at[dy - 1], tok_recv.at[dy - 1], z, x, c, tp
        ).wait_recv()
    tokens_here = normed[...].reshape(block, model)
    forget_twin(other).wait_recv()
    forget_rows = jnp.concatenate(
        [
            forget_all[i // plane_blocks, (i // NC) % NX, i % NC]
            for i in range(nz * plane_blocks)
        ],
        axis=1,
    ).astype(BF16)
    logits = lax.dot_general(
        forget_rows, tokens_here, CONTRACT_LAST, preferred_element_type=F32
    )
    head_row = lax.broadcasted_iota(jnp.int32, (8, block), 0)
    offsets = jnp.zeros((8, block), F32)
    for h in range(heads):
        offsets = jnp.where(head_row == h, offset_ref[h], offsets)
    n_tokens = nz * plane_blocks * block
    logits = logits + offsets + jnp.log(jnp.full((8, block), n_tokens, F32))
    log_gates = jnp.minimum(logits, 0.0) - jnp.log1p(jnp.exp(-jnp.abs(logits)))
    row_at = lax.broadcasted_iota(jnp.int32, (block, block), 0)
    col_at = lax.broadcasted_iota(jnp.int32, (block, block), 1)
    cum_here = jnp.dot(
        log_gates, jnp.where(row_at <= col_at, 1.0, 0.0).astype(F32),
        precision=lax.Precision.HIGHEST, preferred_element_type=F32,
    )
    for h in range(heads):
        gates_send[h] = cum_here[h : h + 1, :]
    gates_all[z, x, c] = gates_send[x]

    def gate_x(dx):
        hx = wrap(x + dx, NX)
        return remote(
            gates_send.at[hx], gates_all.at[z, x, c], gx_send.at[dx - 1], gx_recv.at[dx - 1],
            z, hx, c, tp,
        )

    for dx in range(1, NX):
        gate_x(dx).start()

    w_from_twin(0)

    def project(ref, i):
        columns = ref[:, :, :, :, i * width : (i + 1) * width].reshape(model, width)
        return jnp.dot(tokens_here, columns, preferred_element_type=F32)

    lane_at = lax.broadcasted_iota(jnp.int32, (half, LANES), 1)
    keys = project(w_kv, 0)
    values_t = project(w_kv, 1).T.astype(BF16)
    for h in range(heads):
        tile = keys[:, (h // 2) * LANES : (h // 2 + 1) * LANES]
        first, second = tile[:half], tile[half:]
        if h % 2 == 0:
            second = pltpu.roll(second, HEAD_DIM, axis=1)
        else:
            first = pltpu.roll(first, HEAD_DIM, axis=1)
        kv_send[h, :half, :] = jnp.where(lane_at < HEAD_DIM, first, second).astype(BF16)
        value_rows = values_t[h * HEAD_DIM : (h + 1) * HEAD_DIM]
        kv_send[h, half : half + HEAD_DIM, :] = value_rows[:, :half]
        kv_send[h, half + HEAD_DIM :, :] = value_rows[:, half:]

    def kv_x(dx):
        hx = wrap(x + dx, NX)
        return remote(
            kv_send.at[hx], kv_all.at[z, x, c], kx_send.at[dx - 1], kx_recv.at[dx - 1],
            z, hx, c, tp,
        )

    for dx in range(1, NX):
        kv_x(dx).start()
    kv_all[z, x, c] = kv_send[x]
    for way in both:
        ring_hop(kv_all, kz_send, kz_recv, way, 1, 0).start()
    twin(kv_all, kd_send, kd_recv, 0, 0, 0, c).start()

    for dx in range(1, NX):
        place = gates_all.at[z, wrap(x - dx, NX), c]
        remote(
            place, place, gx_send.at[dx - 1], gx_recv.at[dx - 1], z, x, c, tp
        ).wait_recv()

    def gate_z(k):
        cc = c if k % NC == 0 else other
        place = gates_all.at[z, :, c]
        return remote(
            place, place, gz_send.at[k - 1], gz_recv.at[k - 1],
            wrap(z + k // NC, nz), x, cc, tp,
        )

    for k in range(1, nz * NC):
        gate_z(k).start()

    w_from_x(1)
    w_from_twin(1)
    queries_t = (project(w_q, 0).astype(BF16).astype(F32) * HEAD_DIM ** (-0.5)).T.astype(BF16)
    for h in range(heads):
        q_send[h] = queries_t[h * HEAD_DIM : (h + 1) * HEAD_DIM]

    def q_x(dx):
        hx = wrap(x + dx, NX)
        return remote(
            q_send.at[hx], q_recv.at[x], qx_send.at[dx - 1], qx_recv.at[dx - 1], z, hx, c, tp
        )

    for dx in range(1, NX):
        q_x(dx).start()
    q_recv[x] = q_send[x]

    for sub in range(1, NX):
        dx = NX - sub
        place = kv_all.at[z, wrap(x + sub, NX), c]
        remote(
            place, place, kx_send.at[dx - 1], kx_recv.at[dx - 1], z, x, c, tp
        ).wait_recv()
        for way in both:
            ring_hop(kv_all, kz_send, kz_recv, way, 1, sub).start()
        twin(kv_all, kd_send, kd_recv, 0, 0, sub, c).start()

    for dx in range(1, NX):
        place = q_recv.at[wrap(x - dx, NX)]
        remote(
            place, place, qx_send.at[dx - 1], qx_recv.at[dx - 1], z, x, c, tp
        ).wait_recv()

    for k in range(1, nz):
        place = wo_all.at[tp, wrap(z - k, nz), x, c]
        remote(place, place, oz_send.at[k - 1], oz_recv.at[k - 1], up, x, c, tp).wait_recv()
    for dx in range(1, NX):
        wo_x(dx).start()
    ones_at = lax.broadcasted_iota(jnp.int32, (LANES, block), 0)
    no_rows = jnp.zeros((HEAD_DIM, block), BF16)
    for side in (0, 1):
        picks = ((ones_at // 8) % 2 == side) & (ones_at < 6 * 8)
        picks = jnp.where(picks, 1.0, 0.0).astype(BF16)
        for i in range(NX):
            parts = [q_recv[i], no_rows] if side == 0 else [no_rows, q_recv[i]]
            q_rhs[i, side] = jnp.concatenate(parts + [picks], axis=0)

    for k in range(1, nz * NC):
        cc = c if k % NC == 0 else other
        place = gates_all.at[wrap(z - k // NC, nz), :, cc]
        remote(
            place, place, gz_send.at[k - 1], gz_recv.at[k - 1], z, x, other, tp
        ).wait_recv()

    n_blocks = nz * plane_blocks
    gate_rows = gates_all[...].reshape(n_blocks, block)
    mine = z * plane_blocks
    row_block = lax.broadcasted_iota(jnp.int32, (n_blocks, n_blocks), 0)
    col_block = lax.broadcasted_iota(jnp.int32, (n_blocks, n_blocks), 1)
    behind = (col_block >= row_block) & (col_block < mine)
    ahead = (col_block < row_block) & (col_block >= mine)
    steps_between = jnp.where(ahead, 1.0, 0.0) - jnp.where(behind, 1.0, 0.0)
    starts = jnp.dot(
        steps_between, gate_rows[:, half:], precision=lax.Precision.HIGHEST,
        preferred_element_type=F32,
    )[:, half - 1 :]
    bias = -(starts + gate_rows)
    bias_high = bias.astype(BF16).astype(F32)
    bias_rest = bias - bias_high
    bias_mid = bias_rest.astype(BF16).astype(F32)
    bias_low = bias_rest - bias_mid
    no_bias = jnp.zeros((LANES - 6 * plane_blocks, LANES), F32)
    for zz in range(nz):
        here = slice(zz * plane_blocks, (zz + 1) * plane_blocks)
        stack = []
        for part in (bias_high, bias_mid, bias_low):
            stack += [part[here, :half], part[here, half:]]
        bias_all[zz] = jnp.concatenate(stack + [no_bias], axis=0).T.astype(BF16)

    lane_block = lax.broadcasted_iota(jnp.int32, (8, LANES), 1) % 8
    ones_rows = jnp.ones((16, CHUNK * half), BF16)

    def attend(plane, own):
        key_rows = kv_all[plane, :, :, :half, :].reshape(plane_blocks * half, LANES)
        bias_cols = bias_all[plane]
        masks = [
            jnp.where(lane_block == b, 1.0, 0.0)[:1].astype(BF16) for b in range(plane_blocks)
        ]
        bias_tiles = jnp.concatenate([bias_cols * mask for mask in masks], axis=0)
        left[...] = jnp.concatenate([key_rows, bias_tiles], axis=1)

        def score(i, side, b0):
            span = slice(b0 * half, (b0 + CHUNK) * half)
            s = jnp.dot(left[span, :], q_rhs[i, side], preferred_element_type=F32)
            if own:
                row = lax.broadcasted_iota(jnp.int32, s.shape, 0)
                key_at = (b0 + row // half) * block + side * half + row % half
                query_at = lax.broadcasted_iota(jnp.int32, s.shape, 1) + (
                    (i * NC + c) * block
                )
                s = jnp.where(key_at <= query_at, s, -1e30)
            scores[i, side, span, :] = s
            return jnp.max(s, axis=0, keepdims=True)

        def absorb(i, side, b0, top):
            if own and side == 0 and b0 == 0:
                total = jnp.zeros((HEAD_DIM + 16, block), F32)
            else:
                old = run_max[i]
                top = jnp.maximum(old, top)
                total = run_acc[i] * jnp.exp(old - top)
            run_max[i] = top
            span = slice(b0 * half, (b0 + CHUNK) * half)
            weights = jnp.exp(scores[i, side, span, :] - top).astype(BF16)
            lo = half + side * HEAD_DIM
            value_cols = jnp.concatenate(
                [
                    kv_all[plane, b // NC, b % NC, lo : lo + HEAD_DIM, :]
                    for b in range(b0, b0 + CHUNK)
                ],
                axis=1,
            )
            value_cols = jnp.concatenate([value_cols, ones_rows], axis=0)
            run_acc[i] = total + jnp.dot(value_cols, weights, preferred_element_type=F32)

        chunks = [
            (i, side, b0)
            for i in range(NX) for side in (0, 1) for b0 in range(0, plane_blocks, CHUNK)
        ]
        tops = []
        for n in range(len(chunks) + LAG):
            if n < len(chunks):
                tops.append(score(*chunks[n]))
            if n >= LAG:
                absorb(*chunks[n - LAG], tops[n - LAG])

    for sub in range(NX):
        twin(kv_all, kd_send, kd_recv, 0, 0, sub, other).wait_recv()
    attend(z, True)

    for dx in range(1, NX):
        place = wo_all.at[tp, :, wrap(x - dx, NX), c]
        remote(
            place, place, ox_send.at[dx - 1], ox_recv.at[dx - 1], z, x, c, tp
        ).wait_recv()
    for dy in range(1, n_tp):
        wo_y(dy).start()
    wo_twin(0, c).start()

    def kv_step(step):
        for sub in range(NX):
            for way in both:
                whole = (sub < NX // 2) == (way == 0)

                def receive():
                    ring_wait(kv_all, kz_send, kz_recv, way, step, sub)
                    twin(kv_all, kd_send, kd_recv, way, step, sub, c).start()

                    @pl.when(step + (0 if whole else 1) < far)
                    def _():
                        ring_hop(kv_all, kz_send, kz_recv, way, step + 1, sub).start()

                if whole:
                    receive()
                else:
                    pl.when(step < far)(receive)

    def twin_step(step):
        for sub in range(NX):
            for way in both:

                def receive():
                    twin(kv_all, kd_send, kd_recv, way, step, sub, other).wait_recv()

                if (sub < NX // 2) == (way == 0):
                    receive()
                else:
                    pl.when(step < far)(receive)

    def maybe_attend(plane, extra=True):
        @pl.when((plane < z) & extra)
        def _():
            attend(plane, False)

    @pl.loop(1, far + 1)
    def _(step):
        kv_step(step)

        @pl.when(step == far)
        def _():
            for dy in range(1, n_tp):
                place = wo_all.at[wrap(tp - dy, n_tp), :, :, c]
                remote(
                    place, place, oy_send.at[dy - 1], oy_recv.at[dy - 1], z, x, c, tp
                ).wait_recv()
                wo_twin(n_tp - dy, c).start()

        maybe_attend(plane_at(1, step - 1), step > 1)
        twin_step(step)
        maybe_attend(plane_at(0, step))

    my_head = tp * NX + x
    quarter = rows // 2
    low_lane = lax.broadcasted_iota(jnp.int32, (quarter, LANES), 1) < HEAD_DIM

    def att_copy(rel, dy):
        i, yy = wrap(x + rel, NX), wrap(tp + dy, n_tp)
        return remote(
            att_send.at[i, yy], att_recv.at[my_head], at_send.at[rel, dy],
            at_recv.at[my_head], z, i, c, yy,
        )

    for rel in (2, 1, 3, 0):
        i = wrap(x + rel, NX)
        acc = run_acc[i]
        att = acc[:HEAD_DIM] / acc[HEAD_DIM : HEAD_DIM + 1]
        att = jnp.concatenate([att, att], axis=0).T
        for y in range(n_tp):
            first = att[y * rows : y * rows + quarter]
            second = att[y * rows + quarter : (y + 1) * rows]
            att_send[i, y] = jnp.where(low_lane, first, second).astype(BF16)
        for dy in (2, 1, 3, 0):
            if rel or dy:
                att_copy(rel, dy).start()
    att_recv[my_head] = att_send[x, tp]

    for dy in range(n_tp):
        wo_twin(dy, other).wait_recv()
    for k in range(1, NX * n_tp):
        source = wrap(my_head + k, NX * n_tp)
        place = att_recv.at[source]
        remote(place, place, at_send.at[0, 0], at_recv.at[source], z, x, c, tp).wait_recv()

    projected = jnp.zeros((rows, model), F32)
    for y in range(n_tp):
        pieces = []
        for pair in range(NX // 2):
            even = att_recv[y * NX + 2 * pair].astype(F32)
            odd = att_recv[y * NX + 2 * pair + 1].astype(F32)
            first = jnp.where(low_lane, even, pltpu.roll(odd, HEAD_DIM, axis=1))
            second = jnp.where(low_lane, pltpu.roll(even, HEAD_DIM, axis=1), odd)
            pieces.append(jnp.concatenate([first, second], axis=0).astype(BF16))
        columns = jnp.concatenate(pieces, axis=1)
        projected = projected + lax.dot_general(
            columns, wo_all[y].reshape(model, width), CONTRACT_LAST, preferred_element_type=F32
        )
    out_ref[...] = rms_norm(projected, out_gain_ref[...])

    for d in range(1, NX):
        forget_x(d).wait_send()
        wo_x(d).wait_send()
        gate_x(d).wait_send()
        kv_x(d).wait_send()
        q_x(d).wait_send()
    for d in range(1, n_tp):
        tok_copy(d).wait_send()
        wo_y(d).wait_send()
    for d in range(n_tp):
        wo_twin(d, c).wait_send()
    forget_twin(c).wait_send()
    for k in range(1, nz):
        forget_z(k).wait_send()
        wo_z(k).wait_send()
    for a in (0, 1):
        @pl.loop(0, nz)
        def _(k):
            for dx in range(NX):
                if dx > 0:
                    w_x(a, k, dx).wait_send()
                w_twin(a, k, dx, c).wait_send()

        for k in range(1, nz):
            w_z(a, k).wait_send()
    for k in range(1, nz * NC):
        gate_z(k).wait_send()
    for step in range(0, far + 1):
        for way in both:
            if step == 0 and way == 1:
                continue
            for sub in range(NX) if step == 0 else ring_subs(way, step):
                twin(kv_all, kd_send, kd_recv, way, step, sub, c).wait_send()
                if step > 0:
                    ring_hop(kv_all, kz_send, kz_recv, way, step, sub).wait_send()
    for rel in range(NX):
        for dy in range(n_tp):
            if rel or dy:
                att_copy(rel, dy).wait_send()


def solution(mesh):
    n_sp, n_tp = mesh.shape["sp"], mesh.shape["tp"]
    nz = n_sp // (NX * NC)

    def on_device(
        tokens, norm_gain, w_query, w_key, w_value, w_forget, forget_offset, w_out_t, out_gain
    ):
        rows, model = tokens.shape
        w_rows, width = w_query.shape
        heads = w_forget.shape[1]
        block = rows * n_tp
        half = block // 2
        far = nz // 2
        vmem = pl.BlockSpec(memory_space=pltpu.VMEM)
        anywhere = pl.BlockSpec(memory_space=pl.ANY)
        dma = pltpu.SemaphoreType.DMA

        def pair(*shape):
            return [dma(shape), dma(shape)]

        return pl.pallas_call(
            functools.partial(layer_kernel, nz, n_tp),
            out_shape=jax.ShapeDtypeStruct((rows, model), BF16),
            in_specs=[
                vmem, vmem, anywhere, anywhere, anywhere, vmem,
                pl.BlockSpec(memory_space=pltpu.SMEM), anywhere, vmem,
            ],
            out_specs=vmem,
            scratch_shapes=[
                pltpu.VMEM((n_tp, rows, model), BF16),
                pltpu.VMEM((nz, NX, NC, w_rows, 2 * width), BF16),
                pltpu.VMEM((nz, NX, NC, w_rows, width), BF16),
                pltpu.VMEM((n_tp, nz, NX, NC, w_rows, width), BF16),
                pltpu.VMEM((nz, NX, NC, 8, w_rows), F32),
                pltpu.VMEM((heads, 1, block), F32),
                pltpu.VMEM((nz, NX, NC, 1, block), F32),
                pltpu.VMEM((nz, LANES, LANES), BF16),
                pltpu.VMEM((heads, block, LANES), BF16),
                pltpu.VMEM((nz, NX, NC, block, LANES), BF16),
                pltpu.VMEM((heads, HEAD_DIM, block), BF16),
                pltpu.VMEM((NX, HEAD_DIM, block), BF16),
                pltpu.VMEM((NX, 2, block, block), BF16),
                pltpu.VMEM((NX * NC * half, 2 * LANES), BF16),
                pltpu.VMEM((NX, 2, NX * NC * half, block), F32),
                pltpu.VMEM((NX, 1, block), F32),
                pltpu.VMEM((NX, HEAD_DIM + 16, block), F32),
                pltpu.VMEM((NX, n_tp, rows // 2, LANES), BF16),
                pltpu.VMEM((NX * n_tp, rows // 2, LANES), BF16),
                dma((4,)),
                *pair(n_tp - 1),
                *pair(2, nz),
                *pair(2, nz, NX),
                *pair(2, nz, NX),
                *pair(nz - 1),
                *pair(NX - 1),
                *pair(1),
                *pair(nz - 1),
                *pair(NX - 1),
                *pair(n_tp - 1),
                *pair(n_tp),
                *pair(NX - 1),
                *pair(nz * NC - 1),
                *pair(NX - 1),
                *pair(NX - 1),
                *pair(2, far, NX),
                *pair(2, far + 1, NX),
                dma((NX, n_tp)),
                dma((NX * n_tp,)),
            ],
            compiler_params=pltpu.CompilerParams(collective_id=0, has_side_effects=True),
        )(
            tokens, norm_gain.reshape(1, model), w_query, w_key, w_value, w_forget.T,
            forget_offset, w_out_t, out_gain.reshape(1, model),
        )

    return jax.shard_map(
        on_device,
        mesh=mesh,
        in_specs=(
            P(("sp", "tp"), None),
            P(),
            P("sp", "tp"),
            P("sp", "tp"),
            P("sp", "tp"),
            P("sp", "tp"),
            P("tp"),
            P("sp", "tp"),
            P(),
        ),
        out_specs=P(("sp", "tp"), None),
        check_vma=False,
    )
```

```python
import functools

import jax
import jax.numpy as jnp
from jax import lax
from jax.experimental import pallas as pl
from jax.experimental.pallas import tpu as pltpu
from jax.sharding import PartitionSpec as P

HEAD_DIM = 64
LANES = 128
NORM_EPS = 1e-06
NX, NC = 4, 2
CHUNK, LAG = 2, 8
MESH = pl.DeviceIdType.MESH
F32 = jnp.float32
BF16 = jnp.bfloat16
CONTRACT_LAST = (((1,), (1,)), ((), ()))


def rms_norm(floats, gain_row):
    scale_col = lax.rsqrt(jnp.mean(floats * floats, axis=-1, keepdims=True) + NORM_EPS)
    return (floats * scale_col * gain_row).astype(BF16)


def layer_kernel(
    nz, n_tp,
    tokens_ref, gain_ref, wq_ref, wk_ref, wv_ref, wf_ref, offset_ref, wo_ref, out_gain_ref,
    out_ref,
    normed, w_kv, w_q, wo_all, forget_all, gates_send, gates_all, bias_all,
    kv_send, kv_all, q_send, q_recv, q_rhs, key_side, scores, run_max, run_acc, att_send, att_recv,
    local_sem, tok_send, tok_recv, wz_send, wz_recv, wx_send, wx_recv, wd_send, wd_recv,
    fz_send, fz_recv, fx_send, fx_recv, fd_send, fd_recv,
    oz_send, oz_recv, ox_send, ox_recv, oy_send, oy_recv, od_send, od_recv,
    gx_send, gx_recv, gz_send, gz_recv, kx_send, kx_recv, qx_send, qx_recv,
    kz_send, kz_recv, kd_send, kd_recv, at_send, at_recv,
):
    sp, tp = lax.axis_index("sp"), lax.axis_index("tp")
    z = lax.div(sp, NX * NC)
    x = lax.rem(lax.div(sp, NC), NX)
    c = lax.rem(sp, NC)
    rows = tokens_ref.shape[0]
    block = rows * n_tp
    half = block // 2
    model = tokens_ref.shape[1]
    width = wq_ref.shape[1]
    heads = NX
    plane_blocks = NX * NC
    far = nz // 2

    def wrap(value, size):
        return lax.rem(value + size, size)

    def at(zz, xx, cc):
        return (zz * NX + xx) * NC + cc

    def remote(src, dst, send, recv, zz, xx, cc, yy):
        return pltpu.make_async_remote_copy(
            src_ref=src, dst_ref=dst, send_sem=send, recv_sem=recv,
            device_id=(at(zz, xx, cc), yy), device_id_type=MESH,
        )

    def landed(view, sem):
        remote(view, view, sem, sem, z, x, 1 - c, tp).wait_recv()

    def left(view, sem):
        remote(view, view, sem, sem, z, x, 1 - c, tp).wait_send()

    up, down = wrap(z + 1, nz), wrap(z - 1, nz)
    other = 1 - c

    weights = (w_kv, w_q)
    local = [
        pltpu.make_async_copy(
            ref, place.at[z, x, c, :, pl.ds(i * width, width)], local_sem.at[n]
        )
        for n, (ref, place, i) in enumerate(
            ((wk_ref, w_kv, 0), (wv_ref, w_kv, 1), (wq_ref, w_q, 0))
        )
    ]
    local.append(pltpu.make_async_copy(wo_ref, wo_all.at[tp, z, x, c], local_sem.at[3]))
    for copy in local:
        copy.start()

    barrier = pltpu.get_barrier_semaphore()
    near = [(at(z, wrap(x + dx, NX), c), tp) for dx in range(1, NX)]
    near += [(sp, wrap(tp + dy, n_tp)) for dy in range(1, n_tp)]
    near += [(at(wrap(z + dz, nz), x, c), tp) for dz in range(1, nz)]
    near += [(at(z, x, other), tp)]
    for device in near:
        pl.semaphore_signal(barrier, inc=1, device_id_type=MESH, device_id=device)

    forget_all[z, x, c] = jnp.concatenate(
        [wf_ref[...].astype(F32), jnp.zeros((8 - heads, wf_ref.shape[1]), F32)], axis=0
    )
    normed[tp] = rms_norm(tokens_ref[...].astype(F32), gain_ref[...])
    for copy in local:
        copy.wait()
    pl.semaphore_wait(barrier, len(near))

    def w_place(a, k, dx, core):
        return weights[a].at[wrap(z - k, nz), wrap(x + dx, NX), core]

    def w_z(a, k):
        place = w_place(a, 0, 0, c)
        return remote(
            place, place, wz_send.at[a], wz_recv.at[a, k], wrap(z + k, nz), x, c, tp
        )

    def w_x(a, k, dx):
        place = w_place(a, k, 0, c)
        return remote(
            place, place, wx_send.at[a], wx_recv.at[a, k],
            z, wrap(x + dx, NX), c, tp,
        )

    def w_twin(a, k):
        place = weights[a].at[wrap(z - k, nz), :, c]
        return remote(place, place, wd_send.at[a], wd_recv.at[a], z, x, other, tp)

    def w_onward(a, k):
        for dx in (2, 1, 3):
            w_x(a, k, dx).start()

    def nearest(n):
        return jnp.where(lax.rem(n, 2) == 1, lax.div(n + 1, 2), nz - lax.div(n, 2))

    def w_from_z(a, first, last):
        @pl.loop(first, last)
        def _(n):
            k = nearest(n)
            landed(w_place(a, k, 0, c), wz_recv.at[a, k])
            w_onward(a, k)

    def w_from_x(a):
        @pl.loop(0, nz)
        def _(n):
            k = jnp.where(n == 0, 0, nearest(n))
            landed(weights[a].at[0, pl.ds(0, NX - 1), c], wx_recv.at[a, k])
            w_twin(a, k).start()

    def w_from_twin(a):
        landed(weights[a].at[:, :, other], wd_recv.at[a])

    def ring_subs(way, step):
        if step < far:
            return (0, 1, 2, 3)
        return (0, 1) if way == 0 else (2, 3)

    def plane_at(way, step):
        return wrap(z - step, nz) if way == 0 else wrap(z + step, nz)

    def ring_hop(ref, send, recv, way, step, sub):
        place = ref.at[plane_at(way, step - 1), wrap(x + sub, NX), c]
        return remote(
            place, place, send.at[way], recv.at[way, step - 1, sub],
            (up, down)[way], x, c, tp,
        )

    def ring_wait(ref, send, recv, way, step, sub):
        landed(
            ref.at[plane_at(way, step), wrap(x + sub, NX), c], recv.at[way, step - 1, sub]
        )

    def twin(ref, send, recv, way, step, sub):
        place = ref.at[plane_at(way, step), wrap(x + sub, NX), c]
        return remote(place, place, send.at[0], recv.at[way, step], z, x, other, tp)

    def tok_copy(dy):
        return remote(
            normed.at[tp], normed.at[tp], tok_send.at[0], tok_recv.at[0],
            z, x, c, wrap(tp + dy, n_tp),
        )

    def forget_z(k):
        place = forget_all.at[z, x, c]
        return remote(
            place, place, fz_send.at[0], fz_recv.at[0], wrap(z + k, nz), x, c, tp
        )

    def forget_x(dx):
        place = forget_all.at[:, x, c]
        return remote(
            place, place, fx_send.at[0], fx_recv.at[0], z, wrap(x + dx, NX), c, tp
        )

    def forget_twin(core):
        place = forget_all.at[:, :, core]
        return remote(place, place, fd_send.at[0], fd_recv.at[0], z, x, other, tp)

    def wo_z(k):
        place = wo_all.at[tp, z, x, c]
        return remote(
            place, place, oz_send.at[0], oz_recv.at[0], wrap(z + k, nz), x, c, tp
        )

    def wo_x(dx):
        place = wo_all.at[tp, :, x, c]
        return remote(
            place, place, ox_send.at[0], ox_recv.at[0], z, wrap(x + dx, NX), c, tp
        )

    def wo_y(dy):
        place = wo_all.at[tp, :, :, c]
        return remote(
            place, place, oy_send.at[0], oy_recv.at[0], z, x, c, wrap(tp + dy, n_tp)
        )

    def wo_twin(dy):
        place = wo_all.at[wrap(tp + dy, n_tp), :, :, c]
        return remote(place, place, od_send.at[0], od_recv.at[0], z, x, other, tp)

    both = (0, 1)
    far_first = sorted(range(1, nz), key=lambda k: -min(k, nz - k))
    for k in far_first:
        forget_z(k).start()
    for k in far_first:
        w_z(0, k).start()
    for dy in range(1, n_tp):
        tok_copy(dy).start()
    for k in far_first:
        w_z(1, k).start()
    for k in far_first:
        wo_z(k).start()

    w_onward(0, 0)
    w_from_z(0, 1, 5)
    landed(forget_all.at[pl.ds(0, nz - 1), 0, 0], fz_recv.at[0])
    for dx in range(1, NX):
        forget_x(dx).start()
    w_from_z(0, 5, nz)
    w_onward(1, 0)
    w_from_z(1, 1, nz)
    w_from_x(0)
    landed(forget_all.at[:, pl.ds(0, NX - 1), 0], fx_recv.at[0])
    forget_twin(c).start()
    landed(normed.at[pl.ds(0, n_tp - 1)], tok_recv.at[0])
    tokens_here = normed[...].reshape(block, model)
    forget_twin(other).wait_recv()
    forget_rows = jnp.concatenate(
        [
            forget_all[i // plane_blocks, (i // NC) % NX, i % NC]
            for i in range(nz * plane_blocks)
        ],
        axis=1,
    ).astype(BF16)
    logits = lax.dot_general(
        forget_rows, tokens_here, CONTRACT_LAST, preferred_element_type=F32
    )
    head_row = lax.broadcasted_iota(jnp.int32, (8, block), 0)
    offsets = jnp.zeros((8, block), F32)
    for h in range(heads):
        offsets = jnp.where(head_row == h, offset_ref[h], offsets)
    n_tokens = nz * plane_blocks * block
    logits = logits + offsets + jnp.log(jnp.full((8, block), n_tokens, F32))
    log_gates = jnp.minimum(logits, 0.0) - jnp.log1p(jnp.exp(-jnp.abs(logits)))
    row_at = lax.broadcasted_iota(jnp.int32, (block, block), 0)
    col_at = lax.broadcasted_iota(jnp.int32, (block, block), 1)
    cum_here = jnp.dot(
        log_gates, jnp.where(row_at <= col_at, 1.0, 0.0).astype(F32),
        precision=lax.Precision.HIGHEST, preferred_element_type=F32,
    )
    for h in range(heads):
        gates_send[h] = cum_here[h : h + 1, :]
    gates_all[z, x, c] = gates_send[x]

    def gate_x(dx):
        hx = wrap(x + dx, NX)
        return remote(
            gates_send.at[hx], gates_all.at[z, x, c], gx_send.at[0], gx_recv.at[0],
            z, hx, c, tp,
        )

    for dx in range(1, NX):
        gate_x(dx).start()

    w_from_twin(0)

    def project(ref, i):
        columns = ref[:, :, :, :, i * width : (i + 1) * width].reshape(model, width)
        return jnp.dot(tokens_here, columns, preferred_element_type=F32)

    lane_at = lax.broadcasted_iota(jnp.int32, (half, LANES), 1)
    keys = project(w_kv, 0)
    values_t = project(w_kv, 1).T.astype(BF16)
    for h in range(heads):
        tile = keys[:, (h // 2) * LANES : (h // 2 + 1) * LANES]
        first, second = tile[:half], tile[half:]
        if h % 2 == 0:
            second = pltpu.roll(second, HEAD_DIM, axis=1)
        else:
            first = pltpu.roll(first, HEAD_DIM, axis=1)
        kv_send[h, :half, :] = jnp.where(lane_at < HEAD_DIM, first, second).astype(BF16)
        value_rows = values_t[h * HEAD_DIM : (h + 1) * HEAD_DIM]
        kv_send[h, half : half + HEAD_DIM, :] = value_rows[:, :half]
        kv_send[h, half + HEAD_DIM :, :] = value_rows[:, half:]

    def kv_x(dx):
        hx = wrap(x + dx, NX)
        return remote(
            kv_send.at[hx], kv_all.at[z, x, c], kx_send.at[0], kx_recv.at[dx - 1],
            z, hx, c, tp,
        )

    for dx in range(1, NX):
        kv_x(dx).start()
    kv_all[z, x, c] = kv_send[x]
    for way in both:
        ring_hop(kv_all, kz_send, kz_recv, way, 1, 0).start()
    twin(kv_all, kd_send, kd_recv, 0, 0, 0).start()

    landed(gates_all.at[0, pl.ds(0, NX - 1), 0], gx_recv.at[0])

    def gate_z(k):
        cc = c if k % NC == 0 else other
        place = gates_all.at[z, :, c]
        group = min(k - 1, 1)
        return remote(
            place, place, gz_send.at[group], gz_recv.at[group],
            wrap(z + k // NC, nz), x, cc, tp,
        )

    for k in range(1, nz * NC):
        gate_z(k).start()

    def first_sub(step):
        for way in both:
            if 0 not in ring_subs(way, step):
                continue
            ring_wait(kv_all, kz_send, kz_recv, way, step, 0)
            if step < far and 0 in ring_subs(way, step + 1):
                ring_hop(kv_all, kz_send, kz_recv, way, step + 1, 0).start()
            twin(kv_all, kd_send, kd_recv, way, step, 0).start()

    w_from_x(1)
    w_from_twin(1)
    first_sub(1)
    queries_t = (project(w_q, 0).astype(BF16).astype(F32) * HEAD_DIM ** (-0.5)).T.astype(BF16)
    for h in range(heads):
        q_send[h] = queries_t[h * HEAD_DIM : (h + 1) * HEAD_DIM]

    def q_x(dx):
        hx = wrap(x + dx, NX)
        return remote(
            q_send.at[hx], q_recv.at[x], qx_send.at[0], qx_recv.at[0], z, hx, c, tp
        )

    for dx in range(1, NX):
        q_x(dx).start()
    q_recv[x] = q_send[x]

    first_sub(2)
    for sub in (1, 3, 2):
        dx = NX - sub
        landed(kv_all.at[z, wrap(x + sub, NX), c], kx_recv.at[dx - 1])
        for way in both:
            ring_hop(kv_all, kz_send, kz_recv, way, 1, sub).start()
        twin(kv_all, kd_send, kd_recv, 0, 0, sub).start()

    landed(q_recv.at[pl.ds(0, NX - 1)], qx_recv.at[0])
    landed(wo_all.at[0, pl.ds(0, nz - 1), 0, 0], oz_recv.at[0])
    for dx in range(1, NX):
        wo_x(dx).start()
    ones_at = lax.broadcasted_iota(jnp.int32, (LANES, block), 0)
    no_rows = jnp.zeros((HEAD_DIM, block), BF16)
    for side in (0, 1):
        picks = ((ones_at // 8) % 2 == side) & (ones_at < 6 * 8)
        picks = jnp.where(picks, 1.0, 0.0).astype(BF16)
        for i in range(NX):
            parts = [q_recv[i], no_rows] if side == 0 else [no_rows, q_recv[i]]
            q_rhs[i, side] = jnp.concatenate(parts + [picks], axis=0)

    first_sub(3)
    landed(gates_all.at[0, :, 0], gz_recv.at[0])
    landed(gates_all.at[pl.ds(0, nz - 1), :, :], gz_recv.at[1])

    n_blocks = nz * plane_blocks
    gate_rows = gates_all[...].reshape(n_blocks, block)
    mine = z * plane_blocks
    row_block = lax.broadcasted_iota(jnp.int32, (n_blocks, n_blocks), 0)
    col_block = lax.broadcasted_iota(jnp.int32, (n_blocks, n_blocks), 1)
    behind = (col_block >= row_block) & (col_block < mine)
    ahead = (col_block < row_block) & (col_block >= mine)
    steps_between = jnp.where(ahead, 1.0, 0.0) - jnp.where(behind, 1.0, 0.0)
    starts = jnp.dot(
        steps_between, gate_rows[:, half:], precision=lax.Precision.HIGHEST,
        preferred_element_type=F32,
    )[:, half - 1 :]
    bias = -(starts + gate_rows)
    bias_high = bias.astype(BF16).astype(F32)
    bias_rest = bias - bias_high
    bias_mid = bias_rest.astype(BF16).astype(F32)
    bias_low = bias_rest - bias_mid
    no_bias = jnp.zeros((LANES - 6 * plane_blocks, LANES), F32)
    for zz in range(nz):
        here = slice(zz * plane_blocks, (zz + 1) * plane_blocks)
        stack = []
        for part in (bias_high, bias_mid, bias_low):
            stack += [part[here, :half], part[here, half:]]
        bias_all[zz] = jnp.concatenate(stack + [no_bias], axis=0).T.astype(BF16)

    lane_block = lax.broadcasted_iota(jnp.int32, (8, LANES), 1) % 8
    ones_rows = jnp.ones((16, CHUNK * half), BF16)

    def attend(plane, own):
        key_rows = kv_all[plane, :, :, :half, :].reshape(plane_blocks * half, LANES)
        bias_cols = bias_all[plane]
        masks = [
            jnp.where(lane_block == b, 1.0, 0.0)[:1].astype(BF16) for b in range(plane_blocks)
        ]
        bias_tiles = jnp.concatenate([bias_cols * mask for mask in masks], axis=0)
        key_side[...] = jnp.concatenate([key_rows, bias_tiles], axis=1)

        def score(i, side, b0):
            span = slice(b0 * half, (b0 + CHUNK) * half)
            s = jnp.dot(key_side[span, :], q_rhs[i, side], preferred_element_type=F32)
            if own:
                row = lax.broadcasted_iota(jnp.int32, s.shape, 0)
                key_at = (b0 + row // half) * block + side * half + row % half
                query_at = lax.broadcasted_iota(jnp.int32, s.shape, 1) + (
                    (i * NC + c) * block
                )
                s = jnp.where(key_at <= query_at, s, -1e30)
            scores[i, side, span, :] = s
            return jnp.max(s, axis=0, keepdims=True)

        def absorb(i, side, b0, top):
            if own and side == 0 and b0 == 0:
                total = jnp.zeros((HEAD_DIM + 16, block), F32)
            else:
                old = run_max[i]
                top = jnp.maximum(old, top)
                total = run_acc[i] * jnp.exp(old - top)
            run_max[i] = top
            span = slice(b0 * half, (b0 + CHUNK) * half)
            weights = jnp.exp(scores[i, side, span, :] - top).astype(BF16)
            lo = half + side * HEAD_DIM
            value_cols = jnp.concatenate(
                [
                    kv_all[plane, b // NC, b % NC, lo : lo + HEAD_DIM, :]
                    for b in range(b0, b0 + CHUNK)
                ],
                axis=1,
            )
            value_cols = jnp.concatenate([value_cols, ones_rows], axis=0)
            run_acc[i] = total + jnp.dot(value_cols, weights, preferred_element_type=F32)

        chunks = [
            (i, side, b0)
            for side in (0, 1) for b0 in range(0, plane_blocks, CHUNK) for i in range(NX)
        ]
        tops = []
        for n in range(len(chunks) + LAG):
            if n < len(chunks):
                tops.append(score(*chunks[n]))
            if n >= LAG:
                absorb(*chunks[n - LAG], tops[n - LAG])

    landed(kv_all.at[z, :, other], kd_recv.at[0, 0])
    attend(z, True)

    landed(wo_all.at[tp, :, pl.ds(0, NX - 1), c], ox_recv.at[0])
    for dy in range(1, n_tp):
        wo_y(dy).start()
    wo_twin(0).start()
    first_sub(4)

    def kv_step(step, subs):
        for sub in subs:
            for way in both:
                whole = (sub < NX // 2) == (way == 0)

                def receive():
                    ring_wait(kv_all, kz_send, kz_recv, way, step, sub)
                    twin(kv_all, kd_send, kd_recv, way, step, sub).start()

                    @pl.when(step + (0 if whole else 1) < far)
                    def _():
                        ring_hop(kv_all, kz_send, kz_recv, way, step + 1, sub).start()

                if whole:
                    receive()
                else:
                    pl.when(step < far)(receive)

    def twin_step(step):
        for way in both:

            @pl.when(step < far)
            def _():
                landed(kv_all.at[plane_at(way, step), :, other], kd_recv.at[way, step])

            @pl.when(step == far)
            def _():
                landed(
                    kv_all.at[plane_at(way, step), pl.ds(0, NX // 2), other],
                    kd_recv.at[way, step],
                )

    def maybe_attend(plane, extra=True):
        @pl.when((plane < z) & extra)
        def _():
            attend(plane, False)

    @pl.loop(1, far + 1)
    def _(step):
        kv_step(step, (1,))
        maybe_attend(plane_at(1, step - 1), step > 1)
        kv_step(step, (2, 3))

        @pl.when(step == far)
        def _():
            landed(wo_all.at[pl.ds(0, n_tp - 1), :, :, c], oy_recv.at[0])
            for dy in range(1, n_tp):
                wo_twin(dy).start()

        twin_step(step)
        maybe_attend(plane_at(0, step))

    my_head = tp * NX + x
    quarter = rows // 2
    low_lane = lax.broadcasted_iota(jnp.int32, (quarter, LANES), 1) < HEAD_DIM

    def att_copy(rel, dy):
        i, yy = wrap(x + rel, NX), wrap(tp + dy, n_tp)
        return remote(
            att_send.at[i, yy], att_recv.at[my_head], at_send.at[0],
            at_recv.at[0], z, i, c, yy,
        )

    for rel in (2, 1, 3, 0):
        i = wrap(x + rel, NX)
        acc = run_acc[i]
        att = acc[:HEAD_DIM] / acc[HEAD_DIM : HEAD_DIM + 1]
        att = jnp.concatenate([att, att], axis=0).T
        for y in range(n_tp):
            first = att[y * rows : y * rows + quarter]
            second = att[y * rows + quarter : (y + 1) * rows]
            att_send[i, y] = jnp.where(low_lane, first, second).astype(BF16)
        for dy in (2, 1, 3, 0):
            if rel or dy:
                att_copy(rel, dy).start()
    att_recv[my_head] = att_send[x, tp]

    landed(wo_all.at[:, :, :, other], od_recv.at[0])
    landed(att_recv.at[pl.ds(0, NX * n_tp - 1)], at_recv.at[0])

    projected = jnp.zeros((rows, model), F32)
    for y in range(n_tp):
        pieces = []
        for pair in range(NX // 2):
            even = att_recv[y * NX + 2 * pair].astype(F32)
            odd = att_recv[y * NX + 2 * pair + 1].astype(F32)
            first = jnp.where(low_lane, even, pltpu.roll(odd, HEAD_DIM, axis=1))
            second = jnp.where(low_lane, pltpu.roll(even, HEAD_DIM, axis=1), odd)
            pieces.append(jnp.concatenate([first, second], axis=0).astype(BF16))
        columns = jnp.concatenate(pieces, axis=1)
        projected = projected + lax.dot_general(
            columns, wo_all[y].reshape(model, width), CONTRACT_LAST, preferred_element_type=F32
        )
    out_ref[...] = rms_norm(projected, out_gain_ref[...])

    for a in (0, 1):
        left(weights[a].at[pl.ds(0, nz - 1), 0, 0], wz_send.at[a])
        left(weights[a].at[:, pl.ds(0, NX - 1), 0], wx_send.at[a])
        left(weights[a].at[:, :, c], wd_send.at[a])
    left(normed.at[pl.ds(0, n_tp - 1)], tok_send.at[0])
    left(forget_all.at[pl.ds(0, nz - 1), 0, 0], fz_send.at[0])
    left(forget_all.at[:, pl.ds(0, NX - 1), 0], fx_send.at[0])
    forget_twin(c).wait_send()
    left(wo_all.at[0, pl.ds(0, nz - 1), 0, 0], oz_send.at[0])
    left(wo_all.at[0, :, pl.ds(0, NX - 1), 0], ox_send.at[0])
    left(wo_all.at[pl.ds(0, n_tp - 1), :, :, 0], oy_send.at[0])
    left(wo_all.at[:, :, :, 0], od_send.at[0])
    left(gates_all.at[0, pl.ds(0, NX - 1), 0], gx_send.at[0])
    left(gates_all.at[0, :, 0], gz_send.at[0])
    left(gates_all.at[pl.ds(0, nz - 1), :, :], gz_send.at[1])
    left(kv_send.at[pl.ds(0, NX - 1)], kx_send.at[0])
    left(q_send.at[pl.ds(0, NX - 1)], qx_send.at[0])
    left(kv_all.at[:, :, 0], kd_send.at[0])
    for way in both:
        left(kv_all.at[pl.ds(0, nz - 1), pl.ds(0, NX // 2), 0], kz_send.at[way])
    left(att_recv.at[pl.ds(0, NX * n_tp - 1)], at_send.at[0])


def solution(mesh):
    n_sp, n_tp = mesh.shape["sp"], mesh.shape["tp"]
    nz = n_sp // (NX * NC)

    def on_device(
        tokens, norm_gain, w_query, w_key, w_value, w_forget, forget_offset, w_out_t, out_gain
    ):
        rows, model = tokens.shape
        w_rows, width = w_query.shape
        heads = w_forget.shape[1]
        block = rows * n_tp
        half = block // 2
        far = nz // 2
        vmem = pl.BlockSpec(memory_space=pltpu.VMEM)
        anywhere = pl.BlockSpec(memory_space=pl.ANY)
        dma = pltpu.SemaphoreType.DMA

        def pair(*shape):
            return [dma(shape), dma(shape)]

        return pl.pallas_call(
            functools.partial(layer_kernel, nz, n_tp),
            out_shape=jax.ShapeDtypeStruct((rows, model), BF16),
            in_specs=[
                vmem, vmem, anywhere, anywhere, anywhere, vmem,
                pl.BlockSpec(memory_space=pltpu.SMEM), anywhere, vmem,
            ],
            out_specs=vmem,
            scratch_shapes=[
                pltpu.VMEM((n_tp, rows, model), BF16),
                pltpu.VMEM((nz, NX, NC, w_rows, 2 * width), BF16),
                pltpu.VMEM((nz, NX, NC, w_rows, width), BF16),
                pltpu.VMEM((n_tp, nz, NX, NC, w_rows, width), BF16),
                pltpu.VMEM((nz, NX, NC, 8, w_rows), F32),
                pltpu.VMEM((heads, 1, block), F32),
                pltpu.VMEM((nz, NX, NC, 1, block), F32),
                pltpu.VMEM((nz, LANES, LANES), BF16),
                pltpu.VMEM((heads, block, LANES), BF16),
                pltpu.VMEM((nz, NX, NC, block, LANES), BF16),
                pltpu.VMEM((heads, HEAD_DIM, block), BF16),
                pltpu.VMEM((NX, HEAD_DIM, block), BF16),
                pltpu.VMEM((NX, 2, block, block), BF16),
                pltpu.VMEM((NX * NC * half, 2 * LANES), BF16),
                pltpu.VMEM((NX, 2, NX * NC * half, block), F32),
                pltpu.VMEM((NX, 1, block), F32),
                pltpu.VMEM((NX, HEAD_DIM + 16, block), F32),
                pltpu.VMEM((NX, n_tp, rows // 2, LANES), BF16),
                pltpu.VMEM((NX * n_tp, rows // 2, LANES), BF16),
                dma((4,)),
                *pair(1),
                dma((2,)), dma((2, nz)),
                dma((2,)), dma((2, nz)),
                *pair(2),
                *pair(1),
                *pair(1),
                *pair(1),
                *pair(1),
                *pair(1),
                *pair(1),
                *pair(1),
                *pair(1),
                *pair(2),
                dma((1,)), dma((NX - 1,)),
                *pair(1),
                dma((2,)), dma((2, far, NX)),
                dma((1,)), dma((2, far + 1)),
                *pair(1),
            ],
            compiler_params=pltpu.CompilerParams(collective_id=0, has_side_effects=True),
        )(
            tokens, norm_gain.reshape(1, model), w_query, w_key, w_value, w_forget.T,
            forget_offset, w_out_t, out_gain.reshape(1, model),
        )

    return jax.shard_map(
        on_device,
        mesh=mesh,
        in_specs=(
            P(("sp", "tp"), None),
            P(),
            P("sp", "tp"),
            P("sp", "tp"),
            P("sp", "tp"),
            P("sp", "tp"),
            P("tp"),
            P("sp", "tp"),
            P(),
        ),
        out_specs=P(("sp", "tp"), None),
        check_vma=False,
    )
```

```python
import functools

import jax
import jax.numpy as jnp
from jax import lax
from jax.experimental import pallas as pl
from jax.experimental.pallas import tpu as pltpu
from jax.sharding import PartitionSpec as P

HEAD_DIM = 64
LANES = 128
NORM_EPS = 1e-06
NX, NC = 4, 2
CHUNK, LAG = 2, 8
MESH = pl.DeviceIdType.MESH
F32 = jnp.float32
BF16 = jnp.bfloat16
CONTRACT_LAST = (((1,), (1,)), ((), ()))


def rms_norm(floats, gain_row):
    scale_col = lax.rsqrt(jnp.mean(floats * floats, axis=-1, keepdims=True) + NORM_EPS)
    return (floats * scale_col * gain_row).astype(BF16)


def layer_kernel(
    nz, n_tp,
    tokens_ref, gain_ref, wq_ref, wk_ref, wv_ref, wf_ref, offset_ref, wo_ref, out_gain_ref,
    out_ref,
    normed, w_kv, w_q, wo_all, forget_all, gates_send, gates_all, bias_all,
    kv_send, kv_all, q_send, q_recv, q_rhs, key_side, scores, run_max, run_acc, att_send, att_recv,
    local_sem, tok_send, tok_recv, wz_send, wz_recv, wx_send, wx_recv, wd_send, wd_recv,
    fz_send, fz_recv, fx_send, fx_recv, fd_send, fd_recv,
    oz_send, oz_recv, ox_send, ox_recv, oy_send, oy_recv, od_send, od_recv,
    gx_send, gx_recv, gz_send, gz_recv, kx_send, kx_recv, qx_send, qx_recv,
    kz_send, kz_recv, kd_send, kd_recv, at_send, at_recv,
):
    sp, tp = lax.axis_index("sp"), lax.axis_index("tp")
    z = lax.div(sp, NX * NC)
    x = lax.rem(lax.div(sp, NC), NX)
    c = lax.rem(sp, NC)
    rows = tokens_ref.shape[0]
    block = rows * n_tp
    half = block // 2
    model = tokens_ref.shape[1]
    width = wq_ref.shape[1]
    heads = NX
    plane_blocks = NX * NC
    far = nz // 2

    def wrap(value, size):
        return lax.rem(value + size, size)

    def at(zz, xx, cc):
        return (zz * NX + xx) * NC + cc

    def remote(src, dst, send, recv, zz, xx, cc, yy):
        return pltpu.make_async_remote_copy(
            src_ref=src, dst_ref=dst, send_sem=send, recv_sem=recv,
            device_id=(at(zz, xx, cc), yy), device_id_type=MESH,
        )

    def landed(view, sem):
        remote(view, view, sem, sem, z, x, 1 - c, tp).wait_recv()

    def left(view, sem):
        remote(view, view, sem, sem, z, x, 1 - c, tp).wait_send()

    up, down = wrap(z + 1, nz), wrap(z - 1, nz)
    other = 1 - c

    weights = (w_kv, w_q)
    local = [
        pltpu.make_async_copy(
            ref, place.at[z, x, c, :, pl.ds(i * width, width)], local_sem.at[n]
        )
        for n, (ref, place, i) in enumerate(
            ((wk_ref, w_kv, 0), (wv_ref, w_kv, 1), (wq_ref, w_q, 0))
        )
    ]
    local.append(pltpu.make_async_copy(wo_ref, wo_all.at[tp, z, x, c], local_sem.at[3]))
    for copy in local:
        copy.start()

    barrier = pltpu.get_barrier_semaphore()
    near = [(at(z, wrap(x + dx, NX), c), tp) for dx in range(1, NX)]
    near += [(sp, wrap(tp + dy, n_tp)) for dy in range(1, n_tp)]
    near += [(at(wrap(z + dz, nz), x, c), tp) for dz in range(1, nz)]
    near += [(at(z, x, other), tp)]
    for device in near:
        pl.semaphore_signal(barrier, inc=1, device_id_type=MESH, device_id=device)

    w_rows = wf_ref.shape[1]
    forget_all[z, x, c] = jnp.concatenate(
        [wf_ref[...].astype(F32), jnp.zeros((heads, LANES - w_rows), F32)], axis=1
    )
    normed[tp] = rms_norm(tokens_ref[...].astype(F32), gain_ref[...])
    for copy in local:
        copy.wait()
    pl.semaphore_wait(barrier, len(near))

    def w_place(a, k, dx, core):
        return weights[a].at[wrap(z - k, nz), wrap(x + dx, NX), core]

    def w_z(a, k):
        place = w_place(a, 0, 0, c)
        return remote(
            place, place, wz_send.at[a], wz_recv.at[a, k], wrap(z + k, nz), x, c, tp
        )

    def w_x(a, k, dx):
        place = w_place(a, k, 0, c)
        return remote(
            place, place, wx_send.at[a], wx_recv.at[a, k],
            z, wrap(x + dx, NX), c, tp,
        )

    def w_twin(a, k):
        place = weights[a].at[wrap(z - k, nz), :, c]
        return remote(place, place, wd_send.at[a], wd_recv.at[a], z, x, other, tp)

    def w_group_z(k):
        place = w_q.at[z, :, c]
        return remote(
            place, place, wz_send.at[1], wz_recv.at[1, k], wrap(z + k, nz), x, c, tp
        )

    def w_onward(a, k):
        for dx in (2, 1, 3):
            w_x(a, k, dx).start()

    def nearest(n):
        return jnp.where(lax.rem(n, 2) == 1, lax.div(n + 1, 2), nz - lax.div(n, 2))

    def w_from_z(a, first, last):
        @pl.loop(first, last)
        def _(n):
            k = nearest(n)
            landed(w_place(a, k, 0, c), wz_recv.at[a, k])
            w_onward(a, k)

    def w_from_x(first, last):
        @pl.loop(first, last)
        def _(n):
            k = jnp.where(n == 0, 0, nearest(n))
            landed(w_kv.at[0, pl.ds(0, NX - 1), c], wx_recv.at[0, k])
            w_twin(0, k).start()

    def w_from_twin(a):
        landed(weights[a].at[:, :, other], wd_recv.at[a])

    def ring_subs(way, step):
        if step < far:
            return (0, 1, 2, 3)
        return (0, 1) if way == 0 else (2, 3)

    def plane_at(way, step):
        return wrap(z - step, nz) if way == 0 else wrap(z + step, nz)

    def ring_hop(ref, send, recv, way, step, sub):
        place = ref.at[plane_at(way, step - 1), wrap(x + sub, NX), c]
        return remote(
            place, place, send.at[way], recv.at[way, step - 1, sub],
            (up, down)[way], x, c, tp,
        )

    def ring_wait(ref, send, recv, way, step, sub):
        landed(
            ref.at[plane_at(way, step), wrap(x + sub, NX), c], recv.at[way, step - 1, sub]
        )

    def twin(ref, send, recv, way, step, sub):
        place = ref.at[plane_at(way, step), wrap(x + sub, NX), c]
        return remote(place, place, send.at[0], recv.at[way, step], z, x, other, tp)

    def tok_copy(dy):
        return remote(
            normed.at[tp], normed.at[tp], tok_send.at[0], tok_recv.at[0],
            z, x, c, wrap(tp + dy, n_tp),
        )

    def forget_z(k):
        place = forget_all.at[z, x, c]
        return remote(
            place, place, fz_send.at[0], fz_recv.at[0], wrap(z + k, nz), x, c, tp
        )

    def forget_x(dx):
        place = forget_all.at[:, x, c]
        return remote(
            place, place, fx_send.at[0], fx_recv.at[0], z, wrap(x + dx, NX), c, tp
        )

    def forget_twin(core):
        place = forget_all.at[:, :, core]
        return remote(place, place, fd_send.at[0], fd_recv.at[0], z, x, other, tp)

    def wo_z(k):
        place = wo_all.at[tp, z, x, c]
        return remote(
            place, place, oz_send.at[0], oz_recv.at[0], wrap(z + k, nz), x, c, tp
        )

    def wo_x(dx):
        place = wo_all.at[tp, :, x, c]
        return remote(
            place, place, ox_send.at[0], ox_recv.at[0], z, wrap(x + dx, NX), c, tp
        )

    def wo_y(dy):
        place = wo_all.at[tp, :, :, c]
        return remote(
            place, place, oy_send.at[0], oy_recv.at[0], z, x, c, wrap(tp + dy, n_tp)
        )

    def wo_twin(dy):
        place = wo_all.at[wrap(tp + dy, n_tp), :, :, c]
        return remote(place, place, od_send.at[0], od_recv.at[0], z, x, other, tp)

    both = (0, 1)
    far_first = sorted(range(1, nz), key=lambda k: -min(k, nz - k))
    for k in far_first:
        forget_z(k).start()
    for k in far_first:
        w_z(0, k).start()
    for dx in (2, 1, 3):
        w_x(1, 0, dx).start()
    for dy in range(1, n_tp):
        tok_copy(dy).start()

    w_onward(0, 0)
    w_from_z(0, 1, 3)
    landed(w_q.at[0, pl.ds(0, NX - 1), c], wx_recv.at[1, 0])
    for k in far_first:
        w_group_z(k).start()
    for k in far_first:
        wo_z(k).start()
    w_twin(1, 0).start()
    w_from_z(0, 3, 5)
    landed(forget_all.at[pl.ds(0, nz - 1), 0, 0], fz_recv.at[0])
    for dx in range(1, NX):
        forget_x(dx).start()
    w_from_z(0, 5, nz)
    w_from_x(0, 5)
    landed(forget_all.at[:, pl.ds(0, NX - 1), 0], fx_recv.at[0])
    forget_twin(c).start()
    w_from_x(5, nz)
    landed(normed.at[pl.ds(0, n_tp - 1)], tok_recv.at[0])
    tokens_here = normed[...].reshape(block, model)
    forget_twin(other).wait_recv()
    forget_rows = jnp.concatenate(
        [
            forget_all[i // plane_blocks, (i // NC) % NX, i % NC][:, :w_rows]
            for i in range(nz * plane_blocks)
        ],
        axis=1,
    )
    forget_rows = jnp.concatenate(
        [forget_rows, jnp.zeros((8 - heads, model), F32)], axis=0
    ).astype(BF16)
    logits = lax.dot_general(
        forget_rows, tokens_here, CONTRACT_LAST, preferred_element_type=F32
    )
    head_row = lax.broadcasted_iota(jnp.int32, (8, block), 0)
    offsets = jnp.zeros((8, block), F32)
    for h in range(heads):
        offsets = jnp.where(head_row == h, offset_ref[h], offsets)
    n_tokens = nz * plane_blocks * block
    logits = logits + offsets + jnp.log(jnp.full((8, block), n_tokens, F32))
    log_gates = jnp.minimum(logits, 0.0) - jnp.log1p(jnp.exp(-jnp.abs(logits)))
    row_at = lax.broadcasted_iota(jnp.int32, (block, block), 0)
    col_at = lax.broadcasted_iota(jnp.int32, (block, block), 1)
    cum_here = jnp.dot(
        log_gates, jnp.where(row_at <= col_at, 1.0, 0.0).astype(F32),
        precision=lax.Precision.HIGHEST, preferred_element_type=F32,
    )
    for h in range(heads):
        gates_send[h] = cum_here[h : h + 1, :]
    gates_all[z, x, c] = gates_send[x]

    def gate_x(dx):
        hx = wrap(x + dx, NX)
        return remote(
            gates_send.at[hx], gates_all.at[z, x, c], gx_send.at[0], gx_recv.at[0],
            z, hx, c, tp,
        )

    for dx in range(1, NX):
        gate_x(dx).start()

    w_from_twin(0)

    def project(ref, i):
        columns = ref[:, :, :, :, i * width : (i + 1) * width].reshape(model, width)
        return jnp.dot(tokens_here, columns, preferred_element_type=F32)

    lane_at = lax.broadcasted_iota(jnp.int32, (half, LANES), 1)
    keys = project(w_kv, 0)
    values_t = project(w_kv, 1).T.astype(BF16)
    for h in range(heads):
        tile = keys[:, (h // 2) * LANES : (h // 2 + 1) * LANES]
        first, second = tile[:half], tile[half:]
        if h % 2 == 0:
            second = pltpu.roll(second, HEAD_DIM, axis=1)
        else:
            first = pltpu.roll(first, HEAD_DIM, axis=1)
        kv_send[h, :half, :] = jnp.where(lane_at < HEAD_DIM, first, second).astype(BF16)
        value_rows = values_t[h * HEAD_DIM : (h + 1) * HEAD_DIM]
        kv_send[h, half : half + HEAD_DIM, :] = value_rows[:, :half]
        kv_send[h, half + HEAD_DIM :, :] = value_rows[:, half:]

    def kv_x(dx):
        hx = wrap(x + dx, NX)
        return remote(
            kv_send.at[hx], kv_all.at[z, x, c], kx_send.at[0], kx_recv.at[dx - 1],
            z, hx, c, tp,
        )

    for dx in range(1, NX):
        kv_x(dx).start()
    kv_all[z, x, c] = kv_send[x]
    for way in both:
        ring_hop(kv_all, kz_send, kz_recv, way, 1, 0).start()
    twin(kv_all, kd_send, kd_recv, 0, 0, 0).start()

    def first_sub(step):
        for way in both:
            if 0 not in ring_subs(way, step):
                continue
            ring_wait(kv_all, kz_send, kz_recv, way, step, 0)
            if step < far and 0 in ring_subs(way, step + 1):
                ring_hop(kv_all, kz_send, kz_recv, way, step + 1, 0).start()
            twin(kv_all, kd_send, kd_recv, way, step, 0).start()

    @pl.loop(1, nz)
    def _(n):
        k = nearest(n)
        landed(w_q.at[0, :, c], wz_recv.at[1, k])
        w_twin(1, k).start()

    w_from_twin(1)
    queries_t = (project(w_q, 0).astype(BF16).astype(F32) * HEAD_DIM ** (-0.5)).T.astype(BF16)
    for h in range(heads):
        q_send[h] = queries_t[h * HEAD_DIM : (h + 1) * HEAD_DIM]

    def q_x(dx):
        hx = wrap(x + dx, NX)
        return remote(
            q_send.at[hx], q_recv.at[x], qx_send.at[0], qx_recv.at[0], z, hx, c, tp
        )

    for dx in range(1, NX):
        q_x(dx).start()
    q_recv[x] = q_send[x]

    landed(gates_all.at[0, pl.ds(0, NX - 1), 0], gx_recv.at[0])

    def gate_z(k):
        cc = c if k % NC == 0 else other
        place = gates_all.at[z, :, c]
        group = min(k - 1, 1)
        return remote(
            place, place, gz_send.at[group], gz_recv.at[group],
            wrap(z + k // NC, nz), x, cc, tp,
        )

    for k in range(1, nz * NC):
        gate_z(k).start()

    first_sub(1)
    for sub in (1, 3, 2):
        dx = NX - sub
        landed(kv_all.at[z, wrap(x + sub, NX), c], kx_recv.at[dx - 1])
        for way in both:
            ring_hop(kv_all, kz_send, kz_recv, way, 1, sub).start()
        twin(kv_all, kd_send, kd_recv, 0, 0, sub).start()

    landed(q_recv.at[pl.ds(0, NX - 1)], qx_recv.at[0])
    landed(wo_all.at[0, pl.ds(0, nz - 1), 0, 0], oz_recv.at[0])
    for dx in range(1, NX):
        wo_x(dx).start()
    ones_at = lax.broadcasted_iota(jnp.int32, (LANES, block), 0)
    no_rows = jnp.zeros((HEAD_DIM, block), BF16)
    for side in (0, 1):
        picks = ((ones_at // 8) % 2 == side) & (ones_at < 6 * 8)
        picks = jnp.where(picks, 1.0, 0.0).astype(BF16)
        for i in range(NX):
            parts = [q_recv[i], no_rows] if side == 0 else [no_rows, q_recv[i]]
            q_rhs[i, side] = jnp.concatenate(parts + [picks], axis=0)

    landed(gates_all.at[0, :, 0], gz_recv.at[0])
    landed(gates_all.at[pl.ds(0, nz - 1), :, :], gz_recv.at[1])

    n_blocks = nz * plane_blocks
    gate_rows = gates_all[...].reshape(n_blocks, block)
    mine = z * plane_blocks
    row_block = lax.broadcasted_iota(jnp.int32, (n_blocks, n_blocks), 0)
    col_block = lax.broadcasted_iota(jnp.int32, (n_blocks, n_blocks), 1)
    behind = (col_block >= row_block) & (col_block < mine)
    ahead = (col_block < row_block) & (col_block >= mine)
    steps_between = jnp.where(ahead, 1.0, 0.0) - jnp.where(behind, 1.0, 0.0)
    starts = jnp.dot(
        steps_between, gate_rows[:, half:], precision=lax.Precision.HIGHEST,
        preferred_element_type=F32,
    )[:, half - 1 :]
    bias = -(starts + gate_rows)
    bias_high = bias.astype(BF16).astype(F32)
    bias_rest = bias - bias_high
    bias_mid = bias_rest.astype(BF16).astype(F32)
    bias_low = bias_rest - bias_mid
    no_bias = jnp.zeros((LANES - 6 * plane_blocks, LANES), F32)
    for zz in range(nz):
        here = slice(zz * plane_blocks, (zz + 1) * plane_blocks)
        stack = []
        for part in (bias_high, bias_mid, bias_low):
            stack += [part[here, :half], part[here, half:]]
        bias_all[zz] = jnp.concatenate(stack + [no_bias], axis=0).T.astype(BF16)

    lane_block = lax.broadcasted_iota(jnp.int32, (8, LANES), 1) % 8
    ones_rows = jnp.ones((16, CHUNK * half), BF16)

    def attend(plane, own, core=None):
        if core is None:
            blocks = [(b // NC, b % NC) for b in range(plane_blocks)]
            key_rows = kv_all[plane, :, :, :half, :].reshape(plane_blocks * half, LANES)
        else:
            blocks = [(b, core) for b in range(NX)]
            key_rows = kv_all[plane, :, core, :half, :].reshape(NX * half, LANES)
        lag = LAG if core is None else LAG // 2
        bias_cols = bias_all[plane]
        masks = [
            jnp.where(lane_block == xx * NC + cc, 1.0, 0.0)[:1].astype(BF16)
            for xx, cc in blocks
        ]
        bias_tiles = jnp.concatenate([bias_cols * mask for mask in masks], axis=0)
        key_side[: len(blocks) * half, :] = jnp.concatenate([key_rows, bias_tiles], axis=1)

        def score(i, side, b0):
            span = slice(b0 * half, (b0 + CHUNK) * half)
            s = jnp.dot(key_side[span, :], q_rhs[i, side], preferred_element_type=F32)
            if own and b0 == i * NC:
                row = lax.broadcasted_iota(jnp.int32, s.shape, 0)
                key_at = (b0 + row // half) * block + side * half + row % half
                query_at = lax.broadcasted_iota(jnp.int32, s.shape, 1) + (
                    (i * NC + c) * block
                )
                s = jnp.where(key_at <= query_at, s, -1e30)
            scores[i, side, span, :] = s
            return jnp.max(s, axis=0, keepdims=True)

        def absorb(i, side, b0, top):
            if own and side == 0 and b0 == 0:
                total = jnp.zeros((HEAD_DIM + 16, block), F32)
            else:
                old = run_max[i]
                top = jnp.maximum(old, top)
                total = run_acc[i] * jnp.exp(old - top)
            run_max[i] = top
            span = slice(b0 * half, (b0 + CHUNK) * half)
            weights = jnp.exp(scores[i, side, span, :] - top).astype(BF16)
            lo = half + side * HEAD_DIM
            value_cols = jnp.concatenate(
                [
                    kv_all[plane, xx, cc, lo : lo + HEAD_DIM, :]
                    for xx, cc in blocks[b0 : b0 + CHUNK]
                ],
                axis=1,
            )
            value_cols = jnp.concatenate([value_cols, ones_rows], axis=0)
            run_acc[i] = total + jnp.dot(value_cols, weights, preferred_element_type=F32)

        chunks = [
            (i, side, b0)
            for side in (0, 1) for b0 in range(0, len(blocks), CHUNK) for i in range(NX)
            if not own or b0 <= i * NC
        ]
        tops = []
        for n in range(len(chunks) + lag):
            if n < len(chunks):
                tops.append(score(*chunks[n]))
            if n >= lag:
                absorb(*chunks[n - lag], tops[n - lag])

    landed(kv_all.at[z, :, other], kd_recv.at[0, 0])
    attend(z, True)
    first_sub(2)

    def wo_along_y():
        landed(wo_all.at[tp, :, pl.ds(0, NX - 1), c], ox_recv.at[0])
        for dy in range(1, n_tp):
            wo_y(dy).start()
        wo_twin(0).start()

    def kv_step(step, subs):
        for sub in subs:
            for way in both:
                whole = (sub < NX // 2) == (way == 0)

                def receive():
                    ring_wait(kv_all, kz_send, kz_recv, way, step, sub)
                    twin(kv_all, kd_send, kd_recv, way, step, sub).start()

                    @pl.when(step + (0 if whole else 1) < far)
                    def _():
                        ring_hop(kv_all, kz_send, kz_recv, way, step + 1, sub).start()

                if whole:
                    receive()
                else:
                    pl.when(step < far)(receive)

    def twin_step(step):
        for way in both:

            @pl.when(step < far)
            def _():
                landed(kv_all.at[plane_at(way, step), :, other], kd_recv.at[way, step])

            @pl.when(step == far)
            def _():
                landed(
                    kv_all.at[plane_at(way, step), pl.ds(0, NX // 2), other],
                    kd_recv.at[way, step],
                )

    def maybe_attend(plane, extra, core=None):
        @pl.when((plane < z) & extra)
        def _():
            attend(plane, False, core)

    @pl.loop(1, far + 1)
    def _(step):
        kv_step(step, (1,))
        pl.when(step == 1)(wo_along_y)
        pl.when(step == 2)(lambda: first_sub(3))
        pl.when(step == 3)(lambda: first_sub(4))
        maybe_attend(plane_at(1, step - 1), step > 1)
        kv_step(step, (2, 3))

        @pl.when(step == far)
        def _():
            landed(wo_all.at[pl.ds(0, n_tp - 1), :, :, c], oy_recv.at[0])
            for dy in range(1, n_tp):
                wo_twin(dy).start()

        @pl.loop(0, NC)
        def _(part):
            pl.when(part == 1)(lambda: twin_step(step))
            maybe_attend(plane_at(0, step), True, lax.rem(c + part, NC))


    my_head = tp * NX + x
    quarter = rows // 2
    low_lane = lax.broadcasted_iota(jnp.int32, (quarter, LANES), 1) < HEAD_DIM

    def att_copy(rel, dy):
        i, yy = wrap(x + rel, NX), wrap(tp + dy, n_tp)
        return remote(
            att_send.at[i, yy], att_recv.at[my_head], at_send.at[0],
            at_recv.at[0], z, i, c, yy,
        )

    for rel in (2, 1, 3, 0):
        i = wrap(x + rel, NX)
        acc = run_acc[i]
        att = acc[:HEAD_DIM] / acc[HEAD_DIM : HEAD_DIM + 1]
        att = jnp.concatenate([att, att], axis=0).T
        for y in range(n_tp):
            first = att[y * rows : y * rows + quarter]
            second = att[y * rows + quarter : (y + 1) * rows]
            att_send[i, y] = jnp.where(low_lane, first, second).astype(BF16)
        for dy in (2, 1, 3, 0):
            if rel or dy:
                att_copy(rel, dy).start()
    att_recv[my_head] = att_send[x, tp]

    landed(wo_all.at[:, :, :, other], od_recv.at[0])
    landed(att_recv.at[pl.ds(0, NX * n_tp - 1)], at_recv.at[0])

    projected = jnp.zeros((rows, model), F32)
    for y in range(n_tp):
        pieces = []
        for pair in range(NX // 2):
            even = att_recv[y * NX + 2 * pair].astype(F32)
            odd = att_recv[y * NX + 2 * pair + 1].astype(F32)
            first = jnp.where(low_lane, even, pltpu.roll(odd, HEAD_DIM, axis=1))
            second = jnp.where(low_lane, pltpu.roll(even, HEAD_DIM, axis=1), odd)
            pieces.append(jnp.concatenate([first, second], axis=0).astype(BF16))
        columns = jnp.concatenate(pieces, axis=1)
        projected = projected + lax.dot_general(
            columns, wo_all[y].reshape(model, width), CONTRACT_LAST, preferred_element_type=F32
        )
    out_ref[...] = rms_norm(projected, out_gain_ref[...])

    left(w_kv.at[pl.ds(0, nz - 1), 0, 0], wz_send.at[0])
    left(w_kv.at[:, pl.ds(0, NX - 1), 0], wx_send.at[0])
    left(w_q.at[pl.ds(0, nz - 1), :, 0], wz_send.at[1])
    left(w_q.at[0, pl.ds(0, NX - 1), 0], wx_send.at[1])
    for a in (0, 1):
        left(weights[a].at[:, :, c], wd_send.at[a])
    left(normed.at[pl.ds(0, n_tp - 1)], tok_send.at[0])
    left(forget_all.at[pl.ds(0, nz - 1), 0, 0], fz_send.at[0])
    left(forget_all.at[:, pl.ds(0, NX - 1), 0], fx_send.at[0])
    forget_twin(c).wait_send()
    left(wo_all.at[0, pl.ds(0, nz - 1), 0, 0], oz_send.at[0])
    left(wo_all.at[0, :, pl.ds(0, NX - 1), 0], ox_send.at[0])
    left(wo_all.at[pl.ds(0, n_tp - 1), :, :, 0], oy_send.at[0])
    left(wo_all.at[:, :, :, 0], od_send.at[0])
    left(gates_all.at[0, pl.ds(0, NX - 1), 0], gx_send.at[0])
    left(gates_all.at[0, :, 0], gz_send.at[0])
    left(gates_all.at[pl.ds(0, nz - 1), :, :], gz_send.at[1])
    left(kv_send.at[pl.ds(0, NX - 1)], kx_send.at[0])
    left(q_send.at[pl.ds(0, NX - 1)], qx_send.at[0])
    left(kv_all.at[:, :, 0], kd_send.at[0])
    for way in both:
        left(kv_all.at[pl.ds(0, nz - 1), pl.ds(0, NX // 2), 0], kz_send.at[way])
    left(att_recv.at[pl.ds(0, NX * n_tp - 1)], at_send.at[0])


def solution(mesh):
    n_sp, n_tp = mesh.shape["sp"], mesh.shape["tp"]
    nz = n_sp // (NX * NC)

    def on_device(
        tokens, norm_gain, w_query, w_key, w_value, w_forget, forget_offset, w_out_t, out_gain
    ):
        rows, model = tokens.shape
        w_rows, width = w_query.shape
        heads = w_forget.shape[1]
        block = rows * n_tp
        half = block // 2
        far = nz // 2
        vmem = pl.BlockSpec(memory_space=pltpu.VMEM)
        anywhere = pl.BlockSpec(memory_space=pl.ANY)
        dma = pltpu.SemaphoreType.DMA

        def pair(*shape):
            return [dma(shape), dma(shape)]

        return pl.pallas_call(
            functools.partial(layer_kernel, nz, n_tp),
            out_shape=jax.ShapeDtypeStruct((rows, model), BF16),
            in_specs=[
                vmem, vmem, anywhere, anywhere, anywhere, vmem,
                pl.BlockSpec(memory_space=pltpu.SMEM), anywhere, vmem,
            ],
            out_specs=vmem,
            scratch_shapes=[
                pltpu.VMEM((n_tp, rows, model), BF16),
                pltpu.VMEM((nz, NX, NC, w_rows, 2 * width), BF16),
                pltpu.VMEM((nz, NX, NC, w_rows, width), BF16),
                pltpu.VMEM((n_tp, nz, NX, NC, w_rows, width), BF16),
                pltpu.VMEM((nz, NX, NC, heads, LANES), F32),
                pltpu.VMEM((heads, 1, block), F32),
                pltpu.VMEM((nz, NX, NC, 1, block), F32),
                pltpu.VMEM((nz, LANES, LANES), BF16),
                pltpu.VMEM((heads, block, LANES), BF16),
                pltpu.VMEM((nz, NX, NC, block, LANES), BF16),
                pltpu.VMEM((heads, HEAD_DIM, block), BF16),
                pltpu.VMEM((NX, HEAD_DIM, block), BF16),
                pltpu.VMEM((NX, 2, block, block), BF16),
                pltpu.VMEM((NX * NC * half, 2 * LANES), BF16),
                pltpu.VMEM((NX, 2, NX * NC * half, block), F32),
                pltpu.VMEM((NX, 1, block), F32),
                pltpu.VMEM((NX, HEAD_DIM + 16, block), F32),
                pltpu.VMEM((NX, n_tp, rows // 2, LANES), BF16),
                pltpu.VMEM((NX * n_tp, rows // 2, LANES), BF16),
                dma((4,)),
                *pair(1),
                dma((2,)), dma((2, nz)),
                dma((2,)), dma((2, nz)),
                *pair(2),
                *pair(1),
                *pair(1),
                *pair(1),
                *pair(1),
                *pair(1),
                *pair(1),
                *pair(1),
                *pair(1),
                *pair(2),
                dma((1,)), dma((NX - 1,)),
                *pair(1),
                dma((2,)), dma((2, far, NX)),
                dma((1,)), dma((2, far + 1)),
                *pair(1),
            ],
            compiler_params=pltpu.CompilerParams(collective_id=0, has_side_effects=True),
        )(
            tokens, norm_gain.reshape(1, model), w_query, w_key, w_value, w_forget.T,
            forget_offset, w_out_t, out_gain.reshape(1, model),
        )

    return jax.shard_map(
        on_device,
        mesh=mesh,
        in_specs=(
            P(("sp", "tp"), None),
            P(),
            P("sp", "tp"),
            P("sp", "tp"),
            P("sp", "tp"),
            P("sp", "tp"),
            P("tp"),
            P("sp", "tp"),
            P(),
        ),
        out_specs=P(("sp", "tp"), None),
        check_vma=False,
    )
```

```python
import functools

import jax
import jax.numpy as jnp
from jax import lax
from jax.experimental import pallas as pl
from jax.experimental.pallas import tpu as pltpu
from jax.sharding import PartitionSpec as P

HEAD_DIM = 64
LANES = 128
NORM_EPS = 1e-06
NX, NC = 4, 2
WHOLE, HALVES = (1, 16), (2, 8)
MESH = pl.DeviceIdType.MESH
F32 = jnp.float32
BF16 = jnp.bfloat16
CONTRACT_LAST = (((1,), (1,)), ((), ()))


def rms_norm(floats, gain_row):
    scale_col = lax.rsqrt(jnp.mean(floats * floats, axis=-1, keepdims=True) + NORM_EPS)
    return (floats * scale_col * gain_row).astype(BF16)


def layer_kernel(
    nz, n_tp,
    tokens_ref, gain_ref, wq_ref, wk_ref, wv_ref, wf_ref, offset_ref, wo_ref, out_gain_ref,
    out_ref,
    normed, w_kv, w_q, wo_all, forget_all, gates_send, gates_all, bias_all,
    kv_send, kv_relay, kv_all, q_send, q_recv, q_rhs, key_side, scores, run_max, run_acc, att_send, att_recv,
    local_sem, tok_send, tok_recv, wz_send, wz_recv, wx_send, wx_recv, wd_send, wd_recv,
    fz_send, fz_recv, fx_send, fx_recv, fd_send, fd_recv,
    oz_send, oz_recv, ox_send, ox_recv, oy_send, oy_recv, od_send, od_recv,
    gx_send, gx_recv, gz_send, gz_recv, kx_send, kx_recv, qx_send, qx_recv,
    kz_send, kz_recv, kr_send, kr_recv, kt_send, kd_send, kd_recv, at_send, at_recv,
):
    sp, tp = lax.axis_index("sp"), lax.axis_index("tp")
    z = lax.div(sp, NX * NC)
    x = lax.rem(lax.div(sp, NC), NX)
    c = lax.rem(sp, NC)
    rows = tokens_ref.shape[0]
    block = rows * n_tp
    half = block // 2
    model = tokens_ref.shape[1]
    width = wq_ref.shape[1]
    heads = NX
    plane_blocks = NX * NC
    far = nz // 2

    def wrap(value, size):
        return lax.rem(value + size, size)

    def at(zz, xx, cc):
        return (zz * NX + xx) * NC + cc

    def remote(src, dst, send, recv, zz, xx, cc, yy):
        return pltpu.make_async_remote_copy(
            src_ref=src, dst_ref=dst, send_sem=send, recv_sem=recv,
            device_id=(at(zz, xx, cc), yy), device_id_type=MESH,
        )

    def landed(view, sem):
        remote(view, view, sem, sem, z, x, 1 - c, tp).wait_recv()

    def left(view, sem):
        remote(view, view, sem, sem, z, x, 1 - c, tp).wait_send()

    up, down = wrap(z + 1, nz), wrap(z - 1, nz)
    other = 1 - c

    weights = (w_kv, w_q)
    local = [
        pltpu.make_async_copy(
            ref, place.at[z, x, c, :, pl.ds(i * width, width)], local_sem.at[n]
        )
        for n, (ref, place, i) in enumerate(
            ((wk_ref, w_kv, 0), (wv_ref, w_kv, 1), (wq_ref, w_q, 0))
        )
    ]
    local.append(pltpu.make_async_copy(wo_ref, wo_all.at[tp, z, x, c], local_sem.at[3]))
    for copy in local:
        copy.start()

    barrier = pltpu.get_barrier_semaphore()
    near = [(at(z, wrap(x + dx, NX), c), tp) for dx in range(1, NX)]
    near += [(sp, wrap(tp + dy, n_tp)) for dy in range(1, n_tp)]
    near += [(at(wrap(z + dz, nz), x, c), tp) for dz in range(1, nz)]
    near += [(at(z, x, other), tp)]
    for device in near:
        pl.semaphore_signal(barrier, inc=1, device_id_type=MESH, device_id=device)

    w_rows = wf_ref.shape[1]
    forget_all[z, x, c] = jnp.concatenate(
        [wf_ref[...].astype(F32), jnp.zeros((heads, LANES - w_rows), F32)], axis=1
    )
    normed[tp] = rms_norm(tokens_ref[...].astype(F32), gain_ref[...])
    for copy in local:
        copy.wait()
    pl.semaphore_wait(barrier, len(near))

    def w_place(a, k, dx, core):
        return weights[a].at[wrap(z - k, nz), wrap(x + dx, NX), core]

    def w_z(a, k):
        place = w_place(a, 0, 0, c)
        return remote(
            place, place, wz_send.at[a], wz_recv.at[a, k], wrap(z + k, nz), x, c, tp
        )

    def w_x(a, k, dx):
        place = w_place(a, k, 0, c)
        return remote(
            place, place, wx_send.at[a], wx_recv.at[a, k],
            z, wrap(x + dx, NX), c, tp,
        )

    def w_twin(a, k):
        place = weights[a].at[wrap(z - k, nz), :, c]
        return remote(place, place, wd_send.at[a], wd_recv.at[a], z, x, other, tp)

    def w_group_z(k):
        place = w_q.at[z, :, c]
        return remote(
            place, place, wz_send.at[1], wz_recv.at[1, k], wrap(z + k, nz), x, c, tp
        )

    def w_onward(a, k):
        for dx in (2, 1, 3):
            w_x(a, k, dx).start()

    def nearest(n):
        return jnp.where(lax.rem(n, 2) == 1, lax.div(n + 1, 2), nz - lax.div(n, 2))

    def w_from_z(a, first, last):
        @pl.loop(first, last)
        def _(n):
            k = nearest(n)
            landed(w_place(a, k, 0, c), wz_recv.at[a, k])
            w_onward(a, k)

    def w_from_x(first, last):
        @pl.loop(first, last)
        def _(n):
            k = jnp.where(n == 0, 0, nearest(n))
            landed(w_kv.at[0, pl.ds(0, NX - 1), c], wx_recv.at[0, k])
            w_twin(0, k).start()

    def w_from_twin(a):
        landed(weights[a].at[:, :, other], wd_recv.at[a])

    def ring_subs(way, step):
        if step < far:
            return (0, 1, 2, 3)
        return (0, 1) if way == 0 else (2, 3)

    def plane_at(way, step):
        return wrap(z - step, nz) if way == 0 else wrap(z + step, nz)

    def ring_hop(ref, send, recv, way, step, sub):
        place = ref.at[plane_at(way, step - 1), wrap(x + sub, NX), c]
        return remote(
            place, place, send.at[way, min(sub, 1)], recv.at[way, step - 1, sub],
            (up, down)[way], x, c, tp,
        )

    def ring_wait(ref, send, recv, way, step, sub):
        landed(
            ref.at[plane_at(way, step), wrap(x + sub, NX), c], recv.at[way, step - 1, sub]
        )

    def twin(ref, send, recv, way, step, sub):
        place = ref.at[plane_at(way, step), wrap(x + sub, NX), c]
        return remote(place, place, send.at[0], recv.at[way, step], z, x, other, tp)

    def tok_copy(dy):
        return remote(
            normed.at[tp], normed.at[tp], tok_send.at[0], tok_recv.at[0],
            z, x, c, wrap(tp + dy, n_tp),
        )

    def forget_z(k):
        place = forget_all.at[z, x, c]
        return remote(
            place, place, fz_send.at[0], fz_recv.at[0], wrap(z + k, nz), x, c, tp
        )

    def forget_x(dx):
        place = forget_all.at[:, x, c]
        return remote(
            place, place, fx_send.at[0], fx_recv.at[0], z, wrap(x + dx, NX), c, tp
        )

    def forget_twin(core):
        place = forget_all.at[:, :, core]
        return remote(place, place, fd_send.at[0], fd_recv.at[0], z, x, other, tp)

    def wo_z(k):
        place = wo_all.at[tp, z, x, c]
        return remote(
            place, place, oz_send.at[0], oz_recv.at[0], wrap(z + k, nz), x, c, tp
        )

    def wo_x(dx):
        place = wo_all.at[tp, :, x, c]
        return remote(
            place, place, ox_send.at[0], ox_recv.at[0], z, wrap(x + dx, NX), c, tp
        )

    def wo_y(dy):
        place = wo_all.at[tp, :, :, c]
        return remote(
            place, place, oy_send.at[0], oy_recv.at[0], z, x, c, wrap(tp + dy, n_tp)
        )

    def wo_twin(dy):
        place = wo_all.at[wrap(tp + dy, n_tp), :, :, c]
        return remote(place, place, od_send.at[0], od_recv.at[0], z, x, other, tp)

    both = (0, 1)
    far_first = sorted(range(1, nz), key=lambda k: -min(k, nz - k))
    for k in far_first:
        forget_z(k).start()
    for k in far_first:
        w_z(0, k).start()
    for dx in (2, 1, 3):
        w_x(1, 0, dx).start()
    for dy in range(1, n_tp):
        tok_copy(dy).start()

    w_onward(0, 0)
    w_from_z(0, 1, 3)
    landed(w_q.at[0, pl.ds(0, NX - 1), c], wx_recv.at[1, 0])
    for k in far_first:
        w_group_z(k).start()
    for k in far_first:
        wo_z(k).start()
    w_twin(1, 0).start()
    w_from_z(0, 3, 5)
    landed(forget_all.at[pl.ds(0, nz - 1), 0, 0], fz_recv.at[0])
    for dx in range(1, NX):
        forget_x(dx).start()
    w_from_z(0, 5, nz)
    w_from_x(0, 5)
    landed(forget_all.at[:, pl.ds(0, NX - 1), 0], fx_recv.at[0])
    forget_twin(c).start()
    w_from_x(5, nz)
    landed(normed.at[pl.ds(0, n_tp - 1)], tok_recv.at[0])
    tokens_here = normed[...].reshape(block, model)
    forget_twin(other).wait_recv()
    forget_rows = jnp.concatenate(
        [
            forget_all[i // plane_blocks, (i // NC) % NX, i % NC][:, :w_rows]
            for i in range(nz * plane_blocks)
        ],
        axis=1,
    )
    forget_rows = jnp.concatenate(
        [forget_rows, jnp.zeros((8 - heads, model), F32)], axis=0
    ).astype(BF16)
    logits = lax.dot_general(
        forget_rows, tokens_here, CONTRACT_LAST, preferred_element_type=F32
    )
    head_row = lax.broadcasted_iota(jnp.int32, (8, block), 0)
    offsets = jnp.zeros((8, block), F32)
    for h in range(heads):
        offsets = jnp.where(head_row == h, offset_ref[h], offsets)
    n_tokens = nz * plane_blocks * block
    logits = logits + offsets + jnp.log(jnp.full((8, block), n_tokens, F32))
    log_gates = jnp.minimum(logits, 0.0) - jnp.log1p(jnp.exp(-jnp.abs(logits)))
    row_at = lax.broadcasted_iota(jnp.int32, (block, block), 0)
    col_at = lax.broadcasted_iota(jnp.int32, (block, block), 1)
    cum_here = jnp.dot(
        log_gates, jnp.where(row_at <= col_at, 1.0, 0.0).astype(F32),
        precision=lax.Precision.HIGHEST, preferred_element_type=F32,
    )
    for h in range(heads):
        gates_send[h] = cum_here[h : h + 1, :]
    gates_all[z, x, c] = gates_send[x]

    def gate_x(dx):
        hx = wrap(x + dx, NX)
        return remote(
            gates_send.at[hx], gates_all.at[z, x, c], gx_send.at[0], gx_recv.at[0],
            z, hx, c, tp,
        )

    for dx in range(1, NX):
        gate_x(dx).start()

    w_from_twin(0)

    def project(ref, i):
        columns = ref[:, :, :, :, i * width : (i + 1) * width].reshape(model, width)
        return jnp.dot(tokens_here, columns, preferred_element_type=F32)

    lane_at = lax.broadcasted_iota(jnp.int32, (half, LANES), 1)
    keys = project(w_kv, 0)
    values_t = project(w_kv, 1).T.astype(BF16)
    for h in range(heads):
        tile = keys[:, (h // 2) * LANES : (h // 2 + 1) * LANES]
        first, second = tile[:half], tile[half:]
        if h % 2 == 0:
            second = pltpu.roll(second, HEAD_DIM, axis=1)
        else:
            first = pltpu.roll(first, HEAD_DIM, axis=1)
        kv_send[h, :half, :] = jnp.where(lane_at < HEAD_DIM, first, second).astype(BF16)
        value_rows = values_t[h * HEAD_DIM : (h + 1) * HEAD_DIM]
        kv_send[h, half : half + HEAD_DIM, :] = value_rows[:, :half]
        kv_send[h, half + HEAD_DIM :, :] = value_rows[:, half:]

    def kv_x(dx):
        hx = wrap(x + dx, NX)
        return remote(
            kv_send.at[hx], kv_all.at[z, x, c], kx_send.at[0], kx_recv.at[dx - 1],
            z, hx, c, tp,
        )

    for dx in (2, 1, 3):
        kv_x(dx).start()
    kv_all[z, x, c] = kv_send[x]
    for way in both:
        ring_hop(kv_all, kz_send, kz_recv, way, 1, 0).start()
    twin(kv_all, kd_send, kd_recv, 0, 0, 0).start()

    def kv_off(way, dx):
        return remote(
            kv_send.at[wrap(x + dx, NX)], kv_relay.at[way, dx - 1],
            kr_send.at[0], kr_recv.at[way, dx - 1], (up, down)[way], x, c, tp,
        )

    def kv_turn(way, dx):
        return remote(
            kv_relay.at[way, dx - 1], kv_all.at[plane_at(way, 1), x, c],
            kt_send.at[0], kz_recv.at[way, 0, NX - dx], z, wrap(x + dx, NX), c, tp,
        )

    for dx in (2, 1, 3):
        for way in both:
            kv_off(way, dx).start()

    def first_sub(step):
        for way in both:
            if 0 not in ring_subs(way, step):
                continue
            ring_wait(kv_all, kz_send, kz_recv, way, step, 0)
            if step < far and 0 in ring_subs(way, step + 1):
                ring_hop(kv_all, kz_send, kz_recv, way, step + 1, 0).start()
            twin(kv_all, kd_send, kd_recv, way, step, 0).start()

    @pl.loop(1, nz)
    def _(n):
        k = nearest(n)
        landed(w_q.at[0, :, c], wz_recv.at[1, k])
        w_twin(1, k).start()

    w_from_twin(1)
    queries_t = (project(w_q, 0).astype(BF16).astype(F32) * HEAD_DIM ** (-0.5)).T.astype(BF16)
    for h in range(heads):
        q_send[h] = queries_t[h * HEAD_DIM : (h + 1) * HEAD_DIM]

    def q_x(dx):
        hx = wrap(x + dx, NX)
        return remote(
            q_send.at[hx], q_recv.at[x], qx_send.at[0], qx_recv.at[0], z, hx, c, tp
        )

    for dx in range(1, NX):
        q_x(dx).start()
    q_recv[x] = q_send[x]

    landed(gates_all.at[0, pl.ds(0, NX - 1), 0], gx_recv.at[0])

    def gate_z(k):
        cc = c if k % NC == 0 else other
        place = gates_all.at[z, :, c]
        group = min(k - 1, 1)
        return remote(
            place, place, gz_send.at[group], gz_recv.at[group],
            wrap(z + k // NC, nz), x, cc, tp,
        )

    for k in range(1, nz * NC):
        gate_z(k).start()

    first_sub(1)
    for dx in (2, 1, 3):
        for way in both:
            landed(kv_relay.at[way, dx - 1], kr_recv.at[way, dx - 1])
            kv_turn(way, dx).start()
        landed(kv_all.at[z, wrap(x - dx, NX), c], kx_recv.at[dx - 1])
        twin(kv_all, kd_send, kd_recv, 0, 0, NX - dx).start()

    landed(q_recv.at[pl.ds(0, NX - 1)], qx_recv.at[0])
    landed(wo_all.at[0, pl.ds(0, nz - 1), 0, 0], oz_recv.at[0])
    for dx in range(1, NX):
        wo_x(dx).start()
    ones_at = lax.broadcasted_iota(jnp.int32, (LANES, block), 0)
    no_rows = jnp.zeros((HEAD_DIM, block), BF16)
    for side in (0, 1):
        picks = ((ones_at // 8) % 2 == side) & (ones_at < 6 * 8)
        picks = jnp.where(picks, 1.0, 0.0).astype(BF16)
        for i in range(NX):
            parts = [q_recv[i], no_rows] if side == 0 else [no_rows, q_recv[i]]
            q_rhs[i, side] = jnp.concatenate(parts + [picks], axis=0)

    landed(gates_all.at[0, :, 0], gz_recv.at[0])
    landed(gates_all.at[pl.ds(0, nz - 1), :, :], gz_recv.at[1])

    n_blocks = nz * plane_blocks
    gate_rows = gates_all[...].reshape(n_blocks, block)
    mine = z * plane_blocks
    row_block = lax.broadcasted_iota(jnp.int32, (n_blocks, n_blocks), 0)
    col_block = lax.broadcasted_iota(jnp.int32, (n_blocks, n_blocks), 1)
    behind = (col_block >= row_block) & (col_block < mine)
    ahead = (col_block < row_block) & (col_block >= mine)
    steps_between = jnp.where(ahead, 1.0, 0.0) - jnp.where(behind, 1.0, 0.0)
    starts = jnp.dot(
        steps_between, gate_rows[:, half:], precision=lax.Precision.HIGHEST,
        preferred_element_type=F32,
    )[:, half - 1 :]
    bias = -(starts + gate_rows)
    bias_high = bias.astype(BF16).astype(F32)
    bias_rest = bias - bias_high
    bias_mid = bias_rest.astype(BF16).astype(F32)
    bias_low = bias_rest - bias_mid
    no_bias = jnp.zeros((LANES - 6 * plane_blocks, LANES), F32)
    for zz in range(nz):
        here = slice(zz * plane_blocks, (zz + 1) * plane_blocks)
        stack = []
        for part in (bias_high, bias_mid, bias_low):
            stack += [part[here, :half], part[here, half:]]
        bias_all[zz] = jnp.concatenate(stack + [no_bias], axis=0).T.astype(BF16)

    lane_block = lax.broadcasted_iota(jnp.int32, (8, LANES), 1) % 8

    def attend(plane, own, core=None):
        if core is None:
            blocks = [(b // NC, b % NC) for b in range(plane_blocks)]
            key_rows = kv_all[plane, :, :, :half, :].reshape(plane_blocks * half, LANES)
        else:
            blocks = [(b, core) for b in range(NX)]
            key_rows = kv_all[plane, :, core, :half, :].reshape(NX * half, LANES)
        size, lag = WHOLE if core is None else HALVES
        bias_cols = bias_all[plane]
        masks = [
            jnp.where(lane_block == xx * NC + cc, 1.0, 0.0)[:1].astype(BF16)
            for xx, cc in blocks
        ]
        bias_tiles = jnp.concatenate([bias_cols * mask for mask in masks], axis=0)
        key_side[: len(blocks) * half, :] = jnp.concatenate([key_rows, bias_tiles], axis=1)

        def score(i, side, b0):
            span = slice(b0 * half, (b0 + size) * half)
            s = jnp.dot(key_side[span, :], q_rhs[i, side], preferred_element_type=F32)
            if own and b0 + size > i * NC:
                row = lax.broadcasted_iota(jnp.int32, s.shape, 0)
                key_at = (b0 + row // half) * block + side * half + row % half
                query_at = lax.broadcasted_iota(jnp.int32, s.shape, 1) + (
                    (i * NC + c) * block
                )
                s = jnp.where(key_at <= query_at, s, -1e30)
            scores[i, side, span, :] = s
            return jnp.max(s, axis=0, keepdims=True)

        def absorb(i, side, b0, top):
            if own and side == 0 and b0 == 0:
                total = jnp.zeros((HEAD_DIM + 16, block), F32)
            else:
                old = run_max[i]
                top = jnp.maximum(old, top)
                total = run_acc[i] * jnp.exp(old - top)
            run_max[i] = top
            span = slice(b0 * half, (b0 + size) * half)
            weights = jnp.exp(scores[i, side, span, :] - top).astype(BF16)
            lo = half + side * HEAD_DIM
            value_cols = jnp.concatenate(
                [
                    kv_all[plane, xx, cc, lo : lo + HEAD_DIM, :]
                    for xx, cc in blocks[b0 : b0 + size]
                ],
                axis=1,
            )
            value_cols = jnp.concatenate(
                [value_cols, jnp.ones((16, size * half), BF16)], axis=0
            )
            run_acc[i] = total + jnp.dot(value_cols, weights, preferred_element_type=F32)

        chunks = [
            (i, side, b0)
            for side in (0, 1) for b0 in range(0, len(blocks), size) for i in range(NX)
            if not own or b0 < (i + 1) * NC
        ]
        tops = []
        for n in range(len(chunks) + lag):
            if n < len(chunks):
                tops.append(score(*chunks[n]))
            if n >= lag:
                absorb(*chunks[n - lag], tops[n - lag])

    landed(kv_all.at[z, :, other], kd_recv.at[0, 0])
    attend(z, True)
    first_sub(2)

    def wo_along_y():
        landed(wo_all.at[tp, :, pl.ds(0, NX - 1), c], ox_recv.at[0])
        for dy in range(1, n_tp):
            wo_y(dy).start()
        wo_twin(0).start()

    def kv_step(step, subs):
        for sub in subs:
            for way in both:
                whole = (sub < NX // 2) == (way == 0)

                def receive():
                    ring_wait(kv_all, kz_send, kz_recv, way, step, sub)
                    twin(kv_all, kd_send, kd_recv, way, step, sub).start()

                    @pl.when(step + (0 if whole else 1) < far)
                    def _():
                        ring_hop(kv_all, kz_send, kz_recv, way, step + 1, sub).start()

                if whole:
                    receive()
                else:
                    pl.when(step < far)(receive)

    def twin_step(step):
        for way in both:

            @pl.when(step < far)
            def _():
                landed(kv_all.at[plane_at(way, step), :, other], kd_recv.at[way, step])

            @pl.when(step == far)
            def _():
                landed(
                    kv_all.at[plane_at(way, step), pl.ds(0, NX // 2), other],
                    kd_recv.at[way, step],
                )

    def maybe_attend(plane, extra, core=None):
        @pl.when((plane < z) & extra)
        def _():
            attend(plane, False, core)

    @pl.loop(1, far + 1)
    def _(step):
        kv_step(step, (1,))
        pl.when(step == 2)(lambda: first_sub(3))
        pl.when(step == 2)(wo_along_y)
        pl.when(step == 3)(lambda: first_sub(4))
        maybe_attend(plane_at(1, step - 1), step > 1)
        kv_step(step, (2, 3))

        @pl.loop(0, NC)
        def _(part):
            pl.when(part == 1)(lambda: twin_step(step))
            maybe_attend(plane_at(0, step), True, lax.rem(c + part, NC))


    landed(wo_all.at[pl.ds(0, n_tp - 1), :, :, c], oy_recv.at[0])
    for dy in range(1, n_tp):
        wo_twin(dy).start()

    my_head = tp * NX + x
    quarter = rows // 2
    low_lane = lax.broadcasted_iota(jnp.int32, (quarter, LANES), 1) < HEAD_DIM

    def att_copy(rel, dy):
        i, yy = wrap(x + rel, NX), wrap(tp + dy, n_tp)
        return remote(
            att_send.at[i, yy], att_recv.at[my_head], at_send.at[0],
            at_recv.at[0], z, i, c, yy,
        )

    for rel in (2, 1, 3, 0):
        i = wrap(x + rel, NX)
        acc = run_acc[i]
        att = acc[:HEAD_DIM] / acc[HEAD_DIM : HEAD_DIM + 1]
        att = jnp.concatenate([att, att], axis=0).T
        for y in range(n_tp):
            first = att[y * rows : y * rows + quarter]
            second = att[y * rows + quarter : (y + 1) * rows]
            att_send[i, y] = jnp.where(low_lane, first, second).astype(BF16)
        for dy in (2, 1, 3, 0):
            if rel or dy:
                att_copy(rel, dy).start()
    att_recv[my_head] = att_send[x, tp]

    landed(wo_all.at[:, :, :, other], od_recv.at[0])
    landed(att_recv.at[pl.ds(0, NX * n_tp - 1)], at_recv.at[0])

    projected = jnp.zeros((rows, model), F32)
    for y in range(n_tp):
        pieces = []
        for pair in range(NX // 2):
            even = att_recv[y * NX + 2 * pair].astype(F32)
            odd = att_recv[y * NX + 2 * pair + 1].astype(F32)
            first = jnp.where(low_lane, even, pltpu.roll(odd, HEAD_DIM, axis=1))
            second = jnp.where(low_lane, pltpu.roll(even, HEAD_DIM, axis=1), odd)
            pieces.append(jnp.concatenate([first, second], axis=0).astype(BF16))
        columns = jnp.concatenate(pieces, axis=1)
        projected = projected + lax.dot_general(
            columns, wo_all[y].reshape(model, width), CONTRACT_LAST, preferred_element_type=F32
        )
    out_ref[...] = rms_norm(projected, out_gain_ref[...])

    left(w_kv.at[pl.ds(0, nz - 1), 0, 0], wz_send.at[0])
    left(w_kv.at[:, pl.ds(0, NX - 1), 0], wx_send.at[0])
    left(w_q.at[pl.ds(0, nz - 1), :, 0], wz_send.at[1])
    left(w_q.at[0, pl.ds(0, NX - 1), 0], wx_send.at[1])
    for a in (0, 1):
        left(weights[a].at[:, :, c], wd_send.at[a])
    left(normed.at[pl.ds(0, n_tp - 1)], tok_send.at[0])
    left(forget_all.at[pl.ds(0, nz - 1), 0, 0], fz_send.at[0])
    left(forget_all.at[:, pl.ds(0, NX - 1), 0], fx_send.at[0])
    forget_twin(c).wait_send()
    left(wo_all.at[0, pl.ds(0, nz - 1), 0, 0], oz_send.at[0])
    left(wo_all.at[0, :, pl.ds(0, NX - 1), 0], ox_send.at[0])
    left(wo_all.at[pl.ds(0, n_tp - 1), :, :, 0], oy_send.at[0])
    left(wo_all.at[:, :, :, 0], od_send.at[0])
    left(gates_all.at[0, pl.ds(0, NX - 1), 0], gx_send.at[0])
    left(gates_all.at[0, :, 0], gz_send.at[0])
    left(gates_all.at[pl.ds(0, nz - 1), :, :], gz_send.at[1])
    left(kv_send.at[pl.ds(0, NX - 1)], kx_send.at[0])
    left(q_send.at[pl.ds(0, NX - 1)], qx_send.at[0])
    left(kv_all.at[:, :, 0], kd_send.at[0])
    left(kv_all.at[pl.ds(0, 2 * (NX - 1)), 0, 0], kr_send.at[0])
    left(kv_all.at[pl.ds(0, 2 * (NX - 1)), 0, 0], kt_send.at[0])
    for way in both:
        for early in (0, 1):
            count = sum(
                (sub == 0) == (early == 0) and (sub == 0 or step > 1)
                for step in range(1, far + 1) for sub in ring_subs(way, step)
            )
            left(kv_all.at[pl.ds(0, count), 0, 0], kz_send.at[way, early])
    left(att_recv.at[pl.ds(0, NX * n_tp - 1)], at_send.at[0])


def solution(mesh):
    n_sp, n_tp = mesh.shape["sp"], mesh.shape["tp"]
    nz = n_sp // (NX * NC)

    def on_device(
        tokens, norm_gain, w_query, w_key, w_value, w_forget, forget_offset, w_out_t, out_gain
    ):
        rows, model = tokens.shape
        w_rows, width = w_query.shape
        heads = w_forget.shape[1]
        block = rows * n_tp
        half = block // 2
        far = nz // 2
        vmem = pl.BlockSpec(memory_space=pltpu.VMEM)
        anywhere = pl.BlockSpec(memory_space=pl.ANY)
        dma = pltpu.SemaphoreType.DMA

        def pair(*shape):
            return [dma(shape), dma(shape)]

        return pl.pallas_call(
            functools.partial(layer_kernel, nz, n_tp),
            out_shape=jax.ShapeDtypeStruct((rows, model), BF16),
            in_specs=[
                vmem, vmem, anywhere, anywhere, anywhere, vmem,
                pl.BlockSpec(memory_space=pltpu.SMEM), anywhere, vmem,
            ],
            out_specs=vmem,
            scratch_shapes=[
                pltpu.VMEM((n_tp, rows, model), BF16),
                pltpu.VMEM((nz, NX, NC, w_rows, 2 * width), BF16),
                pltpu.VMEM((nz, NX, NC, w_rows, width), BF16),
                pltpu.VMEM((n_tp, nz, NX, NC, w_rows, width), BF16),
                pltpu.VMEM((nz, NX, NC, heads, LANES), F32),
                pltpu.VMEM((heads, 1, block), F32),
                pltpu.VMEM((nz, NX, NC, 1, block), F32),
                pltpu.VMEM((nz, LANES, LANES), BF16),
                pltpu.VMEM((heads, block, LANES), BF16),
                pltpu.VMEM((2, NX - 1, block, LANES), BF16),
                pltpu.VMEM((nz, NX, NC, block, LANES), BF16),
                pltpu.VMEM((heads, HEAD_DIM, block), BF16),
                pltpu.VMEM((NX, HEAD_DIM, block), BF16),
                pltpu.VMEM((NX, 2, block, block), BF16),
                pltpu.VMEM((NX * NC * half, 2 * LANES), BF16),
                pltpu.VMEM((NX, 2, NX * NC * half, block), F32),
                pltpu.VMEM((NX, 1, block), F32),
                pltpu.VMEM((NX, HEAD_DIM + 16, block), F32),
                pltpu.VMEM((NX, n_tp, rows // 2, LANES), BF16),
                pltpu.VMEM((NX * n_tp, rows // 2, LANES), BF16),
                dma((4,)),
                *pair(1),
                dma((2,)), dma((2, nz)),
                dma((2,)), dma((2, nz)),
                *pair(2),
                *pair(1),
                *pair(1),
                *pair(1),
                *pair(1),
                *pair(1),
                *pair(1),
                *pair(1),
                *pair(1),
                *pair(2),
                dma((1,)), dma((NX - 1,)),
                *pair(1),
                dma((2, 2)), dma((2, far, NX)),
                dma((1,)), dma((2, NX - 1)), dma((1,)),
                dma((1,)), dma((2, far + 1)),
                *pair(1),
            ],
            compiler_params=pltpu.CompilerParams(collective_id=0, has_side_effects=True),
        )(
            tokens, norm_gain.reshape(1, model), w_query, w_key, w_value, w_forget.T,
            forget_offset, w_out_t, out_gain.reshape(1, model),
        )

    return jax.shard_map(
        on_device,
        mesh=mesh,
        in_specs=(
            P(("sp", "tp"), None),
            P(),
            P("sp", "tp"),
            P("sp", "tp"),
            P("sp", "tp"),
            P("sp", "tp"),
            P("tp"),
            P("sp", "tp"),
            P(),
        ),
        out_specs=P(("sp", "tp"), None),
        check_vma=False,
    )
```

```python
import functools

import jax
import jax.numpy as jnp
from jax import lax
from jax.experimental import pallas as pl
from jax.experimental.pallas import tpu as pltpu
from jax.sharding import PartitionSpec as P

HEAD_DIM = 64
LANES = 128
NORM_EPS = 1e-06
NX, NC = 4, 2
CHUNK, LAG = 2, 8
MESH = pl.DeviceIdType.MESH
F32 = jnp.float32
BF16 = jnp.bfloat16
CONTRACT_LAST = (((1,), (1,)), ((), ()))


def rms_norm(floats, gain_row):
    scale_col = lax.rsqrt(jnp.mean(floats * floats, axis=-1, keepdims=True) + NORM_EPS)
    return (floats * scale_col * gain_row).astype(BF16)


def layer_kernel(
    nz, n_tp,
    tokens_ref, gain_ref, wq_ref, wk_ref, wv_ref, wf_ref, offset_ref, wo_ref, out_gain_ref,
    out_ref,
    normed, w_kv, w_q, wo_all, forget_all, gates_send, gates_all, bias_all,
    kv_send, kv_all, q_send, q_recv, q_rhs, key_side, scores, run_max, run_acc, att_send, att_recv,
    local_sem, tok_send, tok_recv, wz_send, wz_recv, wx_send, wx_recv, wd_send, wd_recv,
    fz_send, fz_recv, fx_send, fx_recv, fd_send, fd_recv,
    oz_send, oz_recv, ox_send, ox_recv, oy_send, oy_recv, od_send, od_recv,
    gx_send, gx_recv, gz_send, gz_recv, kx_send, kx_recv, qx_send, qx_recv,
    kz_send, kz_recv, kd_send, kd_recv, at_send, at_recv,
):
    sp, tp = lax.axis_index("sp"), lax.axis_index("tp")
    z = lax.div(sp, NX * NC)
    x = lax.rem(lax.div(sp, NC), NX)
    c = lax.rem(sp, NC)
    rows = tokens_ref.shape[0]
    block = rows * n_tp
    half = block // 2
    model = tokens_ref.shape[1]
    width = wq_ref.shape[1]
    heads = NX
    plane_blocks = NX * NC
    far = nz // 2

    def wrap(value, size):
        return lax.rem(value + size, size)

    def at(zz, xx, cc):
        return (zz * NX + xx) * NC + cc

    def remote(src, dst, send, recv, zz, xx, cc, yy):
        return pltpu.make_async_remote_copy(
            src_ref=src, dst_ref=dst, send_sem=send, recv_sem=recv,
            device_id=(at(zz, xx, cc), yy), device_id_type=MESH,
        )

    def landed(view, sem):
        remote(view, view, sem, sem, z, x, 1 - c, tp).wait_recv()

    def left(view, sem):
        remote(view, view, sem, sem, z, x, 1 - c, tp).wait_send()

    up, down = wrap(z + 1, nz), wrap(z - 1, nz)
    other = 1 - c

    weights = (w_kv, w_q)
    local = [
        pltpu.make_async_copy(
            ref, place.at[z, x, c, :, pl.ds(i * width, width)], local_sem.at[n]
        )
        for n, (ref, place, i) in enumerate(
            ((wk_ref, w_kv, 0), (wv_ref, w_kv, 1), (wq_ref, w_q, 0))
        )
    ]
    local.append(pltpu.make_async_copy(wo_ref, wo_all.at[tp, z, x, c], local_sem.at[3]))
    for copy in local:
        copy.start()

    barrier = pltpu.get_barrier_semaphore()
    near = [(at(z, wrap(x + dx, NX), c), tp) for dx in range(1, NX)]
    near += [(sp, wrap(tp + dy, n_tp)) for dy in range(1, n_tp)]
    near += [(at(wrap(z + dz, nz), x, c), tp) for dz in range(1, nz)]
    near += [(at(z, x, other), tp)]
    for device in near:
        pl.semaphore_signal(barrier, inc=1, device_id_type=MESH, device_id=device)

    w_rows = wf_ref.shape[1]
    forget_all[z, x, c] = jnp.concatenate(
        [wf_ref[...].astype(F32), jnp.zeros((heads, LANES - w_rows), F32)], axis=1
    )
    normed[tp] = rms_norm(tokens_ref[...].astype(F32), gain_ref[...])
    for copy in local:
        copy.wait()
    pl.semaphore_wait(barrier, len(near))

    def w_place(a, k, dx, core):
        return weights[a].at[wrap(z - k, nz), wrap(x + dx, NX), core]

    def w_z(a, k):
        place = w_place(a, 0, 0, c)
        return remote(
            place, place, wz_send.at[a], wz_recv.at[a, k], wrap(z + k, nz), x, c, tp
        )

    def w_x(a, k, dx):
        place = w_place(a, k, 0, c)
        return remote(
            place, place, wx_send.at[a], wx_recv.at[a, k],
            z, wrap(x + dx, NX), c, tp,
        )

    def w_twin(a, k):
        place = weights[a].at[wrap(z - k, nz), :, c]
        return remote(place, place, wd_send.at[a], wd_recv.at[a], z, x, other, tp)

    def w_group_z(k):
        place = w_q.at[z, :, c]
        return remote(
            place, place, wz_send.at[1], wz_recv.at[1, k], wrap(z + k, nz), x, c, tp
        )

    def w_onward(a, k):
        for dx in (2, 1, 3):
            w_x(a, k, dx).start()

    def nearest(n):
        return jnp.where(lax.rem(n, 2) == 1, lax.div(n + 1, 2), nz - lax.div(n, 2))

    def w_from_z(a, first, last):
        @pl.loop(first, last)
        def _(n):
            k = nearest(n)
            landed(w_place(a, k, 0, c), wz_recv.at[a, k])
            w_onward(a, k)

    def w_from_x(first, last):
        @pl.loop(first, last)
        def _(n):
            k = jnp.where(n == 0, 0, nearest(n))
            landed(w_kv.at[0, pl.ds(0, NX - 1), c], wx_recv.at[0, k])
            w_twin(0, k).start()

    def w_from_twin(a):
        landed(weights[a].at[:, :, other], wd_recv.at[a])

    def ring_subs(way, step):
        if step < far:
            return (0, 1, 2, 3)
        return (0, 1) if way == 0 else (2, 3)

    def plane_at(way, step):
        return wrap(z - step, nz) if way == 0 else wrap(z + step, nz)

    def ring_hop(ref, send, recv, way, step, sub):
        place = ref.at[plane_at(way, step - 1), wrap(x + sub, NX), c]
        return remote(
            place, place, send.at[way], recv.at[way, step - 1, sub],
            (up, down)[way], x, c, tp,
        )

    def ring_wait(ref, send, recv, way, step, sub):
        landed(
            ref.at[plane_at(way, step), wrap(x + sub, NX), c], recv.at[way, step - 1, sub]
        )

    def twin(ref, send, recv, way, step, sub):
        place = ref.at[plane_at(way, step), wrap(x + sub, NX), c]
        return remote(place, place, send.at[0], recv.at[way, step], z, x, other, tp)

    def tok_copy(dy):
        return remote(
            normed.at[tp], normed.at[tp], tok_send.at[0], tok_recv.at[0],
            z, x, c, wrap(tp + dy, n_tp),
        )

    def forget_z(k):
        place = forget_all.at[z, x, c]
        return remote(
            place, place, fz_send.at[0], fz_recv.at[0], wrap(z + k, nz), x, c, tp
        )

    def forget_x(dx):
        place = forget_all.at[:, x, c]
        return remote(
            place, place, fx_send.at[0], fx_recv.at[0], z, wrap(x + dx, NX), c, tp
        )

    def forget_twin(core):
        place = forget_all.at[:, :, core]
        return remote(place, place, fd_send.at[0], fd_recv.at[0], z, x, other, tp)

    def wo_z(k):
        place = wo_all.at[tp, z, x, c]
        return remote(
            place, place, oz_send.at[0], oz_recv.at[0], wrap(z + k, nz), x, c, tp
        )

    def wo_x(dx):
        place = wo_all.at[tp, :, x, c]
        return remote(
            place, place, ox_send.at[0], ox_recv.at[0], z, wrap(x + dx, NX), c, tp
        )

    def wo_y(dy):
        place = wo_all.at[tp, :, :, c]
        return remote(
            place, place, oy_send.at[0], oy_recv.at[0], z, x, c, wrap(tp + dy, n_tp)
        )

    def wo_twin(dy):
        place = wo_all.at[wrap(tp + dy, n_tp), :, :, c]
        return remote(place, place, od_send.at[0], od_recv.at[0], z, x, other, tp)

    both = (0, 1)
    far_first = sorted(range(1, nz), key=lambda k: -min(k, nz - k))
    for k in far_first:
        forget_z(k).start()
    for k in far_first:
        w_z(0, k).start()
    for dx in (2, 1, 3):
        w_x(1, 0, dx).start()
    for dy in range(1, n_tp):
        tok_copy(dy).start()

    w_onward(0, 0)
    w_from_z(0, 1, 3)
    landed(w_q.at[0, pl.ds(0, NX - 1), c], wx_recv.at[1, 0])
    for k in far_first:
        w_group_z(k).start()
    for k in far_first:
        wo_z(k).start()
    w_twin(1, 0).start()
    w_from_z(0, 3, 5)
    landed(forget_all.at[pl.ds(0, nz - 1), 0, 0], fz_recv.at[0])
    for dx in range(1, NX):
        forget_x(dx).start()
    w_from_z(0, 5, nz)
    w_from_x(0, 5)
    landed(forget_all.at[:, pl.ds(0, NX - 1), 0], fx_recv.at[0])
    forget_twin(c).start()
    w_from_x(5, nz)
    landed(normed.at[pl.ds(0, n_tp - 1)], tok_recv.at[0])
    tokens_here = normed[...].reshape(block, model)
    forget_twin(other).wait_recv()
    forget_rows = jnp.concatenate(
        [
            forget_all[i // plane_blocks, (i // NC) % NX, i % NC][:, :w_rows]
            for i in range(nz * plane_blocks)
        ],
        axis=1,
    )
    forget_rows = jnp.concatenate(
        [forget_rows, jnp.zeros((8 - heads, model), F32)], axis=0
    ).astype(BF16)
    logits = lax.dot_general(
        forget_rows, tokens_here, CONTRACT_LAST, preferred_element_type=F32
    )
    head_row = lax.broadcasted_iota(jnp.int32, (8, block), 0)
    offsets = jnp.zeros((8, block), F32)
    for h in range(heads):
        offsets = jnp.where(head_row == h, offset_ref[h], offsets)
    n_tokens = nz * plane_blocks * block
    logits = logits + offsets + jnp.log(jnp.full((8, block), n_tokens, F32))
    log_gates = jnp.minimum(logits, 0.0) - jnp.log1p(jnp.exp(-jnp.abs(logits)))
    row_at = lax.broadcasted_iota(jnp.int32, (block, block), 0)
    col_at = lax.broadcasted_iota(jnp.int32, (block, block), 1)
    cum_here = jnp.dot(
        log_gates, jnp.where(row_at <= col_at, 1.0, 0.0).astype(F32),
        precision=lax.Precision.HIGHEST, preferred_element_type=F32,
    )
    for h in range(heads):
        gates_send[h] = cum_here[h : h + 1, :]
    gates_all[z, x, c] = gates_send[x]

    def gate_x(dx):
        hx = wrap(x + dx, NX)
        return remote(
            gates_send.at[hx], gates_all.at[z, x, c], gx_send.at[0], gx_recv.at[0],
            z, hx, c, tp,
        )

    for dx in range(1, NX):
        gate_x(dx).start()

    w_from_twin(0)

    def project(ref, i):
        columns = ref[:, :, :, :, i * width : (i + 1) * width].reshape(model, width)
        return jnp.dot(tokens_here, columns, preferred_element_type=F32)

    lane_at = lax.broadcasted_iota(jnp.int32, (half, LANES), 1)
    keys = project(w_kv, 0)
    values_t = project(w_kv, 1).T.astype(BF16)
    for h in range(heads):
        tile = keys[:, (h // 2) * LANES : (h // 2 + 1) * LANES]
        first, second = tile[:half], tile[half:]
        if h % 2 == 0:
            second = pltpu.roll(second, HEAD_DIM, axis=1)
        else:
            first = pltpu.roll(first, HEAD_DIM, axis=1)
        kv_send[h, :half, :] = jnp.where(lane_at < HEAD_DIM, first, second).astype(BF16)
        value_rows = values_t[h * HEAD_DIM : (h + 1) * HEAD_DIM]
        kv_send[h, half : half + HEAD_DIM, :] = value_rows[:, :half]
        kv_send[h, half + HEAD_DIM :, :] = value_rows[:, half:]

    def kv_x(dx):
        hx = wrap(x + dx, NX)
        return remote(
            kv_send.at[hx], kv_all.at[z, x, c], kx_send.at[0], kx_recv.at[dx - 1],
            z, hx, c, tp,
        )

    for dx in range(1, NX):
        kv_x(dx).start()
    kv_all[z, x, c] = kv_send[x]
    for way in both:
        ring_hop(kv_all, kz_send, kz_recv, way, 1, 0).start()
    twin(kv_all, kd_send, kd_recv, 0, 0, 0).start()

    def first_sub(step):
        for way in both:
            if 0 not in ring_subs(way, step):
                continue
            ring_wait(kv_all, kz_send, kz_recv, way, step, 0)
            if step < far and 0 in ring_subs(way, step + 1):
                ring_hop(kv_all, kz_send, kz_recv, way, step + 1, 0).start()
            twin(kv_all, kd_send, kd_recv, way, step, 0).start()

    @pl.loop(1, nz)
    def _(n):
        k = nearest(n)
        landed(w_q.at[0, :, c], wz_recv.at[1, k])
        w_twin(1, k).start()

    w_from_twin(1)
    queries_t = (project(w_q, 0).astype(BF16).astype(F32) * HEAD_DIM ** (-0.5)).T.astype(BF16)
    for h in range(heads):
        q_send[h] = queries_t[h * HEAD_DIM : (h + 1) * HEAD_DIM]

    def q_x(dx):
        hx = wrap(x + dx, NX)
        return remote(
            q_send.at[hx], q_recv.at[x], qx_send.at[0], qx_recv.at[0], z, hx, c, tp
        )

    for dx in range(1, NX):
        q_x(dx).start()
    q_recv[x] = q_send[x]

    landed(gates_all.at[0, pl.ds(0, NX - 1), 0], gx_recv.at[0])

    def gate_z(k):
        cc = c if k % NC == 0 else other
        place = gates_all.at[z, :, c]
        group = min(k - 1, 1)
        return remote(
            place, place, gz_send.at[group], gz_recv.at[group],
            wrap(z + k // NC, nz), x, cc, tp,
        )

    for k in range(1, nz * NC):
        gate_z(k).start()

    first_sub(1)
    for sub in (1, 3, 2):
        dx = NX - sub
        landed(kv_all.at[z, wrap(x + sub, NX), c], kx_recv.at[dx - 1])
        for way in both:
            ring_hop(kv_all, kz_send, kz_recv, way, 1, sub).start()
        twin(kv_all, kd_send, kd_recv, 0, 0, sub).start()

    landed(q_recv.at[pl.ds(0, NX - 1)], qx_recv.at[0])
    landed(wo_all.at[0, pl.ds(0, nz - 1), 0, 0], oz_recv.at[0])
    for dx in range(1, NX):
        wo_x(dx).start()
    ones_at = lax.broadcasted_iota(jnp.int32, (LANES, block), 0)
    no_rows = jnp.zeros((HEAD_DIM, block), BF16)
    for side in (0, 1):
        picks = ((ones_at // 8) % 2 == side) & (ones_at < 6 * 8)
        picks = jnp.where(picks, 1.0, 0.0).astype(BF16)
        for i in range(NX):
            parts = [q_recv[i], no_rows] if side == 0 else [no_rows, q_recv[i]]
            q_rhs[i, side] = jnp.concatenate(parts + [picks], axis=0)

    landed(gates_all.at[0, :, 0], gz_recv.at[0])
    landed(gates_all.at[pl.ds(0, nz - 1), :, :], gz_recv.at[1])

    n_blocks = nz * plane_blocks
    gate_rows = gates_all[...].reshape(n_blocks, block)
    mine = z * plane_blocks
    row_block = lax.broadcasted_iota(jnp.int32, (n_blocks, n_blocks), 0)
    col_block = lax.broadcasted_iota(jnp.int32, (n_blocks, n_blocks), 1)
    behind = (col_block >= row_block) & (col_block < mine)
    ahead = (col_block < row_block) & (col_block >= mine)
    steps_between = jnp.where(ahead, 1.0, 0.0) - jnp.where(behind, 1.0, 0.0)
    starts = jnp.dot(
        steps_between, gate_rows[:, half:], precision=lax.Precision.HIGHEST,
        preferred_element_type=F32,
    )[:, half - 1 :]
    bias = -(starts + gate_rows)
    bias_high = bias.astype(BF16).astype(F32)
    bias_rest = bias - bias_high
    bias_mid = bias_rest.astype(BF16).astype(F32)
    bias_low = bias_rest - bias_mid
    no_bias = jnp.zeros((LANES - 6 * plane_blocks, LANES), F32)
    for zz in range(nz):
        here = slice(zz * plane_blocks, (zz + 1) * plane_blocks)
        stack = []
        for part in (bias_high, bias_mid, bias_low):
            stack += [part[here, :half], part[here, half:]]
        bias_all[zz] = jnp.concatenate(stack + [no_bias], axis=0).T.astype(BF16)

    lane_block = lax.broadcasted_iota(jnp.int32, (8, LANES), 1) % 8
    ones_rows = jnp.ones((16, CHUNK * half), BF16)

    def attend(plane, own, core=None):
        if core is None:
            blocks = [(b // NC, b % NC) for b in range(plane_blocks)]
            key_rows = kv_all[plane, :, :, :half, :].reshape(plane_blocks * half, LANES)
        else:
            blocks = [(b, core) for b in range(NX)]
            key_rows = kv_all[plane, :, core, :half, :].reshape(NX * half, LANES)
        bias_cols = bias_all[plane]
        masks = [
            jnp.where(lane_block == xx * NC + cc, 1.0, 0.0)[:1].astype(BF16)
            for xx, cc in blocks
        ]
        bias_tiles = jnp.concatenate([bias_cols * mask for mask in masks], axis=0)
        key_side[: len(blocks) * half, :] = jnp.concatenate([key_rows, bias_tiles], axis=1)

        def score(i, side, b0):
            span = slice(b0 * half, (b0 + CHUNK) * half)
            s = jnp.dot(key_side[span, :], q_rhs[i, side], preferred_element_type=F32)
            if own and b0 == i * NC:
                row = lax.broadcasted_iota(jnp.int32, s.shape, 0)
                key_at = (b0 + row // half) * block + side * half + row % half
                query_at = lax.broadcasted_iota(jnp.int32, s.shape, 1) + (
                    (i * NC + c) * block
                )
                s = jnp.where(key_at <= query_at, s, -1e30)
            scores[i, side, span, :] = s
            return jnp.max(s, axis=0, keepdims=True)

        def absorb(i, side, b0, top):
            if own and side == 0 and b0 == 0:
                total = jnp.zeros((HEAD_DIM + 16, block), F32)
            else:
                old = run_max[i]
                top = jnp.maximum(old, top)
                total = run_acc[i] * jnp.exp(old - top)
            run_max[i] = top
            span = slice(b0 * half, (b0 + CHUNK) * half)
            weights = jnp.exp(scores[i, side, span, :] - top).astype(BF16)
            lo = half + side * HEAD_DIM
            value_cols = jnp.concatenate(
                [
                    kv_all[plane, xx, cc, lo : lo + HEAD_DIM, :]
                    for xx, cc in blocks[b0 : b0 + CHUNK]
                ],
                axis=1,
            )
            value_cols = jnp.concatenate([value_cols, ones_rows], axis=0)
            run_acc[i] = total + jnp.dot(value_cols, weights, preferred_element_type=F32)

        chunks = [
            (i, side, b0)
            for side in (0, 1) for b0 in range(0, len(blocks), CHUNK) for i in range(NX)
            if not own or b0 <= i * NC
        ]
        tops = []
        for n in range(len(chunks) + LAG):
            if n < len(chunks):
                tops.append(score(*chunks[n]))
            if n >= LAG:
                absorb(*chunks[n - LAG], tops[n - LAG])

    landed(kv_all.at[z, :, other], kd_recv.at[0, 0])
    attend(z, True)
    first_sub(2)

    def wo_along_y():
        landed(wo_all.at[tp, :, pl.ds(0, NX - 1), c], ox_recv.at[0])
        for dy in range(1, n_tp):
            wo_y(dy).start()
        wo_twin(0).start()

    def kv_step(step, subs):
        for sub in subs:
            for way in both:
                whole = (sub < NX // 2) == (way == 0)

                def receive():
                    ring_wait(kv_all, kz_send, kz_recv, way, step, sub)
                    twin(kv_all, kd_send, kd_recv, way, step, sub).start()

                    @pl.when(step + (0 if whole else 1) < far)
                    def _():
                        ring_hop(kv_all, kz_send, kz_recv, way, step + 1, sub).start()

                if whole:
                    receive()
                else:
                    pl.when(step < far)(receive)

    def twin_step(step):
        for way in both:

            @pl.when(step < far)
            def _():
                landed(kv_all.at[plane_at(way, step), :, other], kd_recv.at[way, step])

            @pl.when(step == far)
            def _():
                landed(
                    kv_all.at[plane_at(way, step), pl.ds(0, NX // 2), other],
                    kd_recv.at[way, step],
                )

    def maybe_attend(plane, extra, core=None):
        @pl.when((plane < z) & extra)
        def _():
            attend(plane, False, core)

    @pl.loop(1, far + 1)
    def _(step):
        kv_step(step, (1,))
        pl.when(step == 2)(lambda: first_sub(3))
        pl.when(step == 2)(wo_along_y)
        pl.when(step == 3)(lambda: first_sub(4))
        maybe_attend(plane_at(1, step - 1), step > 1)
        kv_step(step, (2, 3))

        @pl.loop(0, NC)
        def _(part):
            pl.when(part == 1)(lambda: twin_step(step))
            maybe_attend(plane_at(0, step), True, lax.rem(c + part, NC))


    my_head = tp * NX + x
    quarter = rows // 2
    low_lane = lax.broadcasted_iota(jnp.int32, (quarter, LANES), 1) < HEAD_DIM

    def att_copy(rel, dy):
        i, yy = wrap(x + rel, NX), wrap(tp + dy, n_tp)
        return remote(
            att_send.at[i, yy], att_recv.at[my_head], at_send.at[0],
            at_recv.at[0], z, i, c, yy,
        )

    for rel in (2, 1, 3, 0):
        i = wrap(x + rel, NX)
        acc = run_acc[i]
        att = acc[:HEAD_DIM] / acc[HEAD_DIM : HEAD_DIM + 1]
        att = jnp.concatenate([att, att], axis=0).T
        for y in range(n_tp):
            first = att[y * rows : y * rows + quarter]
            second = att[y * rows + quarter : (y + 1) * rows]
            att_send[i, y] = jnp.where(low_lane, first, second).astype(BF16)
        for dy in (2, 1, 3, 0):
            if rel or dy:
                att_copy(rel, dy).start()
    att_recv[my_head] = att_send[x, tp]
    landed(wo_all.at[pl.ds(0, n_tp - 1), :, :, c], oy_recv.at[0])
    for dy in range(1, n_tp):
        wo_twin(dy).start()

    landed(wo_all.at[:, :, :, other], od_recv.at[0])
    landed(att_recv.at[pl.ds(0, NX * n_tp - 1)], at_recv.at[0])

    projected = jnp.zeros((rows, model), F32)
    for y in range(n_tp):
        pieces = []
        for pair in range(NX // 2):
            even = att_recv[y * NX + 2 * pair].astype(F32)
            odd = att_recv[y * NX + 2 * pair + 1].astype(F32)
            first = jnp.where(low_lane, even, pltpu.roll(odd, HEAD_DIM, axis=1))
            second = jnp.where(low_lane, pltpu.roll(even, HEAD_DIM, axis=1), odd)
            pieces.append(jnp.concatenate([first, second], axis=0).astype(BF16))
        columns = jnp.concatenate(pieces, axis=1)
        projected = projected + lax.dot_general(
            columns, wo_all[y].reshape(model, width), CONTRACT_LAST, preferred_element_type=F32
        )
    out_ref[...] = rms_norm(projected, out_gain_ref[...])

    left(w_kv.at[pl.ds(0, nz - 1), 0, 0], wz_send.at[0])
    left(w_kv.at[:, pl.ds(0, NX - 1), 0], wx_send.at[0])
    left(w_q.at[pl.ds(0, nz - 1), :, 0], wz_send.at[1])
    left(w_q.at[0, pl.ds(0, NX - 1), 0], wx_send.at[1])
    for a in (0, 1):
        left(weights[a].at[:, :, c], wd_send.at[a])
    left(normed.at[pl.ds(0, n_tp - 1)], tok_send.at[0])
    left(forget_all.at[pl.ds(0, nz - 1), 0, 0], fz_send.at[0])
    left(forget_all.at[:, pl.ds(0, NX - 1), 0], fx_send.at[0])
    forget_twin(c).wait_send()
    left(wo_all.at[0, pl.ds(0, nz - 1), 0, 0], oz_send.at[0])
    left(wo_all.at[0, :, pl.ds(0, NX - 1), 0], ox_send.at[0])
    left(wo_all.at[pl.ds(0, n_tp - 1), :, :, 0], oy_send.at[0])
    left(wo_all.at[:, :, :, 0], od_send.at[0])
    left(gates_all.at[0, pl.ds(0, NX - 1), 0], gx_send.at[0])
    left(gates_all.at[0, :, 0], gz_send.at[0])
    left(gates_all.at[pl.ds(0, nz - 1), :, :], gz_send.at[1])
    left(kv_send.at[pl.ds(0, NX - 1)], kx_send.at[0])
    left(q_send.at[pl.ds(0, NX - 1)], qx_send.at[0])
    left(kv_all.at[:, :, 0], kd_send.at[0])
    for way in both:
        left(kv_all.at[pl.ds(0, nz - 1), pl.ds(0, NX // 2), 0], kz_send.at[way])
    left(att_recv.at[pl.ds(0, NX * n_tp - 1)], at_send.at[0])


def solution(mesh):
    n_sp, n_tp = mesh.shape["sp"], mesh.shape["tp"]
    nz = n_sp // (NX * NC)

    def on_device(
        tokens, norm_gain, w_query, w_key, w_value, w_forget, forget_offset, w_out_t, out_gain
    ):
        rows, model = tokens.shape
        w_rows, width = w_query.shape
        heads = w_forget.shape[1]
        block = rows * n_tp
        half = block // 2
        far = nz // 2
        vmem = pl.BlockSpec(memory_space=pltpu.VMEM)
        anywhere = pl.BlockSpec(memory_space=pl.ANY)
        dma = pltpu.SemaphoreType.DMA

        def pair(*shape):
            return [dma(shape), dma(shape)]

        return pl.pallas_call(
            functools.partial(layer_kernel, nz, n_tp),
            out_shape=jax.ShapeDtypeStruct((rows, model), BF16),
            in_specs=[
                vmem, vmem, anywhere, anywhere, anywhere, vmem,
                pl.BlockSpec(memory_space=pltpu.SMEM), anywhere, vmem,
            ],
            out_specs=vmem,
            scratch_shapes=[
                pltpu.VMEM((n_tp, rows, model), BF16),
                pltpu.VMEM((nz, NX, NC, w_rows, 2 * width), BF16),
                pltpu.VMEM((nz, NX, NC, w_rows, width), BF16),
                pltpu.VMEM((n_tp, nz, NX, NC, w_rows, width), BF16),
                pltpu.VMEM((nz, NX, NC, heads, LANES), F32),
                pltpu.VMEM((heads, 1, block), F32),
                pltpu.VMEM((nz, NX, NC, 1, block), F32),
                pltpu.VMEM((nz, LANES, LANES), BF16),
                pltpu.VMEM((heads, block, LANES), BF16),
                pltpu.VMEM((nz, NX, NC, block, LANES), BF16),
                pltpu.VMEM((heads, HEAD_DIM, block), BF16),
                pltpu.VMEM((NX, HEAD_DIM, block), BF16),
                pltpu.VMEM((NX, 2, block, block), BF16),
                pltpu.VMEM((NX * NC * half, 2 * LANES), BF16),
                pltpu.VMEM((NX, 2, NX * NC * half, block), F32),
                pltpu.VMEM((NX, 1, block), F32),
                pltpu.VMEM((NX, HEAD_DIM + 16, block), F32),
                pltpu.VMEM((NX, n_tp, rows // 2, LANES), BF16),
                pltpu.VMEM((NX * n_tp, rows // 2, LANES), BF16),
                dma((4,)),
                *pair(1),
                dma((2,)), dma((2, nz)),
                dma((2,)), dma((2, nz)),
                *pair(2),
                *pair(1),
                *pair(1),
                *pair(1),
                *pair(1),
                *pair(1),
                *pair(1),
                *pair(1),
                *pair(1),
                *pair(2),
                dma((1,)), dma((NX - 1,)),
                *pair(1),
                dma((2,)), dma((2, far, NX)),
                dma((1,)), dma((2, far + 1)),
                *pair(1),
            ],
            compiler_params=pltpu.CompilerParams(collective_id=0, has_side_effects=True),
        )(
            tokens, norm_gain.reshape(1, model), w_query, w_key, w_value, w_forget.T,
            forget_offset, w_out_t, out_gain.reshape(1, model),
        )

    return jax.shard_map(
        on_device,
        mesh=mesh,
        in_specs=(
            P(("sp", "tp"), None),
            P(),
            P("sp", "tp"),
            P("sp", "tp"),
            P("sp", "tp"),
            P("sp", "tp"),
            P("tp"),
            P("sp", "tp"),
            P(),
        ),
        out_specs=P(("sp", "tp"), None),
        check_vma=False,
    )
```

```python
import functools

import jax
import jax.numpy as jnp
from jax import lax
from jax.experimental import pallas as pl
from jax.experimental.pallas import tpu as pltpu
from jax.sharding import PartitionSpec as P

HEAD_DIM = 64
LANES = 128
NORM_EPS = 1e-06
NX, NC = 4, 2
CHUNK, LAG = 2, 8
MESH = pl.DeviceIdType.MESH
F32 = jnp.float32
BF16 = jnp.bfloat16
CONTRACT_LAST = (((1,), (1,)), ((), ()))


def rms_norm(floats, gain_row):
    scale_col = lax.rsqrt(jnp.mean(floats * floats, axis=-1, keepdims=True) + NORM_EPS)
    return (floats * scale_col * gain_row).astype(BF16)


def layer_kernel(
    nz, n_tp,
    tokens_ref, gain_ref, wq_ref, wk_ref, wv_ref, wf_ref, offset_ref, wo_ref, out_gain_ref,
    out_ref,
    normed, w_kv, w_q, wo_all, forget_all, gates_send, gates_all, bias_all,
    kv_send, kv_all, q_send, q_recv, q_rhs, key_side, scores, run_max, run_acc, att_send, att_recv,
    local_sem, tok_send, tok_recv, wz_send, wz_recv, wx_send, wx_recv, wd_send, wd_recv,
    fz_send, fz_recv, fx_send, fx_recv, fd_send, fd_recv,
    oz_send, oz_recv, ox_send, ox_recv, oy_send, oy_recv, od_send, od_recv,
    gx_send, gx_recv, gz_send, gz_recv, kx_send, kx_recv, qx_send, qx_recv,
    kz_send, kz_recv, kd_send, kd_recv, at_send, at_recv,
):
    sp, tp = lax.axis_index("sp"), lax.axis_index("tp")
    z = lax.div(sp, NX * NC)
    x = lax.rem(lax.div(sp, NC), NX)
    c = lax.rem(sp, NC)
    rows = tokens_ref.shape[0]
    block = rows * n_tp
    half = block // 2
    model = tokens_ref.shape[1]
    width = wq_ref.shape[1]
    heads = NX
    plane_blocks = NX * NC
    far = nz // 2

    def wrap(value, size):
        return lax.rem(value + size, size)

    def at(zz, xx, cc):
        return (zz * NX + xx) * NC + cc

    def remote(src, dst, send, recv, zz, xx, cc, yy):
        return pltpu.make_async_remote_copy(
            src_ref=src, dst_ref=dst, send_sem=send, recv_sem=recv,
            device_id=(at(zz, xx, cc), yy), device_id_type=MESH,
        )

    def landed(view, sem):
        remote(view, view, sem, sem, z, x, 1 - c, tp).wait_recv()

    def left(view, sem):
        remote(view, view, sem, sem, z, x, 1 - c, tp).wait_send()

    up, down = wrap(z + 1, nz), wrap(z - 1, nz)
    other = 1 - c

    weights = (w_kv, w_q)
    local = [
        pltpu.make_async_copy(
            ref, place.at[z, x, c, :, pl.ds(i * width, width)], local_sem.at[n]
        )
        for n, (ref, place, i) in enumerate(
            ((wk_ref, w_kv, 0), (wv_ref, w_kv, 1), (wq_ref, w_q, 0))
        )
    ]
    local.append(pltpu.make_async_copy(wo_ref, wo_all.at[tp, z, x, c], local_sem.at[3]))
    for copy in local:
        copy.start()

    barrier = pltpu.get_barrier_semaphore()
    near = [(at(z, wrap(x + dx, NX), c), tp) for dx in range(1, NX)]
    near += [(sp, wrap(tp + dy, n_tp)) for dy in range(1, n_tp)]
    near += [(at(wrap(z + dz, nz), x, c), tp) for dz in range(1, nz)]
    near += [(at(z, x, other), tp)]
    for device in near:
        pl.semaphore_signal(barrier, inc=1, device_id_type=MESH, device_id=device)

    w_rows = wf_ref.shape[1]
    forget_all[z, x, c] = jnp.concatenate(
        [wf_ref[...].astype(F32), jnp.zeros((heads, LANES - w_rows), F32)], axis=1
    )
    normed[tp] = rms_norm(tokens_ref[...].astype(F32), gain_ref[...])
    for copy in local:
        copy.wait()
    pl.semaphore_wait(barrier, len(near))

    def w_place(a, k, dx, core):
        return weights[a].at[wrap(z - k, nz), wrap(x + dx, NX), core]

    def w_z(a, k):
        place = w_place(a, 0, 0, c)
        return remote(
            place, place, wz_send.at[a], wz_recv.at[a, k], wrap(z + k, nz), x, c, tp
        )

    def w_x(a, k, dx):
        place = w_place(a, k, 0, c)
        return remote(
            place, place, wx_send.at[a], wx_recv.at[a, k],
            z, wrap(x + dx, NX), c, tp,
        )

    def w_twin(a, k):
        place = weights[a].at[wrap(z - k, nz), :, c]
        return remote(place, place, wd_send.at[a], wd_recv.at[a], z, x, other, tp)

    def w_group_z(k):
        place = w_q.at[z, :, c]
        return remote(
            place, place, wz_send.at[1], wz_recv.at[1, k], wrap(z + k, nz), x, c, tp
        )

    def w_onward(a, k):
        for dx in (2, 1, 3):
            w_x(a, k, dx).start()

    def nearest(n):
        return jnp.where(lax.rem(n, 2) == 1, lax.div(n + 1, 2), nz - lax.div(n, 2))

    def w_from_z(a, first, last):
        @pl.loop(first, last)
        def _(n):
            k = nearest(n)
            landed(w_place(a, k, 0, c), wz_recv.at[a, k])
            w_onward(a, k)

    def w_from_x(first, last):
        @pl.loop(first, last)
        def _(n):
            k = jnp.where(n == 0, 0, nearest(n))
            landed(w_kv.at[0, pl.ds(0, NX - 1), c], wx_recv.at[0, k])
            w_twin(0, k).start()

    def w_from_twin(a):
        landed(weights[a].at[:, :, other], wd_recv.at[a])

    def plane_at(way, step):
        return wrap(z - step, nz) if way == 0 else wrap(z + step, nz)

    def steps_of(way, sub):
        return far if (sub < NX // 2) == (way == 0) else far - 1

    def sends(way, step, sub):
        inside = step <= steps_of(way, sub)
        if way == 0:
            return inside & (z >= step - 1) & (z < nz - 1)
        return inside & (wrap(z + step - 1, nz) < steps_of(way, sub))

    def receives(way, step, sub):
        inside = step <= steps_of(way, sub)
        if way == 0:
            return inside & (z >= step)
        return inside & (wrap(z + step, nz) < steps_of(way, sub))

    def reads(way, step):
        return z >= step if way == 0 else z + step >= nz

    def ring_hop(ref, send, recv, way, step, sub):
        place = ref.at[plane_at(way, step - 1), wrap(x + sub, NX), c]
        return remote(
            place, place, send.at[way, step - 1, sub], recv.at[way, step - 1, sub],
            (up, down)[way], x, c, tp,
        )

    def ring_wait(ref, send, recv, way, step, sub):
        landed(
            ref.at[plane_at(way, step), wrap(x + sub, NX), c], recv.at[way, step - 1, sub]
        )

    def twin(ref, send, recv, way, step, sub):
        place = ref.at[plane_at(way, step), wrap(x + sub, NX), c]
        return remote(place, place, send.at[way, step], recv.at[way, step], z, x, other, tp)

    def tok_copy(dy):
        return remote(
            normed.at[tp], normed.at[tp], tok_send.at[0], tok_recv.at[0],
            z, x, c, wrap(tp + dy, n_tp),
        )

    def forget_z(k):
        place = forget_all.at[z, x, c]
        return remote(
            place, place, fz_send.at[0], fz_recv.at[0], wrap(z + k, nz), x, c, tp
        )

    def forget_x(dx):
        place = forget_all.at[:, x, c]
        return remote(
            place, place, fx_send.at[0], fx_recv.at[0], z, wrap(x + dx, NX), c, tp
        )

    def forget_twin(core):
        place = forget_all.at[:, :, core]
        return remote(place, place, fd_send.at[0], fd_recv.at[0], z, x, other, tp)

    def wo_z(k):
        place = wo_all.at[tp, z, x, c]
        return remote(
            place, place, oz_send.at[0], oz_recv.at[0], wrap(z + k, nz), x, c, tp
        )

    def wo_x(dx):
        place = wo_all.at[tp, :, x, c]
        return remote(
            place, place, ox_send.at[0], ox_recv.at[0], z, wrap(x + dx, NX), c, tp
        )

    def wo_y(dy):
        place = wo_all.at[tp, :, :, c]
        return remote(
            place, place, oy_send.at[0], oy_recv.at[0], z, x, c, wrap(tp + dy, n_tp)
        )

    def wo_twin(dy):
        place = wo_all.at[wrap(tp + dy, n_tp), :, :, c]
        return remote(place, place, od_send.at[0], od_recv.at[0], z, x, other, tp)

    both = (0, 1)
    far_first = sorted(range(1, nz), key=lambda k: -min(k, nz - k))
    for k in far_first:
        forget_z(k).start()
    for k in far_first:
        w_z(0, k).start()
    for dx in (2, 1, 3):
        w_x(1, 0, dx).start()
    for dy in range(1, n_tp):
        tok_copy(dy).start()

    w_onward(0, 0)
    w_from_z(0, 1, 3)
    landed(w_q.at[0, pl.ds(0, NX - 1), c], wx_recv.at[1, 0])
    for k in far_first:
        w_group_z(k).start()
    for k in far_first:
        wo_z(k).start()
    w_twin(1, 0).start()
    w_from_z(0, 3, 5)
    landed(forget_all.at[pl.ds(0, nz - 1), 0, 0], fz_recv.at[0])
    for dx in range(1, NX):
        forget_x(dx).start()
    w_from_z(0, 5, nz)
    w_from_x(0, 5)
    landed(forget_all.at[:, pl.ds(0, NX - 1), 0], fx_recv.at[0])
    forget_twin(c).start()
    w_from_x(5, nz)
    landed(normed.at[pl.ds(0, n_tp - 1)], tok_recv.at[0])
    tokens_here = normed[...].reshape(block, model)
    forget_twin(other).wait_recv()
    forget_rows = jnp.concatenate(
        [
            forget_all[i // plane_blocks, (i // NC) % NX, i % NC][:, :w_rows]
            for i in range(nz * plane_blocks)
        ],
        axis=1,
    )
    forget_rows = jnp.concatenate(
        [forget_rows, jnp.zeros((8 - heads, model), F32)], axis=0
    ).astype(BF16)
    logits = lax.dot_general(
        forget_rows, tokens_here, CONTRACT_LAST, preferred_element_type=F32
    )
    head_row = lax.broadcasted_iota(jnp.int32, (8, block), 0)
    offsets = jnp.zeros((8, block), F32)
    for h in range(heads):
        offsets = jnp.where(head_row == h, offset_ref[h], offsets)
    n_tokens = nz * plane_blocks * block
    logits = logits + offsets + jnp.log(jnp.full((8, block), n_tokens, F32))
    log_gates = jnp.minimum(logits, 0.0) - jnp.log1p(jnp.exp(-jnp.abs(logits)))
    row_at = lax.broadcasted_iota(jnp.int32, (block, block), 0)
    col_at = lax.broadcasted_iota(jnp.int32, (block, block), 1)
    cum_here = jnp.dot(
        log_gates, jnp.where(row_at <= col_at, 1.0, 0.0).astype(F32),
        precision=lax.Precision.HIGHEST, preferred_element_type=F32,
    )
    for h in range(heads):
        gates_send[h] = cum_here[h : h + 1, :]
    gates_all[z, x, c] = gates_send[x]

    def gate_x(dx):
        hx = wrap(x + dx, NX)
        return remote(
            gates_send.at[hx], gates_all.at[z, x, c], gx_send.at[0], gx_recv.at[0],
            z, hx, c, tp,
        )

    for dx in range(1, NX):
        gate_x(dx).start()

    w_from_twin(0)

    def project(ref, i):
        columns = ref[:, :, :, :, i * width : (i + 1) * width].reshape(model, width)
        return jnp.dot(tokens_here, columns, preferred_element_type=F32)

    lane_at = lax.broadcasted_iota(jnp.int32, (half, LANES), 1)
    keys = project(w_kv, 0)
    values_t = project(w_kv, 1).T.astype(BF16)
    for h in range(heads):
        tile = keys[:, (h // 2) * LANES : (h // 2 + 1) * LANES]
        first, second = tile[:half], tile[half:]
        if h % 2 == 0:
            second = pltpu.roll(second, HEAD_DIM, axis=1)
        else:
            first = pltpu.roll(first, HEAD_DIM, axis=1)
        kv_send[h, :half, :] = jnp.where(lane_at < HEAD_DIM, first, second).astype(BF16)
        value_rows = values_t[h * HEAD_DIM : (h + 1) * HEAD_DIM]
        kv_send[h, half : half + HEAD_DIM, :] = value_rows[:, :half]
        kv_send[h, half + HEAD_DIM :, :] = value_rows[:, half:]

    def kv_x(dx):
        hx = wrap(x + dx, NX)
        return remote(
            kv_send.at[hx], kv_all.at[z, x, c], kx_send.at[0], kx_recv.at[dx - 1],
            z, hx, c, tp,
        )

    for dx in range(1, NX):
        kv_x(dx).start()
    kv_all[z, x, c] = kv_send[x]

    def ring_enter(sub):
        for way in both:
            pl.when(sends(way, 1, sub))(
                lambda way=way: ring_hop(kv_all, kz_send, kz_recv, way, 1, sub).start()
            )
        twin(kv_all, kd_send, kd_recv, 0, 0, sub).start()

    ring_enter(0)

    def ring_poll(way, step, sub):
        @pl.when(receives(way, step, sub))
        def _():
            ring_wait(kv_all, kz_send, kz_recv, way, step, sub)

            @pl.when(sends(way, step + 1, sub))
            def _():
                ring_hop(kv_all, kz_send, kz_recv, way, step + 1, sub).start()

            @pl.when(reads(way, step))
            def _():
                twin(kv_all, kd_send, kd_recv, way, step, sub).start()

    def first_sub(step):
        for way in both:
            ring_poll(way, step, 0)

    @pl.loop(1, nz)
    def _(n):
        k = nearest(n)
        landed(w_q.at[0, :, c], wz_recv.at[1, k])
        w_twin(1, k).start()

    w_from_twin(1)
    queries_t = (project(w_q, 0).astype(BF16).astype(F32) * HEAD_DIM ** (-0.5)).T.astype(BF16)
    for h in range(heads):
        q_send[h] = queries_t[h * HEAD_DIM : (h + 1) * HEAD_DIM]

    def q_x(dx):
        hx = wrap(x + dx, NX)
        return remote(
            q_send.at[hx], q_recv.at[x], qx_send.at[0], qx_recv.at[0], z, hx, c, tp
        )

    for dx in range(1, NX):
        q_x(dx).start()
    q_recv[x] = q_send[x]

    landed(gates_all.at[0, pl.ds(0, NX - 1), 0], gx_recv.at[0])

    def gate_z(k):
        cc = c if k % NC == 0 else other
        place = gates_all.at[z, :, c]
        group = min(k - 1, 1)
        return remote(
            place, place, gz_send.at[group], gz_recv.at[group],
            wrap(z + k // NC, nz), x, cc, tp,
        )

    for k in range(1, nz * NC):
        gate_z(k).start()

    first_sub(1)
    for sub in (1, 3, 2):
        dx = NX - sub
        landed(kv_all.at[z, wrap(x + sub, NX), c], kx_recv.at[dx - 1])
        ring_enter(sub)

    landed(q_recv.at[pl.ds(0, NX - 1)], qx_recv.at[0])
    landed(wo_all.at[0, pl.ds(0, nz - 1), 0, 0], oz_recv.at[0])
    for dx in range(1, NX):
        wo_x(dx).start()
    ones_at = lax.broadcasted_iota(jnp.int32, (LANES, block), 0)
    no_rows = jnp.zeros((HEAD_DIM, block), BF16)
    for side in (0, 1):
        picks = ((ones_at // 8) % 2 == side) & (ones_at < 6 * 8)
        picks = jnp.where(picks, 1.0, 0.0).astype(BF16)
        for i in range(NX):
            parts = [q_recv[i], no_rows] if side == 0 else [no_rows, q_recv[i]]
            q_rhs[i, side] = jnp.concatenate(parts + [picks], axis=0)

    landed(gates_all.at[0, :, 0], gz_recv.at[0])
    landed(gates_all.at[pl.ds(0, nz - 1), :, :], gz_recv.at[1])

    n_blocks = nz * plane_blocks
    gate_rows = gates_all[...].reshape(n_blocks, block)
    mine = z * plane_blocks
    row_block = lax.broadcasted_iota(jnp.int32, (n_blocks, n_blocks), 0)
    col_block = lax.broadcasted_iota(jnp.int32, (n_blocks, n_blocks), 1)
    behind = (col_block >= row_block) & (col_block < mine)
    ahead = (col_block < row_block) & (col_block >= mine)
    steps_between = jnp.where(ahead, 1.0, 0.0) - jnp.where(behind, 1.0, 0.0)
    starts = jnp.dot(
        steps_between, gate_rows[:, half:], precision=lax.Precision.HIGHEST,
        preferred_element_type=F32,
    )[:, half - 1 :]
    bias = -(starts + gate_rows)
    bias_high = bias.astype(BF16).astype(F32)
    bias_rest = bias - bias_high
    bias_mid = bias_rest.astype(BF16).astype(F32)
    bias_low = bias_rest - bias_mid
    no_bias = jnp.zeros((LANES - 6 * plane_blocks, LANES), F32)
    for zz in range(nz):
        here = slice(zz * plane_blocks, (zz + 1) * plane_blocks)
        stack = []
        for part in (bias_high, bias_mid, bias_low):
            stack += [part[here, :half], part[here, half:]]
        bias_all[zz] = jnp.concatenate(stack + [no_bias], axis=0).T.astype(BF16)

    lane_block = lax.broadcasted_iota(jnp.int32, (8, LANES), 1) % 8
    ones_rows = jnp.ones((16, CHUNK * half), BF16)

    def attend(plane, own, core=None):
        if core is None:
            blocks = [(b // NC, b % NC) for b in range(plane_blocks)]
            key_rows = kv_all[plane, :, :, :half, :].reshape(plane_blocks * half, LANES)
        else:
            blocks = [(b, core) for b in range(NX)]
            key_rows = kv_all[plane, :, core, :half, :].reshape(NX * half, LANES)
        bias_cols = bias_all[plane]
        masks = [
            jnp.where(lane_block == xx * NC + cc, 1.0, 0.0)[:1].astype(BF16)
            for xx, cc in blocks
        ]
        bias_tiles = jnp.concatenate([bias_cols * mask for mask in masks], axis=0)
        key_side[: len(blocks) * half, :] = jnp.concatenate([key_rows, bias_tiles], axis=1)

        def score(i, side, b0):
            span = slice(b0 * half, (b0 + CHUNK) * half)
            s = jnp.dot(key_side[span, :], q_rhs[i, side], preferred_element_type=F32)
            if own and b0 == i * NC:
                row = lax.broadcasted_iota(jnp.int32, s.shape, 0)
                key_at = (b0 + row // half) * block + side * half + row % half
                query_at = lax.broadcasted_iota(jnp.int32, s.shape, 1) + (
                    (i * NC + c) * block
                )
                s = jnp.where(key_at <= query_at, s, -1e30)
            scores[i, side, span, :] = s
            return jnp.max(s, axis=0, keepdims=True)

        def absorb(i, side, b0, top):
            if own and side == 0 and b0 == 0:
                total = jnp.zeros((HEAD_DIM + 16, block), F32)
            else:
                old = run_max[i]
                top = jnp.maximum(old, top)
                total = run_acc[i] * jnp.exp(old - top)
            run_max[i] = top
            span = slice(b0 * half, (b0 + CHUNK) * half)
            weights = jnp.exp(scores[i, side, span, :] - top).astype(BF16)
            lo = half + side * HEAD_DIM
            value_cols = jnp.concatenate(
                [
                    kv_all[plane, xx, cc, lo : lo + HEAD_DIM, :]
                    for xx, cc in blocks[b0 : b0 + CHUNK]
                ],
                axis=1,
            )
            value_cols = jnp.concatenate([value_cols, ones_rows], axis=0)
            run_acc[i] = total + jnp.dot(value_cols, weights, preferred_element_type=F32)

        chunks = [
            (i, side, b0)
            for side in (0, 1) for b0 in range(0, len(blocks), CHUNK) for i in range(NX)
            if not own or b0 <= i * NC
        ]
        tops = []
        for n in range(len(chunks) + LAG):
            if n < len(chunks):
                tops.append(score(*chunks[n]))
            if n >= LAG:
                absorb(*chunks[n - LAG], tops[n - LAG])

    landed(kv_all.at[z, :, other], kd_recv.at[0, 0])
    attend(z, True)
    first_sub(2)

    def wo_along_y():
        landed(wo_all.at[tp, :, pl.ds(0, NX - 1), c], ox_recv.at[0])
        for dy in range(1, n_tp):
            wo_y(dy).start()
        wo_twin(0).start()

    def kv_step(step, subs):
        for sub in subs:
            for way in both:
                ring_poll(way, step, sub)

    def twin_step(step):
        for way in both:

            @pl.when(reads(way, step) & (step < far))
            def _():
                landed(kv_all.at[plane_at(way, step), :, other], kd_recv.at[way, step])

            @pl.when(reads(way, step) & (step == far))
            def _():
                landed(
                    kv_all.at[plane_at(way, step), pl.ds(0, NX // 2), other],
                    kd_recv.at[way, step],
                )

    def maybe_attend(plane, extra, core=None):
        @pl.when((plane < z) & extra)
        def _():
            attend(plane, False, core)

    @pl.loop(1, far + 1)
    def _(step):
        kv_step(step, (1,))
        pl.when(step == 2)(lambda: first_sub(3))
        pl.when(step == 2)(wo_along_y)
        pl.when(step == 3)(lambda: first_sub(4))
        maybe_attend(plane_at(1, step - 1), step > 1)
        kv_step(step, (2, 3))

        @pl.loop(0, NC)
        def _(part):
            pl.when(part == 1)(lambda: twin_step(step))
            maybe_attend(plane_at(0, step), True, lax.rem(c + part, NC))


    my_head = tp * NX + x
    quarter = rows // 2
    low_lane = lax.broadcasted_iota(jnp.int32, (quarter, LANES), 1) < HEAD_DIM

    def att_copy(rel, dy):
        i, yy = wrap(x + rel, NX), wrap(tp + dy, n_tp)
        return remote(
            att_send.at[i, yy], att_recv.at[my_head], at_send.at[0],
            at_recv.at[0], z, i, c, yy,
        )

    for rel in (2, 1, 3, 0):
        i = wrap(x + rel, NX)
        acc = run_acc[i]
        att = acc[:HEAD_DIM] / acc[HEAD_DIM : HEAD_DIM + 1]
        att = jnp.concatenate([att, att], axis=0).T
        for y in range(n_tp):
            first = att[y * rows : y * rows + quarter]
            second = att[y * rows + quarter : (y + 1) * rows]
            att_send[i, y] = jnp.where(low_lane, first, second).astype(BF16)
        for dy in (2, 1, 3, 0):
            if rel or dy:
                att_copy(rel, dy).start()
    att_recv[my_head] = att_send[x, tp]
    landed(wo_all.at[pl.ds(0, n_tp - 1), :, :, c], oy_recv.at[0])
    for dy in range(1, n_tp):
        wo_twin(dy).start()

    landed(wo_all.at[:, :, :, other], od_recv.at[0])
    landed(att_recv.at[pl.ds(0, NX * n_tp - 1)], at_recv.at[0])

    projected = jnp.zeros((rows, model), F32)
    for y in range(n_tp):
        pieces = []
        for pair in range(NX // 2):
            even = att_recv[y * NX + 2 * pair].astype(F32)
            odd = att_recv[y * NX + 2 * pair + 1].astype(F32)
            first = jnp.where(low_lane, even, pltpu.roll(odd, HEAD_DIM, axis=1))
            second = jnp.where(low_lane, pltpu.roll(even, HEAD_DIM, axis=1), odd)
            pieces.append(jnp.concatenate([first, second], axis=0).astype(BF16))
        columns = jnp.concatenate(pieces, axis=1)
        projected = projected + lax.dot_general(
            columns, wo_all[y].reshape(model, width), CONTRACT_LAST, preferred_element_type=F32
        )
    out_ref[...] = rms_norm(projected, out_gain_ref[...])

    left(w_kv.at[pl.ds(0, nz - 1), 0, 0], wz_send.at[0])
    left(w_kv.at[:, pl.ds(0, NX - 1), 0], wx_send.at[0])
    left(w_q.at[pl.ds(0, nz - 1), :, 0], wz_send.at[1])
    left(w_q.at[0, pl.ds(0, NX - 1), 0], wx_send.at[1])
    for a in (0, 1):
        left(weights[a].at[:, :, c], wd_send.at[a])
    left(normed.at[pl.ds(0, n_tp - 1)], tok_send.at[0])
    left(forget_all.at[pl.ds(0, nz - 1), 0, 0], fz_send.at[0])
    left(forget_all.at[:, pl.ds(0, NX - 1), 0], fx_send.at[0])
    forget_twin(c).wait_send()
    left(wo_all.at[0, pl.ds(0, nz - 1), 0, 0], oz_send.at[0])
    left(wo_all.at[0, :, pl.ds(0, NX - 1), 0], ox_send.at[0])
    left(wo_all.at[pl.ds(0, n_tp - 1), :, :, 0], oy_send.at[0])
    left(wo_all.at[:, :, :, 0], od_send.at[0])
    left(gates_all.at[0, pl.ds(0, NX - 1), 0], gx_send.at[0])
    left(gates_all.at[0, :, 0], gz_send.at[0])
    left(gates_all.at[pl.ds(0, nz - 1), :, :], gz_send.at[1])
    left(kv_send.at[pl.ds(0, NX - 1)], kx_send.at[0])
    left(q_send.at[pl.ds(0, NX - 1)], qx_send.at[0])
    left(kv_all.at[0, :, 0], kd_send.at[0, 0])
    for way in both:
        for step in range(1, far + 1):
            count = NX if step < far else NX // 2

            @pl.when(reads(way, step))
            def _():
                left(kv_all.at[0, pl.ds(0, count), 0], kd_send.at[way, step])

            for sub in range(NX):
                if step <= steps_of(way, sub):

                    @pl.when(sends(way, step, sub))
                    def _():
                        left(kv_all.at[0, 0, 0], kz_send.at[way, step - 1, sub])
    left(att_recv.at[pl.ds(0, NX * n_tp - 1)], at_send.at[0])


def solution(mesh):
    n_sp, n_tp = mesh.shape["sp"], mesh.shape["tp"]
    nz = n_sp // (NX * NC)

    def on_device(
        tokens, norm_gain, w_query, w_key, w_value, w_forget, forget_offset, w_out_t, out_gain
    ):
        rows, model = tokens.shape
        w_rows, width = w_query.shape
        heads = w_forget.shape[1]
        block = rows * n_tp
        half = block // 2
        far = nz // 2
        vmem = pl.BlockSpec(memory_space=pltpu.VMEM)
        anywhere = pl.BlockSpec(memory_space=pl.ANY)
        dma = pltpu.SemaphoreType.DMA

        def pair(*shape):
            return [dma(shape), dma(shape)]

        return pl.pallas_call(
            functools.partial(layer_kernel, nz, n_tp),
            out_shape=jax.ShapeDtypeStruct((rows, model), BF16),
            in_specs=[
                vmem, vmem, anywhere, anywhere, anywhere, vmem,
                pl.BlockSpec(memory_space=pltpu.SMEM), anywhere, vmem,
            ],
            out_specs=vmem,
            scratch_shapes=[
                pltpu.VMEM((n_tp, rows, model), BF16),
                pltpu.VMEM((nz, NX, NC, w_rows, 2 * width), BF16),
                pltpu.VMEM((nz, NX, NC, w_rows, width), BF16),
                pltpu.VMEM((n_tp, nz, NX, NC, w_rows, width), BF16),
                pltpu.VMEM((nz, NX, NC, heads, LANES), F32),
                pltpu.VMEM((heads, 1, block), F32),
                pltpu.VMEM((nz, NX, NC, 1, block), F32),
                pltpu.VMEM((nz, LANES, LANES), BF16),
                pltpu.VMEM((heads, block, LANES), BF16),
                pltpu.VMEM((nz, NX, NC, block, LANES), BF16),
                pltpu.VMEM((heads, HEAD_DIM, block), BF16),
                pltpu.VMEM((NX, HEAD_DIM, block), BF16),
                pltpu.VMEM((NX, 2, block, block), BF16),
                pltpu.VMEM((NX * NC * half, 2 * LANES), BF16),
                pltpu.VMEM((NX, 2, NX * NC * half, block), F32),
                pltpu.VMEM((NX, 1, block), F32),
                pltpu.VMEM((NX, HEAD_DIM + 16, block), F32),
                pltpu.VMEM((NX, n_tp, rows // 2, LANES), BF16),
                pltpu.VMEM((NX * n_tp, rows // 2, LANES), BF16),
                dma((4,)),
                *pair(1),
                dma((2,)), dma((2, nz)),
                dma((2,)), dma((2, nz)),
                *pair(2),
                *pair(1),
                *pair(1),
                *pair(1),
                *pair(1),
                *pair(1),
                *pair(1),
                *pair(1),
                *pair(1),
                *pair(2),
                dma((1,)), dma((NX - 1,)),
                *pair(1),
                *pair(2, far, NX),
                *pair(2, far + 1),
                *pair(1),
            ],
            compiler_params=pltpu.CompilerParams(collective_id=0, has_side_effects=True),
        )(
            tokens, norm_gain.reshape(1, model), w_query, w_key, w_value, w_forget.T,
            forget_offset, w_out_t, out_gain.reshape(1, model),
        )

    return jax.shard_map(
        on_device,
        mesh=mesh,
        in_specs=(
            P(("sp", "tp"), None),
            P(),
            P("sp", "tp"),
            P("sp", "tp"),
            P("sp", "tp"),
            P("sp", "tp"),
            P("tp"),
            P("sp", "tp"),
            P(),
        ),
        out_specs=P(("sp", "tp"), None),
        check_vma=False,
    )
```

```python
import functools

import jax
import jax.numpy as jnp
from jax import lax
from jax.experimental import pallas as pl
from jax.experimental.pallas import tpu as pltpu
from jax.sharding import PartitionSpec as P

HEAD_DIM = 64
LANES = 128
NORM_EPS = 1e-06
NX, NC = 4, 2
CHUNK, LAG = 2, 8
MESH = pl.DeviceIdType.MESH
F32 = jnp.float32
BF16 = jnp.bfloat16
CONTRACT_LAST = (((1,), (1,)), ((), ()))


def rms_norm(floats, gain_row):
    scale_col = lax.rsqrt(jnp.mean(floats * floats, axis=-1, keepdims=True) + NORM_EPS)
    return (floats * scale_col * gain_row).astype(BF16)


def layer_kernel(
    nz, n_tp,
    tokens_ref, gain_ref, wq_ref, wk_ref, wv_ref, wf_ref, offset_ref, wo_ref, out_gain_ref,
    out_ref,
    normed, w_kv, w_q, wo_all, forget_all, gates_send, gates_all, bias_all,
    kv_send, kv_all, q_send, q_recv, q_rhs, key_side, scores, run_max, run_acc, att_send, att_recv,
    local_sem, tok_send, tok_recv, wz_send, wz_recv, wx_send, wx_recv, wd_send, wd_recv,
    fz_send, fz_recv, fx_send, fx_recv, fd_send, fd_recv,
    oz_send, oz_recv, ox_send, ox_recv, oy_send, oy_recv, od_send, od_recv,
    gx_send, gx_recv, gz_send, gz_recv, kx_send, kx_recv, qx_send, qx_recv,
    kz_send, kz_recv, kd_send, kd_recv, at_send, at_recv,
):
    sp, tp = lax.axis_index("sp"), lax.axis_index("tp")
    z = lax.div(sp, NX * NC)
    x = lax.rem(lax.div(sp, NC), NX)
    c = lax.rem(sp, NC)
    rows = tokens_ref.shape[0]
    block = rows * n_tp
    half = block // 2
    model = tokens_ref.shape[1]
    width = wq_ref.shape[1]
    heads = NX
    plane_blocks = NX * NC
    far = nz // 2

    def wrap(value, size):
        return lax.rem(value + size, size)

    def at(zz, xx, cc):
        return (zz * NX + xx) * NC + cc

    def remote(src, dst, send, recv, zz, xx, cc, yy):
        return pltpu.make_async_remote_copy(
            src_ref=src, dst_ref=dst, send_sem=send, recv_sem=recv,
            device_id=(at(zz, xx, cc), yy), device_id_type=MESH,
        )

    def landed(view, sem):
        remote(view, view, sem, sem, z, x, 1 - c, tp).wait_recv()

    def left(view, sem):
        remote(view, view, sem, sem, z, x, 1 - c, tp).wait_send()

    up, down = wrap(z + 1, nz), wrap(z - 1, nz)
    other = 1 - c

    weights = (w_kv, w_q)
    local = [
        pltpu.make_async_copy(
            ref, place.at[z, x, c, :, pl.ds(i * width, width)], local_sem.at[n]
        )
        for n, (ref, place, i) in enumerate(
            ((wk_ref, w_kv, 0), (wv_ref, w_kv, 1), (wq_ref, w_q, 0))
        )
    ]
    local.append(pltpu.make_async_copy(wo_ref, wo_all.at[tp, z, x, c], local_sem.at[3]))
    for copy in local:
        copy.start()

    barrier = pltpu.get_barrier_semaphore()
    near = [(at(z, wrap(x + dx, NX), c), tp) for dx in range(1, NX)]
    near += [(sp, wrap(tp + dy, n_tp)) for dy in range(1, n_tp)]
    near += [(at(wrap(z + dz, nz), x, c), tp) for dz in range(1, nz)]
    near += [(at(z, x, other), tp)]
    for device in near:
        pl.semaphore_signal(barrier, inc=1, device_id_type=MESH, device_id=device)

    w_rows = wf_ref.shape[1]
    forget_all[z, x, c] = jnp.concatenate(
        [wf_ref[...].astype(F32), jnp.zeros((heads, LANES - w_rows), F32)], axis=1
    )
    normed[tp] = rms_norm(tokens_ref[...].astype(F32), gain_ref[...])
    for copy in local:
        copy.wait()
    pl.semaphore_wait(barrier, len(near))

    def w_place(a, k, dx, core):
        return weights[a].at[wrap(z - k, nz), wrap(x + dx, NX), core]

    def w_z(a, k):
        place = w_place(a, 0, 0, c)
        return remote(
            place, place, wz_send.at[a], wz_recv.at[a, k], wrap(z + k, nz), x, c, tp
        )

    def w_x(a, k, dx):
        place = w_place(a, k, 0, c)
        return remote(
            place, place, wx_send.at[a], wx_recv.at[a, k],
            z, wrap(x + dx, NX), c, tp,
        )

    def w_twin(a, k):
        place = weights[a].at[wrap(z - k, nz), :, c]
        return remote(place, place, wd_send.at[a], wd_recv.at[a], z, x, other, tp)

    def w_group_z(k):
        place = w_q.at[z, :, c]
        return remote(
            place, place, wz_send.at[1], wz_recv.at[1, k], wrap(z + k, nz), x, c, tp
        )

    def w_onward(a, k):
        for dx in (2, 1, 3):
            w_x(a, k, dx).start()

    def nearest(n):
        return jnp.where(lax.rem(n, 2) == 1, lax.div(n + 1, 2), nz - lax.div(n, 2))

    def w_from_z(a, first, last):
        @pl.loop(first, last)
        def _(n):
            k = nearest(n)
            landed(w_place(a, k, 0, c), wz_recv.at[a, k])
            w_onward(a, k)

    def w_from_x(first, last):
        @pl.loop(first, last)
        def _(n):
            k = jnp.where(n == 0, 0, nearest(n))
            landed(w_kv.at[0, pl.ds(0, NX - 1), c], wx_recv.at[0, k])
            w_twin(0, k).start()

    def w_from_twin(a):
        landed(weights[a].at[:, :, other], wd_recv.at[a])

    def plane_at(way, step):
        return wrap(z - step, nz) if way == 0 else wrap(z + step, nz)

    def steps_of(way, sub):
        return far if (sub < NX // 2) == (way == 0) else far - 1

    def sends(way, step, sub):
        inside = step <= steps_of(way, sub)
        if way == 0:
            return inside & (z >= step - 1) & (z < nz - 1)
        return inside & (wrap(z + step - 1, nz) < steps_of(way, sub))

    def receives(way, step, sub):
        inside = step <= steps_of(way, sub)
        if way == 0:
            return inside & (z >= step)
        return inside & (wrap(z + step, nz) < steps_of(way, sub))

    def reads(way, step):
        return z >= step if way == 0 else z + step >= nz

    def ring_hop(ref, send, recv, way, step, sub):
        place = ref.at[plane_at(way, step - 1), wrap(x + sub, NX), c]
        return remote(
            place, place, send.at[way, step - 1, sub], recv.at[way, step - 1, sub],
            (up, down)[way], x, c, tp,
        )

    def ring_wait(ref, send, recv, way, step, sub):
        landed(
            ref.at[plane_at(way, step), wrap(x + sub, NX), c], recv.at[way, step - 1, sub]
        )

    def twin(ref, send, recv, way, step, sub):
        place = ref.at[plane_at(way, step), wrap(x + sub, NX), c]
        return remote(place, place, send.at[way, step], recv.at[way, step], z, x, other, tp)

    def tok_copy(dy):
        return remote(
            normed.at[tp], normed.at[tp], tok_send.at[0], tok_recv.at[0],
            z, x, c, wrap(tp + dy, n_tp),
        )

    def forget_z(k):
        place = forget_all.at[z, x, c]
        return remote(
            place, place, fz_send.at[0], fz_recv.at[0], wrap(z + k, nz), x, c, tp
        )

    def forget_x(dx):
        place = forget_all.at[:, x, c]
        return remote(
            place, place, fx_send.at[0], fx_recv.at[0], z, wrap(x + dx, NX), c, tp
        )

    def forget_twin(core):
        place = forget_all.at[:, :, core]
        return remote(place, place, fd_send.at[0], fd_recv.at[0], z, x, other, tp)

    def wo_z(k):
        place = wo_all.at[tp, z, x, c]
        return remote(
            place, place, oz_send.at[0], oz_recv.at[0], wrap(z + k, nz), x, c, tp
        )

    def wo_x(dx):
        place = wo_all.at[tp, :, x, c]
        return remote(
            place, place, ox_send.at[0], ox_recv.at[0], z, wrap(x + dx, NX), c, tp
        )

    def wo_y(dy):
        place = wo_all.at[tp, :, :, c]
        return remote(
            place, place, oy_send.at[0], oy_recv.at[0], z, x, c, wrap(tp + dy, n_tp)
        )

    def wo_twin(dy):
        place = wo_all.at[wrap(tp + dy, n_tp), :, :, c]
        return remote(place, place, od_send.at[0], od_recv.at[0], z, x, other, tp)

    both = (0, 1)
    far_first = sorted(range(1, nz), key=lambda k: -min(k, nz - k))
    for k in far_first:
        forget_z(k).start()
    for k in far_first:
        w_z(0, k).start()
    for dx in (2, 1, 3):
        w_x(1, 0, dx).start()
    for dy in range(1, n_tp):
        tok_copy(dy).start()

    w_onward(0, 0)
    w_from_z(0, 1, 3)
    landed(w_q.at[0, pl.ds(0, NX - 1), c], wx_recv.at[1, 0])
    for k in far_first:
        w_group_z(k).start()
    for k in far_first:
        wo_z(k).start()
    w_twin(1, 0).start()
    w_from_z(0, 3, 5)
    landed(forget_all.at[pl.ds(0, nz - 1), 0, 0], fz_recv.at[0])
    for dx in range(1, NX):
        forget_x(dx).start()
    w_from_z(0, 5, nz)
    w_from_x(0, 5)
    landed(forget_all.at[:, pl.ds(0, NX - 1), 0], fx_recv.at[0])
    forget_twin(c).start()
    w_from_x(5, nz)
    landed(normed.at[pl.ds(0, n_tp - 1)], tok_recv.at[0])
    tokens_here = normed[...].reshape(block, model)
    forget_twin(other).wait_recv()
    forget_rows = jnp.concatenate(
        [
            forget_all[i // plane_blocks, (i // NC) % NX, i % NC][:, :w_rows]
            for i in range(nz * plane_blocks)
        ],
        axis=1,
    )
    forget_rows = jnp.concatenate(
        [forget_rows, jnp.zeros((8 - heads, model), F32)], axis=0
    ).astype(BF16)
    logits = lax.dot_general(
        forget_rows, tokens_here, CONTRACT_LAST, preferred_element_type=F32
    )
    head_row = lax.broadcasted_iota(jnp.int32, (8, block), 0)
    offsets = jnp.zeros((8, block), F32)
    for h in range(heads):
        offsets = jnp.where(head_row == h, offset_ref[h], offsets)
    n_tokens = nz * plane_blocks * block
    logits = logits + offsets + jnp.log(jnp.full((8, block), n_tokens, F32))
    log_gates = jnp.minimum(logits, 0.0) - jnp.log1p(jnp.exp(-jnp.abs(logits)))
    row_at = lax.broadcasted_iota(jnp.int32, (block, block), 0)
    col_at = lax.broadcasted_iota(jnp.int32, (block, block), 1)
    cum_here = jnp.dot(
        log_gates, jnp.where(row_at <= col_at, 1.0, 0.0).astype(F32),
        precision=lax.Precision.HIGHEST, preferred_element_type=F32,
    )
    for h in range(heads):
        gates_send[h] = cum_here[h : h + 1, :]
    gates_all[z, x, c] = gates_send[x]

    def gate_x(dx):
        hx = wrap(x + dx, NX)
        return remote(
            gates_send.at[hx], gates_all.at[z, x, c], gx_send.at[0], gx_recv.at[0],
            z, hx, c, tp,
        )

    for dx in range(1, NX):
        gate_x(dx).start()

    w_from_twin(0)

    def project(ref, i):
        columns = ref[:, :, :, :, i * width : (i + 1) * width].reshape(model, width)
        return jnp.dot(tokens_here, columns, preferred_element_type=F32)

    lane_at = lax.broadcasted_iota(jnp.int32, (half, LANES), 1)
    keys = project(w_kv, 0)
    values_t = project(w_kv, 1).T.astype(BF16)
    for h in range(heads):
        tile = keys[:, (h // 2) * LANES : (h // 2 + 1) * LANES]
        first, second = tile[:half], tile[half:]
        if h % 2 == 0:
            second = pltpu.roll(second, HEAD_DIM, axis=1)
        else:
            first = pltpu.roll(first, HEAD_DIM, axis=1)
        kv_send[h, :half, :] = jnp.where(lane_at < HEAD_DIM, first, second).astype(BF16)
        value_rows = values_t[h * HEAD_DIM : (h + 1) * HEAD_DIM]
        kv_send[h, half : half + HEAD_DIM, :] = value_rows[:, :half]
        kv_send[h, half + HEAD_DIM :, :] = value_rows[:, half:]

    def kv_x(dx):
        hx = wrap(x + dx, NX)
        return remote(
            kv_send.at[hx], kv_all.at[z, x, c], kx_send.at[0], kx_recv.at[dx - 1],
            z, hx, c, tp,
        )

    for dx in range(1, NX):
        kv_x(dx).start()
    kv_all[z, x, c] = kv_send[x]

    def ring_enter(sub):
        for way in both:
            pl.when(sends(way, 1, sub))(
                lambda way=way: ring_hop(kv_all, kz_send, kz_recv, way, 1, sub).start()
            )
        twin(kv_all, kd_send, kd_recv, 0, 0, sub).start()

    ring_enter(0)

    def ring_poll(way, step, sub):
        @pl.when(receives(way, step, sub))
        def _():
            ring_wait(kv_all, kz_send, kz_recv, way, step, sub)

            @pl.when(sends(way, step + 1, sub))
            def _():
                ring_hop(kv_all, kz_send, kz_recv, way, step + 1, sub).start()

            @pl.when(reads(way, step))
            def _():
                twin(kv_all, kd_send, kd_recv, way, step, sub).start()

    def first_sub(step):
        for way in both:
            ring_poll(way, step, 0)

    @pl.loop(1, nz)
    def _(n):
        k = nearest(n)
        landed(w_q.at[0, :, c], wz_recv.at[1, k])
        w_twin(1, k).start()

    w_from_twin(1)
    queries_t = (project(w_q, 0).astype(BF16).astype(F32) * HEAD_DIM ** (-0.5)).T.astype(BF16)
    for h in range(heads):
        q_send[h] = queries_t[h * HEAD_DIM : (h + 1) * HEAD_DIM]

    def q_x(dx):
        hx = wrap(x + dx, NX)
        return remote(
            q_send.at[hx], q_recv.at[x], qx_send.at[0], qx_recv.at[0], z, hx, c, tp
        )

    for dx in range(1, NX):
        q_x(dx).start()
    q_recv[x] = q_send[x]

    landed(gates_all.at[0, pl.ds(0, NX - 1), 0], gx_recv.at[0])

    def gate_z(k):
        cc = c if k % NC == 0 else other
        place = gates_all.at[z, :, c]
        group = min(k - 1, 1)
        return remote(
            place, place, gz_send.at[group], gz_recv.at[group],
            wrap(z + k // NC, nz), x, cc, tp,
        )

    for k in range(1, nz * NC):
        gate_z(k).start()

    first_sub(1)
    for sub in (1, 3, 2):
        dx = NX - sub
        landed(kv_all.at[z, wrap(x + sub, NX), c], kx_recv.at[dx - 1])
        ring_enter(sub)

    landed(q_recv.at[pl.ds(0, NX - 1)], qx_recv.at[0])
    landed(wo_all.at[0, pl.ds(0, nz - 1), 0, 0], oz_recv.at[0])
    for dx in range(1, NX):
        wo_x(dx).start()
    ones_at = lax.broadcasted_iota(jnp.int32, (LANES, block), 0)
    no_rows = jnp.zeros((HEAD_DIM, block), BF16)
    for side in (0, 1):
        picks = ((ones_at // 8) % 2 == side) & (ones_at < 6 * 8)
        picks = jnp.where(picks, 1.0, 0.0).astype(BF16)
        for i in range(NX):
            parts = [q_recv[i], no_rows] if side == 0 else [no_rows, q_recv[i]]
            q_rhs[i, side] = jnp.concatenate(parts + [picks], axis=0)

    landed(gates_all.at[0, :, 0], gz_recv.at[0])
    landed(gates_all.at[pl.ds(0, nz - 1), :, :], gz_recv.at[1])

    n_blocks = nz * plane_blocks
    gate_rows = gates_all[...].reshape(n_blocks, block)
    mine = z * plane_blocks
    row_block = lax.broadcasted_iota(jnp.int32, (n_blocks, n_blocks), 0)
    col_block = lax.broadcasted_iota(jnp.int32, (n_blocks, n_blocks), 1)
    behind = (col_block >= row_block) & (col_block < mine)
    ahead = (col_block < row_block) & (col_block >= mine)
    steps_between = jnp.where(ahead, 1.0, 0.0) - jnp.where(behind, 1.0, 0.0)
    starts = jnp.dot(
        steps_between, gate_rows[:, half:], precision=lax.Precision.HIGHEST,
        preferred_element_type=F32,
    )[:, half - 1 :]
    bias = -(starts + gate_rows)
    bias_high = bias.astype(BF16).astype(F32)
    bias_rest = bias - bias_high
    bias_mid = bias_rest.astype(BF16).astype(F32)
    bias_low = bias_rest - bias_mid
    no_bias = jnp.zeros((LANES - 6 * plane_blocks, LANES), F32)
    for zz in range(nz):
        here = slice(zz * plane_blocks, (zz + 1) * plane_blocks)
        stack = []
        for part in (bias_high, bias_mid, bias_low):
            stack += [part[here, :half], part[here, half:]]
        bias_all[zz] = jnp.concatenate(stack + [no_bias], axis=0).T.astype(BF16)

    lane_block = lax.broadcasted_iota(jnp.int32, (8, LANES), 1) % 8
    ones_rows = jnp.ones((16, CHUNK * half), BF16)

    def attend(plane, own, core=None):
        if core is None:
            blocks = [(b // NC, b % NC) for b in range(plane_blocks)]
            key_rows = kv_all[plane, :, :, :half, :].reshape(plane_blocks * half, LANES)
        else:
            blocks = [(b, core) for b in range(NX)]
            key_rows = kv_all[plane, :, core, :half, :].reshape(NX * half, LANES)
        bias_cols = bias_all[plane]
        masks = [
            jnp.where(lane_block == xx * NC + cc, 1.0, 0.0)[:1].astype(BF16)
            for xx, cc in blocks
        ]
        bias_tiles = jnp.concatenate([bias_cols * mask for mask in masks], axis=0)
        key_side[: len(blocks) * half, :] = jnp.concatenate([key_rows, bias_tiles], axis=1)

        def score(i, side, b0):
            span = slice(b0 * half, (b0 + CHUNK) * half)
            s = jnp.dot(key_side[span, :], q_rhs[i, side], preferred_element_type=F32)
            if own and b0 == i * NC:
                row = lax.broadcasted_iota(jnp.int32, s.shape, 0)
                key_at = (b0 + row // half) * block + side * half + row % half
                query_at = lax.broadcasted_iota(jnp.int32, s.shape, 1) + (
                    (i * NC + c) * block
                )
                s = jnp.where(key_at <= query_at, s, -1e30)
            scores[i, side, span, :] = s
            return jnp.max(s, axis=0, keepdims=True)

        def absorb(i, side, b0, top):
            if own and side == 0 and b0 == 0:
                total = jnp.zeros((HEAD_DIM + 16, block), F32)
            else:
                old = run_max[i]
                top = jnp.maximum(old, top)
                total = run_acc[i] * jnp.exp(old - top)
            run_max[i] = top
            span = slice(b0 * half, (b0 + CHUNK) * half)
            weights = jnp.exp(scores[i, side, span, :] - top).astype(BF16)
            lo = half + side * HEAD_DIM
            value_cols = jnp.concatenate(
                [
                    kv_all[plane, xx, cc, lo : lo + HEAD_DIM, :]
                    for xx, cc in blocks[b0 : b0 + CHUNK]
                ],
                axis=1,
            )
            value_cols = jnp.concatenate([value_cols, ones_rows], axis=0)
            run_acc[i] = total + jnp.dot(value_cols, weights, preferred_element_type=F32)

        chunks = [
            (i, side, b0)
            for side in (0, 1) for b0 in range(0, len(blocks), CHUNK) for i in range(NX)
            if not own or b0 <= i * NC
        ]
        tops = []
        for n in range(len(chunks) + LAG):
            if n < len(chunks):
                tops.append(score(*chunks[n]))
            if n >= LAG:
                absorb(*chunks[n - LAG], tops[n - LAG])

    landed(kv_all.at[z, :, other], kd_recv.at[0, 0])
    attend(z, True)
    first_sub(2)

    def wo_along_y():
        landed(wo_all.at[tp, :, pl.ds(0, NX - 1), c], ox_recv.at[0])
        for dy in range(1, n_tp):
            wo_y(dy).start()
        wo_twin(0).start()

    def kv_step(step, subs):
        for sub in subs:
            for way in both:
                ring_poll(way, step, sub)

    def twin_step(step):
        for way in both:

            @pl.when(reads(way, step) & (step < far))
            def _():
                landed(kv_all.at[plane_at(way, step), :, other], kd_recv.at[way, step])

            @pl.when(reads(way, step) & (step == far))
            def _():
                landed(
                    kv_all.at[plane_at(way, step), pl.ds(0, NX // 2), other],
                    kd_recv.at[way, step],
                )

    def maybe_attend(plane, extra, core=None):
        @pl.when((plane < z) & extra)
        def _():
            attend(plane, False, core)

    kv_step(1, (1,))

    @pl.loop(1, far + 1)
    def _(step):
        kv_step(step, (2,))
        pl.when(step == 2)(lambda: first_sub(3))
        pl.when(step == 3)(lambda: first_sub(4))
        maybe_attend(plane_at(1, step - 1), step > 1)
        kv_step(step, (3,))
        pl.when(step == 1)(wo_along_y)

        @pl.loop(0, NC)
        def _(part):
            @pl.when(part == 1)
            def _():
                twin_step(step)
                kv_step(step + 1, (1,))

            maybe_attend(plane_at(0, step), True, lax.rem(c + part, NC))


    my_head = tp * NX + x
    quarter = rows // 2
    low_lane = lax.broadcasted_iota(jnp.int32, (quarter, LANES), 1) < HEAD_DIM

    def att_copy(rel, dy):
        i, yy = wrap(x + rel, NX), wrap(tp + dy, n_tp)
        return remote(
            att_send.at[i, yy], att_recv.at[my_head], at_send.at[0],
            at_recv.at[0], z, i, c, yy,
        )

    for rel in (2, 1, 3, 0):
        i = wrap(x + rel, NX)
        acc = run_acc[i]
        att = acc[:HEAD_DIM] / acc[HEAD_DIM : HEAD_DIM + 1]
        att = jnp.concatenate([att, att], axis=0).T
        for y in range(n_tp):
            first = att[y * rows : y * rows + quarter]
            second = att[y * rows + quarter : (y + 1) * rows]
            att_send[i, y] = jnp.where(low_lane, first, second).astype(BF16)
        for dy in (2, 1, 3, 0):
            if rel or dy:
                att_copy(rel, dy).start()
    att_recv[my_head] = att_send[x, tp]
    landed(wo_all.at[pl.ds(0, n_tp - 1), :, :, c], oy_recv.at[0])
    for dy in range(1, n_tp):
        wo_twin(dy).start()

    landed(wo_all.at[:, :, :, other], od_recv.at[0])
    landed(att_recv.at[pl.ds(0, NX * n_tp - 1)], at_recv.at[0])

    projected = jnp.zeros((rows, model), F32)
    for y in range(n_tp):
        pieces = []
        for pair in range(NX // 2):
            even = att_recv[y * NX + 2 * pair].astype(F32)
            odd = att_recv[y * NX + 2 * pair + 1].astype(F32)
            first = jnp.where(low_lane, even, pltpu.roll(odd, HEAD_DIM, axis=1))
            second = jnp.where(low_lane, pltpu.roll(even, HEAD_DIM, axis=1), odd)
            pieces.append(jnp.concatenate([first, second], axis=0).astype(BF16))
        columns = jnp.concatenate(pieces, axis=1)
        projected = projected + lax.dot_general(
            columns, wo_all[y].reshape(model, width), CONTRACT_LAST, preferred_element_type=F32
        )
    out_ref[...] = rms_norm(projected, out_gain_ref[...])

    left(w_kv.at[pl.ds(0, nz - 1), 0, 0], wz_send.at[0])
    left(w_kv.at[:, pl.ds(0, NX - 1), 0], wx_send.at[0])
    left(w_q.at[pl.ds(0, nz - 1), :, 0], wz_send.at[1])
    left(w_q.at[0, pl.ds(0, NX - 1), 0], wx_send.at[1])
    for a in (0, 1):
        left(weights[a].at[:, :, c], wd_send.at[a])
    left(normed.at[pl.ds(0, n_tp - 1)], tok_send.at[0])
    left(forget_all.at[pl.ds(0, nz - 1), 0, 0], fz_send.at[0])
    left(forget_all.at[:, pl.ds(0, NX - 1), 0], fx_send.at[0])
    forget_twin(c).wait_send()
    left(wo_all.at[0, pl.ds(0, nz - 1), 0, 0], oz_send.at[0])
    left(wo_all.at[0, :, pl.ds(0, NX - 1), 0], ox_send.at[0])
    left(wo_all.at[pl.ds(0, n_tp - 1), :, :, 0], oy_send.at[0])
    left(wo_all.at[:, :, :, 0], od_send.at[0])
    left(gates_all.at[0, pl.ds(0, NX - 1), 0], gx_send.at[0])
    left(gates_all.at[0, :, 0], gz_send.at[0])
    left(gates_all.at[pl.ds(0, nz - 1), :, :], gz_send.at[1])
    left(kv_send.at[pl.ds(0, NX - 1)], kx_send.at[0])
    left(q_send.at[pl.ds(0, NX - 1)], qx_send.at[0])
    left(kv_all.at[0, :, 0], kd_send.at[0, 0])
    for way in both:
        for step in range(1, far + 1):
            count = NX if step < far else NX // 2

            @pl.when(reads(way, step))
            def _():
                left(kv_all.at[0, pl.ds(0, count), 0], kd_send.at[way, step])

            for sub in range(NX):
                if step <= steps_of(way, sub):

                    @pl.when(sends(way, step, sub))
                    def _():
                        left(kv_all.at[0, 0, 0], kz_send.at[way, step - 1, sub])
    left(att_recv.at[pl.ds(0, NX * n_tp - 1)], at_send.at[0])


def solution(mesh):
    n_sp, n_tp = mesh.shape["sp"], mesh.shape["tp"]
    nz = n_sp // (NX * NC)

    def on_device(
        tokens, norm_gain, w_query, w_key, w_value, w_forget, forget_offset, w_out_t, out_gain
    ):
        rows, model = tokens.shape
        w_rows, width = w_query.shape
        heads = w_forget.shape[1]
        block = rows * n_tp
        half = block // 2
        far = nz // 2
        vmem = pl.BlockSpec(memory_space=pltpu.VMEM)
        anywhere = pl.BlockSpec(memory_space=pl.ANY)
        dma = pltpu.SemaphoreType.DMA

        def pair(*shape):
            return [dma(shape), dma(shape)]

        return pl.pallas_call(
            functools.partial(layer_kernel, nz, n_tp),
            out_shape=jax.ShapeDtypeStruct((rows, model), BF16),
            in_specs=[
                vmem, vmem, anywhere, anywhere, anywhere, vmem,
                pl.BlockSpec(memory_space=pltpu.SMEM), anywhere, vmem,
            ],
            out_specs=vmem,
            scratch_shapes=[
                pltpu.VMEM((n_tp, rows, model), BF16),
                pltpu.VMEM((nz, NX, NC, w_rows, 2 * width), BF16),
                pltpu.VMEM((nz, NX, NC, w_rows, width), BF16),
                pltpu.VMEM((n_tp, nz, NX, NC, w_rows, width), BF16),
                pltpu.VMEM((nz, NX, NC, heads, LANES), F32),
                pltpu.VMEM((heads, 1, block), F32),
                pltpu.VMEM((nz, NX, NC, 1, block), F32),
                pltpu.VMEM((nz, LANES, LANES), BF16),
                pltpu.VMEM((heads, block, LANES), BF16),
                pltpu.VMEM((nz, NX, NC, block, LANES), BF16),
                pltpu.VMEM((heads, HEAD_DIM, block), BF16),
                pltpu.VMEM((NX, HEAD_DIM, block), BF16),
                pltpu.VMEM((NX, 2, block, block), BF16),
                pltpu.VMEM((NX * NC * half, 2 * LANES), BF16),
                pltpu.VMEM((NX, 2, NX * NC * half, block), F32),
                pltpu.VMEM((NX, 1, block), F32),
                pltpu.VMEM((NX, HEAD_DIM + 16, block), F32),
                pltpu.VMEM((NX, n_tp, rows // 2, LANES), BF16),
                pltpu.VMEM((NX * n_tp, rows // 2, LANES), BF16),
                dma((4,)),
                *pair(1),
                dma((2,)), dma((2, nz)),
                dma((2,)), dma((2, nz)),
                *pair(2),
                *pair(1),
                *pair(1),
                *pair(1),
                *pair(1),
                *pair(1),
                *pair(1),
                *pair(1),
                *pair(1),
                *pair(2),
                dma((1,)), dma((NX - 1,)),
                *pair(1),
                *pair(2, far, NX),
                *pair(2, far + 1),
                *pair(1),
            ],
            compiler_params=pltpu.CompilerParams(collective_id=0, has_side_effects=True),
        )(
            tokens, norm_gain.reshape(1, model), w_query, w_key, w_value, w_forget.T,
            forget_offset, w_out_t, out_gain.reshape(1, model),
        )

    return jax.shard_map(
        on_device,
        mesh=mesh,
        in_specs=(
            P(("sp", "tp"), None),
            P(),
            P("sp", "tp"),
            P("sp", "tp"),
            P("sp", "tp"),
            P("sp", "tp"),
            P("tp"),
            P("sp", "tp"),
            P(),
        ),
        out_specs=P(("sp", "tp"), None),
        check_vma=False,
    )
```

```python
import functools

import jax
import jax.numpy as jnp
from jax import lax
from jax.experimental import pallas as pl
from jax.experimental.pallas import tpu as pltpu
from jax.sharding import PartitionSpec as P

HEAD_DIM = 64
LANES = 128
NORM_EPS = 1e-06
NX, NC = 4, 2
CHUNK, LAG = 2, 8
MESH = pl.DeviceIdType.MESH
F32 = jnp.float32
BF16 = jnp.bfloat16
CONTRACT_LAST = (((1,), (1,)), ((), ()))


def rms_norm(floats, gain_row):
    scale_col = lax.rsqrt(jnp.mean(floats * floats, axis=-1, keepdims=True) + NORM_EPS)
    return (floats * scale_col * gain_row).astype(BF16)


def layer_kernel(
    nz, n_tp,
    tokens_ref, gain_ref, wq_ref, wk_ref, wv_ref, wf_ref, offset_ref, wo_ref, out_gain_ref,
    out_ref,
    normed, w_kv, w_q, wo_all, forget_all, gates_send, gates_all, bias_all,
    kv_send, kv_all, q_send, q_recv, q_rhs, key_side, scores, run_max, run_acc, att_send, att_recv,
    local_sem, tok_send, tok_recv, wz_send, wz_recv, wx_send, wx_recv, wd_send, wd_recv,
    fz_send, fz_recv, fx_send, fx_recv, fd_send, fd_recv,
    oz_send, oz_recv, ox_send, ox_recv, oy_send, oy_recv, od_send, od_recv,
    gx_send, gx_recv, gz_send, gz_recv, kx_send, kx_recv, qx_send, qx_recv,
    kz_send, kz_recv, kd_send, kd_recv, at_send, at_recv,
):
    sp, tp = lax.axis_index("sp"), lax.axis_index("tp")
    z = lax.div(sp, NX * NC)
    x = lax.rem(lax.div(sp, NC), NX)
    c = lax.rem(sp, NC)
    rows = tokens_ref.shape[0]
    block = rows * n_tp
    half = block // 2
    model = tokens_ref.shape[1]
    width = wq_ref.shape[1]
    heads = NX
    plane_blocks = NX * NC
    far = nz // 2

    def wrap(value, size):
        return lax.rem(value + size, size)

    def at(zz, xx, cc):
        return (zz * NX + xx) * NC + cc

    def remote(src, dst, send, recv, zz, xx, cc, yy):
        return pltpu.make_async_remote_copy(
            src_ref=src, dst_ref=dst, send_sem=send, recv_sem=recv,
            device_id=(at(zz, xx, cc), yy), device_id_type=MESH,
        )

    def landed(view, sem):
        remote(view, view, sem, sem, z, x, 1 - c, tp).wait_recv()

    def left(view, sem):
        remote(view, view, sem, sem, z, x, 1 - c, tp).wait_send()

    up, down = wrap(z + 1, nz), wrap(z - 1, nz)
    other = 1 - c

    weights = (w_kv, w_q)
    local = [
        pltpu.make_async_copy(
            ref, place.at[z, x, c, :, pl.ds(i * width, width)], local_sem.at[n]
        )
        for n, (ref, place, i) in enumerate(
            ((wk_ref, w_kv, 0), (wv_ref, w_kv, 1), (wq_ref, w_q, 0))
        )
    ]
    local.append(pltpu.make_async_copy(wo_ref, wo_all.at[tp, z, x, c], local_sem.at[3]))
    for copy in local:
        copy.start()

    barrier = pltpu.get_barrier_semaphore()
    near = [(at(z, wrap(x + dx, NX), c), tp) for dx in range(1, NX)]
    near += [(sp, wrap(tp + dy, n_tp)) for dy in range(1, n_tp)]
    near += [(at(wrap(z + dz, nz), x, c), tp) for dz in range(1, nz)]
    near += [(at(z, x, other), tp)]
    for device in near:
        pl.semaphore_signal(barrier, inc=1, device_id_type=MESH, device_id=device)

    w_rows = wf_ref.shape[1]
    forget_all[z, x, c] = jnp.concatenate(
        [wf_ref[...].astype(F32), jnp.zeros((heads, LANES - w_rows), F32)], axis=1
    )
    normed[tp] = rms_norm(tokens_ref[...].astype(F32), gain_ref[...])
    for copy in local:
        copy.wait()
    pl.semaphore_wait(barrier, len(near))

    def w_place(a, k, dx, core):
        return weights[a].at[wrap(z - k, nz), wrap(x + dx, NX), core]

    def w_z(a, k):
        place = w_place(a, 0, 0, c)
        return remote(
            place, place, wz_send.at[a], wz_recv.at[a, k], wrap(z + k, nz), x, c, tp
        )

    def w_x(a, k, dx):
        place = w_place(a, k, 0, c)
        return remote(
            place, place, wx_send.at[a], wx_recv.at[a, k],
            z, wrap(x + dx, NX), c, tp,
        )

    def w_twin(a, k):
        place = weights[a].at[wrap(z - k, nz), :, c]
        return remote(place, place, wd_send.at[a], wd_recv.at[a], z, x, other, tp)

    def w_group_z(k):
        place = w_q.at[z, :, c]
        return remote(
            place, place, wz_send.at[1], wz_recv.at[1, k], wrap(z + k, nz), x, c, tp
        )

    def w_onward(a, k):
        for dx in (2, 1, 3):
            w_x(a, k, dx).start()

    def nearest(n):
        return jnp.where(lax.rem(n, 2) == 1, lax.div(n + 1, 2), nz - lax.div(n, 2))

    def w_from_z(a, first, last):
        @pl.loop(first, last)
        def _(n):
            k = nearest(n)
            landed(w_place(a, k, 0, c), wz_recv.at[a, k])
            w_onward(a, k)

    def w_from_x(first, last):
        @pl.loop(first, last)
        def _(n):
            k = jnp.where(n == 0, 0, nearest(n))
            landed(w_kv.at[0, pl.ds(0, NX - 1), c], wx_recv.at[0, k])
            w_twin(0, k).start()

    def w_from_twin(a):
        landed(weights[a].at[:, :, other], wd_recv.at[a])

    def plane_at(way, step):
        return wrap(z - step, nz) if way == 0 else wrap(z + step, nz)

    def steps_of(way, sub):
        return far if (sub < NX // 2) == (way == 0) else far - 1

    def sends(way, step, sub):
        inside = step <= steps_of(way, sub)
        if way == 0:
            return inside & (z >= step - 1) & (z < nz - 1)
        return inside & (wrap(z + step - 1, nz) < steps_of(way, sub))

    def receives(way, step, sub):
        inside = step <= steps_of(way, sub)
        if way == 0:
            return inside & (z >= step)
        return inside & (wrap(z + step, nz) < steps_of(way, sub))

    def reads(way, step):
        return z >= step if way == 0 else z + step >= nz

    def ring_hop(ref, send, recv, way, step, sub):
        place = ref.at[plane_at(way, step - 1), wrap(x + sub, NX), c]
        return remote(
            place, place, send.at[way, step - 1, sub], recv.at[way, step - 1, sub],
            (up, down)[way], x, c, tp,
        )

    def ring_wait(ref, send, recv, way, step, sub):
        landed(
            ref.at[plane_at(way, step), wrap(x + sub, NX), c], recv.at[way, step - 1, sub]
        )

    def twin(ref, send, recv, way, step, sub):
        place = ref.at[plane_at(way, step), wrap(x + sub, NX), c]
        return remote(
            place, place, send.at[way, step], recv.at[way, step, sub // 2], z, x, other, tp
        )

    def tok_copy(dy):
        return remote(
            normed.at[tp], normed.at[tp], tok_send.at[0], tok_recv.at[0],
            z, x, c, wrap(tp + dy, n_tp),
        )

    def forget_z(k):
        place = forget_all.at[z, x, c]
        return remote(
            place, place, fz_send.at[0], fz_recv.at[0], wrap(z + k, nz), x, c, tp
        )

    def forget_x(dx):
        place = forget_all.at[:, x, c]
        return remote(
            place, place, fx_send.at[0], fx_recv.at[0], z, wrap(x + dx, NX), c, tp
        )

    def forget_twin(core):
        place = forget_all.at[:, :, core]
        return remote(place, place, fd_send.at[0], fd_recv.at[0], z, x, other, tp)

    def wo_z(k):
        place = wo_all.at[tp, z, x, c]
        return remote(
            place, place, oz_send.at[0], oz_recv.at[0], wrap(z + k, nz), x, c, tp
        )

    def wo_x(dx):
        place = wo_all.at[tp, :, x, c]
        return remote(
            place, place, ox_send.at[0], ox_recv.at[0], z, wrap(x + dx, NX), c, tp
        )

    def wo_y(dy):
        place = wo_all.at[tp, :, :, c]
        return remote(
            place, place, oy_send.at[0], oy_recv.at[0], z, x, c, wrap(tp + dy, n_tp)
        )

    def wo_twin(dy):
        place = wo_all.at[wrap(tp + dy, n_tp), :, :, c]
        return remote(place, place, od_send.at[0], od_recv.at[0], z, x, other, tp)

    both = (0, 1)
    far_first = sorted(range(1, nz), key=lambda k: -min(k, nz - k))
    for k in far_first:
        forget_z(k).start()
    for k in far_first:
        w_z(0, k).start()
    for dx in (2, 1, 3):
        w_x(1, 0, dx).start()
    for dy in range(1, n_tp):
        tok_copy(dy).start()

    w_onward(0, 0)
    w_from_z(0, 1, 3)
    landed(w_q.at[0, pl.ds(0, NX - 1), c], wx_recv.at[1, 0])
    for k in far_first:
        w_group_z(k).start()
    for k in far_first:
        wo_z(k).start()
    w_twin(1, 0).start()
    w_from_z(0, 3, 5)
    landed(forget_all.at[pl.ds(0, nz - 1), 0, 0], fz_recv.at[0])
    for dx in range(1, NX):
        forget_x(dx).start()
    w_from_z(0, 5, nz)
    w_from_x(0, 5)
    landed(forget_all.at[:, pl.ds(0, NX - 1), 0], fx_recv.at[0])
    forget_twin(c).start()
    w_from_x(5, nz)
    landed(normed.at[pl.ds(0, n_tp - 1)], tok_recv.at[0])
    tokens_here = normed[...].reshape(block, model)
    forget_twin(other).wait_recv()
    forget_rows = jnp.concatenate(
        [
            forget_all[i // plane_blocks, (i // NC) % NX, i % NC][:, :w_rows]
            for i in range(nz * plane_blocks)
        ],
        axis=1,
    )
    forget_rows = jnp.concatenate(
        [forget_rows, jnp.zeros((8 - heads, model), F32)], axis=0
    ).astype(BF16)
    logits = lax.dot_general(
        forget_rows, tokens_here, CONTRACT_LAST, preferred_element_type=F32
    )
    head_row = lax.broadcasted_iota(jnp.int32, (8, block), 0)
    offsets = jnp.zeros((8, block), F32)
    for h in range(heads):
        offsets = jnp.where(head_row == h, offset_ref[h], offsets)
    n_tokens = nz * plane_blocks * block
    logits = logits + offsets + jnp.log(jnp.full((8, block), n_tokens, F32))
    log_gates = jnp.minimum(logits, 0.0) - jnp.log1p(jnp.exp(-jnp.abs(logits)))
    row_at = lax.broadcasted_iota(jnp.int32, (block, block), 0)
    col_at = lax.broadcasted_iota(jnp.int32, (block, block), 1)
    cum_here = jnp.dot(
        log_gates, jnp.where(row_at <= col_at, 1.0, 0.0).astype(F32),
        precision=lax.Precision.HIGHEST, preferred_element_type=F32,
    )
    for h in range(heads):
        gates_send[h] = cum_here[h : h + 1, :]
    gates_all[z, x, c] = gates_send[x]

    def gate_x(dx):
        hx = wrap(x + dx, NX)
        return remote(
            gates_send.at[hx], gates_all.at[z, x, c], gx_send.at[0], gx_recv.at[0],
            z, hx, c, tp,
        )

    for dx in range(1, NX):
        gate_x(dx).start()

    w_from_twin(0)

    def project(ref, i):
        columns = ref[:, :, :, :, i * width : (i + 1) * width].reshape(model, width)
        return jnp.dot(tokens_here, columns, preferred_element_type=F32)

    lane_at = lax.broadcasted_iota(jnp.int32, (half, LANES), 1)
    keys = project(w_kv, 0)
    values_t = project(w_kv, 1).T.astype(BF16)
    for h in range(heads):
        tile = keys[:, (h // 2) * LANES : (h // 2 + 1) * LANES]
        first, second = tile[:half], tile[half:]
        if h % 2 == 0:
            second = pltpu.roll(second, HEAD_DIM, axis=1)
        else:
            first = pltpu.roll(first, HEAD_DIM, axis=1)
        kv_send[h, :half, :] = jnp.where(lane_at < HEAD_DIM, first, second).astype(BF16)
        value_rows = values_t[h * HEAD_DIM : (h + 1) * HEAD_DIM]
        kv_send[h, half : half + HEAD_DIM, :] = value_rows[:, :half]
        kv_send[h, half + HEAD_DIM :, :] = value_rows[:, half:]

    def kv_x(dx):
        hx = wrap(x + dx, NX)
        return remote(
            kv_send.at[hx], kv_all.at[z, x, c], kx_send.at[0], kx_recv.at[dx - 1],
            z, hx, c, tp,
        )

    for dx in range(1, NX):
        kv_x(dx).start()
    kv_all[z, x, c] = kv_send[x]

    def ring_enter(sub):
        for way in both:
            pl.when(sends(way, 1, sub))(
                lambda way=way: ring_hop(kv_all, kz_send, kz_recv, way, 1, sub).start()
            )
        twin(kv_all, kd_send, kd_recv, 0, 0, sub).start()

    ring_enter(0)

    def ring_poll(way, step, sub):
        @pl.when(receives(way, step, sub))
        def _():
            ring_wait(kv_all, kz_send, kz_recv, way, step, sub)

            @pl.when(sends(way, step + 1, sub))
            def _():
                ring_hop(kv_all, kz_send, kz_recv, way, step + 1, sub).start()

            @pl.when(reads(way, step))
            def _():
                twin(kv_all, kd_send, kd_recv, way, step, sub).start()

    def first_sub(step):
        for way in both:
            ring_poll(way, step, 0)

    @pl.loop(1, nz)
    def _(n):
        k = nearest(n)
        landed(w_q.at[0, :, c], wz_recv.at[1, k])
        w_twin(1, k).start()

    w_from_twin(1)
    queries_t = (project(w_q, 0).astype(BF16).astype(F32) * HEAD_DIM ** (-0.5)).T.astype(BF16)
    for h in range(heads):
        q_send[h] = queries_t[h * HEAD_DIM : (h + 1) * HEAD_DIM]

    def q_x(dx):
        hx = wrap(x + dx, NX)
        return remote(
            q_send.at[hx], q_recv.at[x], qx_send.at[0], qx_recv.at[0], z, hx, c, tp
        )

    for dx in range(1, NX):
        q_x(dx).start()
    q_recv[x] = q_send[x]

    landed(gates_all.at[0, pl.ds(0, NX - 1), 0], gx_recv.at[0])

    def gate_z(k):
        cc = c if k % NC == 0 else other
        place = gates_all.at[z, :, c]
        group = min(k - 1, 1)
        return remote(
            place, place, gz_send.at[group], gz_recv.at[group],
            wrap(z + k // NC, nz), x, cc, tp,
        )

    for k in range(1, nz * NC):
        gate_z(k).start()

    first_sub(1)
    for sub in (1, 3, 2):
        dx = NX - sub
        landed(kv_all.at[z, wrap(x + sub, NX), c], kx_recv.at[dx - 1])
        ring_enter(sub)

    landed(q_recv.at[pl.ds(0, NX - 1)], qx_recv.at[0])
    landed(wo_all.at[0, pl.ds(0, nz - 1), 0, 0], oz_recv.at[0])
    for dx in range(1, NX):
        wo_x(dx).start()
    ones_at = lax.broadcasted_iota(jnp.int32, (LANES, block), 0)
    no_rows = jnp.zeros((HEAD_DIM, block), BF16)
    for side in (0, 1):
        picks = ((ones_at // 8) % 2 == side) & (ones_at < 6 * 8)
        picks = jnp.where(picks, 1.0, 0.0).astype(BF16)
        for i in range(NX):
            parts = [q_recv[i], no_rows] if side == 0 else [no_rows, q_recv[i]]
            q_rhs[i, side] = jnp.concatenate(parts + [picks], axis=0)

    landed(gates_all.at[0, :, 0], gz_recv.at[0])
    landed(gates_all.at[pl.ds(0, nz - 1), :, :], gz_recv.at[1])

    n_blocks = nz * plane_blocks
    gate_rows = gates_all[...].reshape(n_blocks, block)
    mine = z * plane_blocks
    row_block = lax.broadcasted_iota(jnp.int32, (n_blocks, n_blocks), 0)
    col_block = lax.broadcasted_iota(jnp.int32, (n_blocks, n_blocks), 1)
    behind = (col_block >= row_block) & (col_block < mine)
    ahead = (col_block < row_block) & (col_block >= mine)
    steps_between = jnp.where(ahead, 1.0, 0.0) - jnp.where(behind, 1.0, 0.0)
    starts = jnp.dot(
        steps_between, gate_rows[:, half:], precision=lax.Precision.HIGHEST,
        preferred_element_type=F32,
    )[:, half - 1 :]
    bias = -(starts + gate_rows)
    bias_high = bias.astype(BF16).astype(F32)
    bias_rest = bias - bias_high
    bias_mid = bias_rest.astype(BF16).astype(F32)
    bias_low = bias_rest - bias_mid
    no_bias = jnp.zeros((LANES - 6 * plane_blocks, LANES), F32)
    for zz in range(nz):
        here = slice(zz * plane_blocks, (zz + 1) * plane_blocks)
        stack = []
        for part in (bias_high, bias_mid, bias_low):
            stack += [part[here, :half], part[here, half:]]
        bias_all[zz] = jnp.concatenate(stack + [no_bias], axis=0).T.astype(BF16)

    lane_block = lax.broadcasted_iota(jnp.int32, (8, LANES), 1) % 8
    ones_rows = jnp.ones((16, CHUNK * half), BF16)

    def attend(plane, own, duo=None):
        if duo is None:
            blocks = [(b // NC, b % NC) for b in range(plane_blocks)]
            key_rows = kv_all[plane, :, :, :half, :].reshape(plane_blocks * half, LANES)
        else:
            blocks = [(wrap(x + 2 * duo + d, NX), cc) for d in (0, 1) for cc in range(NC)]
            key_rows = jnp.concatenate(
                [kv_all[plane, xx, cc, :half, :] for xx, cc in blocks], axis=0
            )
        bias_cols = bias_all[plane]
        masks = [
            jnp.where(lane_block == xx * NC + cc, 1.0, 0.0)[:1].astype(BF16)
            for xx, cc in blocks
        ]
        bias_tiles = jnp.concatenate([bias_cols * mask for mask in masks], axis=0)
        key_side[: len(blocks) * half, :] = jnp.concatenate([key_rows, bias_tiles], axis=1)

        def score(i, side, b0):
            span = slice(b0 * half, (b0 + CHUNK) * half)
            s = jnp.dot(key_side[span, :], q_rhs[i, side], preferred_element_type=F32)
            if own and b0 == i * NC:
                row = lax.broadcasted_iota(jnp.int32, s.shape, 0)
                key_at = (b0 + row // half) * block + side * half + row % half
                query_at = lax.broadcasted_iota(jnp.int32, s.shape, 1) + (
                    (i * NC + c) * block
                )
                s = jnp.where(key_at <= query_at, s, -1e30)
            scores[i, side, span, :] = s
            return jnp.max(s, axis=0, keepdims=True)

        def absorb(i, side, b0, top):
            if own and side == 0 and b0 == 0:
                total = jnp.zeros((HEAD_DIM + 16, block), F32)
            else:
                old = run_max[i]
                top = jnp.maximum(old, top)
                total = run_acc[i] * jnp.exp(old - top)
            run_max[i] = top
            span = slice(b0 * half, (b0 + CHUNK) * half)
            weights = jnp.exp(scores[i, side, span, :] - top).astype(BF16)
            lo = half + side * HEAD_DIM
            value_cols = jnp.concatenate(
                [
                    kv_all[plane, xx, cc, lo : lo + HEAD_DIM, :]
                    for xx, cc in blocks[b0 : b0 + CHUNK]
                ],
                axis=1,
            )
            value_cols = jnp.concatenate([value_cols, ones_rows], axis=0)
            run_acc[i] = total + jnp.dot(value_cols, weights, preferred_element_type=F32)

        chunks = [
            (i, side, b0)
            for side in (0, 1) for b0 in range(0, len(blocks), CHUNK) for i in range(NX)
            if not own or b0 <= i * NC
        ]
        tops = []
        for n in range(len(chunks) + LAG):
            if n < len(chunks):
                tops.append(score(*chunks[n]))
            if n >= LAG:
                absorb(*chunks[n - LAG], tops[n - LAG])

    for pair in (0, 1):
        landed(kv_all.at[z, pl.ds(0, NX // 2), other], kd_recv.at[0, 0, pair])
    attend(z, True)
    first_sub(2)

    def wo_along_y():
        landed(wo_all.at[tp, :, pl.ds(0, NX - 1), c], ox_recv.at[0])
        for dy in range(1, n_tp):
            wo_y(dy).start()
        wo_twin(0).start()

    def kv_step(step, subs):
        for sub in subs:
            for way in both:
                ring_poll(way, step, sub)

    def twin_wait(plane, way, step, duo):
        landed(kv_all.at[plane, pl.ds(0, NX // 2), other], kd_recv.at[way, step, duo])

    kv_step(1, (1,))

    @pl.loop(0, 2)
    def _(way):
        plane = jnp.where(way == 0, wrap(z - 1, nz), wrap(z + 1, nz))

        @pl.when(plane < z)
        def _():
            twin_wait(plane, way, 1, 0)
            attend(plane, False, 0)

    @pl.loop(1, far + 1)
    def _(step):
        kv_step(step, (2,))
        pl.when(step == 2)(lambda: kv_step(2, (1,)))
        pl.when(step == 2)(lambda: first_sub(3))
        pl.when(step == 3)(lambda: first_sub(4))
        @pl.when((step > 2) & reads(1, step - 1))
        def _():
            plane = plane_at(1, step - 1)
            for duo in (0, 1):
                twin_wait(plane, 1, step - 1, duo)
            attend(plane, False)

        kv_step(step, (3,))
        pl.when(step == 1)(wo_along_y)

        @pl.loop(jnp.where(step == 1, 1, 0), jnp.where(step == 1, 3, 2))
        def _(part):
            pl.when((part == 1) & (step > 1))(lambda: kv_step(step + 1, (1,)))
            duo = jnp.minimum(part, 1)
            plane = jnp.where(part == 2, wrap(z + 1, nz), wrap(z - step, nz))

            @pl.when(plane < z)
            def _():
                way = jnp.where(step == far, duo, jnp.where(part == 2, 1, 0))
                twin_wait(plane, way, step, duo)
                attend(plane, False, duo)


    my_head = tp * NX + x
    quarter = rows // 2
    low_lane = lax.broadcasted_iota(jnp.int32, (quarter, LANES), 1) < HEAD_DIM

    def att_copy(rel, dy):
        i, yy = wrap(x + rel, NX), wrap(tp + dy, n_tp)
        return remote(
            att_send.at[i, yy], att_recv.at[my_head], at_send.at[0],
            at_recv.at[0], z, i, c, yy,
        )

    for rel in (2, 1, 3, 0):
        i = wrap(x + rel, NX)
        acc = run_acc[i]
        att = acc[:HEAD_DIM] / acc[HEAD_DIM : HEAD_DIM + 1]
        att = jnp.concatenate([att, att], axis=0).T
        for y in range(n_tp):
            first = att[y * rows : y * rows + quarter]
            second = att[y * rows + quarter : (y + 1) * rows]
            att_send[i, y] = jnp.where(low_lane, first, second).astype(BF16)
        for dy in (2, 1, 3, 0):
            if rel or dy:
                att_copy(rel, dy).start()
    att_recv[my_head] = att_send[x, tp]
    landed(wo_all.at[pl.ds(0, n_tp - 1), :, :, c], oy_recv.at[0])
    for dy in range(1, n_tp):
        wo_twin(dy).start()

    landed(wo_all.at[:, :, :, other], od_recv.at[0])
    landed(att_recv.at[pl.ds(0, NX * n_tp - 1)], at_recv.at[0])

    projected = jnp.zeros((rows, model), F32)
    for y in range(n_tp):
        pieces = []
        for pair in range(NX // 2):
            even = att_recv[y * NX + 2 * pair].astype(F32)
            odd = att_recv[y * NX + 2 * pair + 1].astype(F32)
            first = jnp.where(low_lane, even, pltpu.roll(odd, HEAD_DIM, axis=1))
            second = jnp.where(low_lane, pltpu.roll(even, HEAD_DIM, axis=1), odd)
            pieces.append(jnp.concatenate([first, second], axis=0).astype(BF16))
        columns = jnp.concatenate(pieces, axis=1)
        projected = projected + lax.dot_general(
            columns, wo_all[y].reshape(model, width), CONTRACT_LAST, preferred_element_type=F32
        )
    out_ref[...] = rms_norm(projected, out_gain_ref[...])

    left(w_kv.at[pl.ds(0, nz - 1), 0, 0], wz_send.at[0])
    left(w_kv.at[:, pl.ds(0, NX - 1), 0], wx_send.at[0])
    left(w_q.at[pl.ds(0, nz - 1), :, 0], wz_send.at[1])
    left(w_q.at[0, pl.ds(0, NX - 1), 0], wx_send.at[1])
    for a in (0, 1):
        left(weights[a].at[:, :, c], wd_send.at[a])
    left(normed.at[pl.ds(0, n_tp - 1)], tok_send.at[0])
    left(forget_all.at[pl.ds(0, nz - 1), 0, 0], fz_send.at[0])
    left(forget_all.at[:, pl.ds(0, NX - 1), 0], fx_send.at[0])
    forget_twin(c).wait_send()
    left(wo_all.at[0, pl.ds(0, nz - 1), 0, 0], oz_send.at[0])
    left(wo_all.at[0, :, pl.ds(0, NX - 1), 0], ox_send.at[0])
    left(wo_all.at[pl.ds(0, n_tp - 1), :, :, 0], oy_send.at[0])
    left(wo_all.at[:, :, :, 0], od_send.at[0])
    left(gates_all.at[0, pl.ds(0, NX - 1), 0], gx_send.at[0])
    left(gates_all.at[0, :, 0], gz_send.at[0])
    left(gates_all.at[pl.ds(0, nz - 1), :, :], gz_send.at[1])
    left(kv_send.at[pl.ds(0, NX - 1)], kx_send.at[0])
    left(q_send.at[pl.ds(0, NX - 1)], qx_send.at[0])
    left(kv_all.at[0, :, 0], kd_send.at[0, 0])
    for way in both:
        for step in range(1, far + 1):
            count = NX if step < far else NX // 2

            @pl.when(reads(way, step))
            def _():
                left(kv_all.at[0, pl.ds(0, count), 0], kd_send.at[way, step])

            for sub in range(NX):
                if step <= steps_of(way, sub):

                    @pl.when(sends(way, step, sub))
                    def _():
                        left(kv_all.at[0, 0, 0], kz_send.at[way, step - 1, sub])
    left(att_recv.at[pl.ds(0, NX * n_tp - 1)], at_send.at[0])


def solution(mesh):
    n_sp, n_tp = mesh.shape["sp"], mesh.shape["tp"]
    nz = n_sp // (NX * NC)

    def on_device(
        tokens, norm_gain, w_query, w_key, w_value, w_forget, forget_offset, w_out_t, out_gain
    ):
        rows, model = tokens.shape
        w_rows, width = w_query.shape
        heads = w_forget.shape[1]
        block = rows * n_tp
        half = block // 2
        far = nz // 2
        vmem = pl.BlockSpec(memory_space=pltpu.VMEM)
        anywhere = pl.BlockSpec(memory_space=pl.ANY)
        dma = pltpu.SemaphoreType.DMA

        def pair(*shape):
            return [dma(shape), dma(shape)]

        return pl.pallas_call(
            functools.partial(layer_kernel, nz, n_tp),
            out_shape=jax.ShapeDtypeStruct((rows, model), BF16),
            in_specs=[
                vmem, vmem, anywhere, anywhere, anywhere, vmem,
                pl.BlockSpec(memory_space=pltpu.SMEM), anywhere, vmem,
            ],
            out_specs=vmem,
            scratch_shapes=[
                pltpu.VMEM((n_tp, rows, model), BF16),
                pltpu.VMEM((nz, NX, NC, w_rows, 2 * width), BF16),
                pltpu.VMEM((nz, NX, NC, w_rows, width), BF16),
                pltpu.VMEM((n_tp, nz, NX, NC, w_rows, width), BF16),
                pltpu.VMEM((nz, NX, NC, heads, LANES), F32),
                pltpu.VMEM((heads, 1, block), F32),
                pltpu.VMEM((nz, NX, NC, 1, block), F32),
                pltpu.VMEM((nz, LANES, LANES), BF16),
                pltpu.VMEM((heads, block, LANES), BF16),
                pltpu.VMEM((nz, NX, NC, block, LANES), BF16),
                pltpu.VMEM((heads, HEAD_DIM, block), BF16),
                pltpu.VMEM((NX, HEAD_DIM, block), BF16),
                pltpu.VMEM((NX, 2, block, block), BF16),
                pltpu.VMEM((NX * NC * half, 2 * LANES), BF16),
                pltpu.VMEM((NX, 2, NX * NC * half, block), F32),
                pltpu.VMEM((NX, 1, block), F32),
                pltpu.VMEM((NX, HEAD_DIM + 16, block), F32),
                pltpu.VMEM((NX, n_tp, rows // 2, LANES), BF16),
                pltpu.VMEM((NX * n_tp, rows // 2, LANES), BF16),
                dma((4,)),
                *pair(1),
                dma((2,)), dma((2, nz)),
                dma((2,)), dma((2, nz)),
                *pair(2),
                *pair(1),
                *pair(1),
                *pair(1),
                *pair(1),
                *pair(1),
                *pair(1),
                *pair(1),
                *pair(1),
                *pair(2),
                dma((1,)), dma((NX - 1,)),
                *pair(1),
                *pair(2, far, NX),
                dma((2, far + 1)), dma((2, far + 1, 2)),
                *pair(1),
            ],
            compiler_params=pltpu.CompilerParams(collective_id=0, has_side_effects=True),
        )(
            tokens, norm_gain.reshape(1, model), w_query, w_key, w_value, w_forget.T,
            forget_offset, w_out_t, out_gain.reshape(1, model),
        )

    return jax.shard_map(
        on_device,
        mesh=mesh,
        in_specs=(
            P(("sp", "tp"), None),
            P(),
            P("sp", "tp"),
            P("sp", "tp"),
            P("sp", "tp"),
            P("sp", "tp"),
            P("tp"),
            P("sp", "tp"),
            P(),
        ),
        out_specs=P(("sp", "tp"), None),
        check_vma=False,
    )
```

```python
import functools

import jax
import jax.numpy as jnp
from jax import lax
from jax.experimental import pallas as pl
from jax.experimental.pallas import tpu as pltpu
from jax.sharding import PartitionSpec as P

HEAD_DIM = 64
LANES = 128
NORM_EPS = 1e-06
NX, NC = 4, 2
CHUNK, LAG = 2, 8
MESH = pl.DeviceIdType.MESH
F32 = jnp.float32
BF16 = jnp.bfloat16
CONTRACT_LAST = (((1,), (1,)), ((), ()))


def rms_norm(floats, gain_row):
    scale_col = lax.rsqrt(jnp.mean(floats * floats, axis=-1, keepdims=True) + NORM_EPS)
    return (floats * scale_col * gain_row).astype(BF16)


def layer_kernel(
    nz, n_tp,
    tokens_ref, gain_ref, wq_ref, wk_ref, wv_ref, wf_ref, offset_ref, wo_ref, out_gain_ref,
    out_ref,
    normed, w_kv, w_q, wo_all, forget_all, gates_send, gates_all, bias_all,
    kv_send, kv_all, q_send, q_recv, q_rhs, key_side, scores, run_max, run_acc, att_send, att_recv,
    local_sem, tok_send, tok_recv, wz_send, wz_recv, wx_send, wx_recv, wd_send, wd_recv,
    fz_send, fz_recv, fx_send, fx_recv, fd_send, fd_recv,
    oz_send, oz_recv, ox_send, ox_recv, oy_send, oy_recv, od_send, od_recv,
    gx_send, gx_recv, gz_send, gz_recv, kx_send, kx_recv, qx_send, qx_recv,
    kz_send, kz_recv, kd_send, kd_recv, at_send, at_recv,
):
    sp, tp = lax.axis_index("sp"), lax.axis_index("tp")
    z = lax.div(sp, NX * NC)
    x = lax.rem(lax.div(sp, NC), NX)
    c = lax.rem(sp, NC)
    rows = tokens_ref.shape[0]
    block = rows * n_tp
    half = block // 2
    model = tokens_ref.shape[1]
    width = wq_ref.shape[1]
    heads = NX
    plane_blocks = NX * NC
    far = nz // 2

    def wrap(value, size):
        return lax.rem(value + size, size)

    def at(zz, xx, cc):
        return (zz * NX + xx) * NC + cc

    def remote(src, dst, send, recv, zz, xx, cc, yy):
        return pltpu.make_async_remote_copy(
            src_ref=src, dst_ref=dst, send_sem=send, recv_sem=recv,
            device_id=(at(zz, xx, cc), yy), device_id_type=MESH,
        )

    def landed(view, sem):
        remote(view, view, sem, sem, z, x, 1 - c, tp).wait_recv()

    def left(view, sem):
        remote(view, view, sem, sem, z, x, 1 - c, tp).wait_send()

    up, down = wrap(z + 1, nz), wrap(z - 1, nz)
    other = 1 - c

    weights = (w_kv, w_q)
    local = [
        pltpu.make_async_copy(
            ref, place.at[z, x, c, :, pl.ds(i * width, width)], local_sem.at[n]
        )
        for n, (ref, place, i) in enumerate(
            ((wk_ref, w_kv, 0), (wv_ref, w_kv, 1), (wq_ref, w_q, 0))
        )
    ]
    local.append(pltpu.make_async_copy(wo_ref, wo_all.at[tp, z, x, c], local_sem.at[3]))
    for copy in local:
        copy.start()

    barrier = pltpu.get_barrier_semaphore()
    near = [(at(z, wrap(x + dx, NX), c), tp) for dx in range(1, NX)]
    near += [(sp, wrap(tp + dy, n_tp)) for dy in range(1, n_tp)]
    near += [(at(wrap(z + dz, nz), x, c), tp) for dz in range(1, nz)]
    near += [(at(z, x, other), tp)]
    for device in near:
        pl.semaphore_signal(barrier, inc=1, device_id_type=MESH, device_id=device)

    w_rows = wf_ref.shape[1]
    forget_all[z, x, c] = jnp.concatenate(
        [wf_ref[...].astype(F32), jnp.zeros((heads, LANES - w_rows), F32)], axis=1
    )
    normed[tp] = rms_norm(tokens_ref[...].astype(F32), gain_ref[...])
    for copy in local:
        copy.wait()
    pl.semaphore_wait(barrier, len(near))

    def w_place(a, k, dx, core):
        return weights[a].at[wrap(z - k, nz), wrap(x + dx, NX), core]

    def w_z(a, k):
        place = w_place(a, 0, 0, c)
        return remote(
            place, place, wz_send.at[a], wz_recv.at[a, k], wrap(z + k, nz), x, c, tp
        )

    def w_x(a, k, dx):
        place = w_place(a, k, 0, c)
        return remote(
            place, place, wx_send.at[a], wx_recv.at[a * nz + k],
            z, wrap(x + dx, NX), c, tp,
        )

    def w_twin(a, k):
        place = weights[a].at[wrap(z - k, nz), :, c]
        return remote(place, place, wd_send.at[a], wd_recv.at[a], z, x, other, tp)

    def w_group_z(k):
        place = w_q.at[z, :, c]
        return remote(
            place, place, wz_send.at[1], wz_recv.at[1, k], wrap(z + k, nz), x, c, tp
        )

    def w_onward(a, k):
        for dx in (2, 1, 3):
            w_x(a, k, dx).start()

    def nearest(n):
        return jnp.where(lax.rem(n, 2) == 1, lax.div(n + 1, 2), nz - lax.div(n, 2))

    def w_from_z(a, first, last):
        @pl.loop(first, last)
        def _(n):
            k = nearest(n)
            landed(w_place(a, k, 0, c), wz_recv.at[a, k])
            w_onward(a, k)

    def w_from_x(first, last):
        @pl.loop(first, last)
        def _(n):
            k = jnp.where(n == 0, 0, nearest(n))
            landed(w_kv.at[0, pl.ds(0, NX - 1), c], wx_recv.at[k])
            w_twin(0, k).start()

    def w_from_twin(a):
        landed(weights[a].at[:, :, other], wd_recv.at[a])

    def plane_at(way, step):
        return wrap(z - step, nz) if way == 0 else wrap(z + step, nz)

    def steps_of(way, sub):
        return far if (sub < NX // 2) == (way == 0) else far - 1

    def sends(way, step, sub):
        inside = step <= steps_of(way, sub)
        if way == 0:
            return inside & (z >= step - 1) & (z < nz - 1)
        return inside & (wrap(z + step - 1, nz) < steps_of(way, sub))

    def receives(way, step, sub):
        inside = step <= steps_of(way, sub)
        if way == 0:
            return inside & (z >= step)
        return inside & (wrap(z + step, nz) < steps_of(way, sub))

    def reads(way, step):
        return z >= step if way == 0 else z + step >= nz

    def ring_hop(ref, send, recv, way, step, sub):
        place = ref.at[plane_at(way, step - 1), wrap(x + sub, NX), c]
        return remote(
            place, place, send.at[way, step - 1, sub // 2], recv.at[way, step - 1, sub],
            (up, down)[way], x, c, tp,
        )

    def ring_wait(ref, send, recv, way, step, sub):
        landed(
            ref.at[plane_at(way, step), wrap(x + sub, NX), c], recv.at[way, step - 1, sub]
        )

    def twin(ref, send, recv, way, step, sub):
        place = ref.at[plane_at(way, step), wrap(x + sub, NX), c]
        return remote(place, place, send.at[way, step], recv.at[way, step], z, x, other, tp)

    def tok_copy(dy):
        return remote(
            normed.at[tp], normed.at[tp], tok_send.at[0], tok_recv.at[0],
            z, x, c, wrap(tp + dy, n_tp),
        )

    def forget_z(k):
        place = forget_all.at[z, x, c]
        return remote(
            place, place, fz_send.at[0], fz_recv.at[0], wrap(z + k, nz), x, c, tp
        )

    def forget_x(dx):
        place = forget_all.at[:, x, c]
        return remote(
            place, place, fx_send.at[0], fx_recv.at[0], z, wrap(x + dx, NX), c, tp
        )

    def forget_twin(core):
        place = forget_all.at[:, :, core]
        return remote(place, place, fd_send.at[0], fd_recv.at[0], z, x, other, tp)

    def wo_z(k):
        place = wo_all.at[tp, z, x, c]
        return remote(
            place, place, oz_send.at[0], oz_recv.at[0], wrap(z + k, nz), x, c, tp
        )

    def wo_x(dx):
        place = wo_all.at[tp, :, x, c]
        return remote(
            place, place, ox_send.at[0], ox_recv.at[0], z, wrap(x + dx, NX), c, tp
        )

    def wo_y(dy):
        place = wo_all.at[tp, :, :, c]
        return remote(
            place, place, oy_send.at[0], oy_recv.at[0], z, x, c, wrap(tp + dy, n_tp)
        )

    def wo_twin(dy):
        place = wo_all.at[wrap(tp + dy, n_tp), :, :, c]
        return remote(place, place, od_send.at[0], od_recv.at[0], z, x, other, tp)

    both = (0, 1)
    far_first = sorted(range(1, nz), key=lambda k: -min(k, nz - k))
    for k in far_first:
        forget_z(k).start()
    for k in far_first:
        w_z(0, k).start()
    for dx in (2, 1, 3):
        w_x(1, 0, dx).start()
    for dy in range(1, n_tp):
        tok_copy(dy).start()

    w_onward(0, 0)
    w_from_z(0, 1, 3)
    landed(w_q.at[0, pl.ds(0, NX - 1), c], wx_recv.at[nz])
    for k in far_first:
        w_group_z(k).start()
    for k in far_first:
        wo_z(k).start()
    w_twin(1, 0).start()
    w_from_z(0, 3, 5)
    landed(forget_all.at[pl.ds(0, nz - 1), 0, 0], fz_recv.at[0])
    for dx in range(1, NX):
        forget_x(dx).start()
    w_from_z(0, 5, nz)
    w_from_x(0, 5)
    landed(forget_all.at[:, pl.ds(0, NX - 1), 0], fx_recv.at[0])
    forget_twin(c).start()
    w_from_x(5, nz)
    landed(normed.at[pl.ds(0, n_tp - 1)], tok_recv.at[0])
    tokens_here = normed[...].reshape(block, model)
    forget_twin(other).wait_recv()
    forget_rows = jnp.concatenate(
        [
            forget_all[i // plane_blocks, (i // NC) % NX, i % NC][:, :w_rows]
            for i in range(nz * plane_blocks)
        ],
        axis=1,
    )
    forget_rows = jnp.concatenate(
        [forget_rows, jnp.zeros((8 - heads, model), F32)], axis=0
    ).astype(BF16)
    logits = lax.dot_general(
        forget_rows, tokens_here, CONTRACT_LAST, preferred_element_type=F32
    )
    head_row = lax.broadcasted_iota(jnp.int32, (8, block), 0)
    offsets = jnp.zeros((8, block), F32)
    for h in range(heads):
        offsets = jnp.where(head_row == h, offset_ref[h], offsets)
    n_tokens = nz * plane_blocks * block
    logits = logits + offsets + jnp.log(jnp.full((8, block), n_tokens, F32))
    log_gates = jnp.minimum(logits, 0.0) - jnp.log1p(jnp.exp(-jnp.abs(logits)))
    row_at = lax.broadcasted_iota(jnp.int32, (block, block), 0)
    col_at = lax.broadcasted_iota(jnp.int32, (block, block), 1)
    cum_here = jnp.dot(
        log_gates, jnp.where(row_at <= col_at, 1.0, 0.0).astype(F32),
        precision=lax.Precision.HIGHEST, preferred_element_type=F32,
    )
    for h in range(heads):
        gates_send[h] = cum_here[h : h + 1, :]
    gates_all[z, x, c] = gates_send[x]

    def gate_x(dx):
        hx = wrap(x + dx, NX)
        return remote(
            gates_send.at[hx], gates_all.at[z, x, c], gx_send.at[0], gx_recv.at[0],
            z, hx, c, tp,
        )

    for dx in range(1, NX):
        gate_x(dx).start()

    w_from_twin(0)

    def project(ref, i):
        columns = ref[:, :, :, :, i * width : (i + 1) * width].reshape(model, width)
        return jnp.dot(tokens_here, columns, preferred_element_type=F32)

    lane_at = lax.broadcasted_iota(jnp.int32, (half, LANES), 1)
    keys = project(w_kv, 0)
    values_t = project(w_kv, 1).T.astype(BF16)
    for h in range(heads):
        tile = keys[:, (h // 2) * LANES : (h // 2 + 1) * LANES]
        first, second = tile[:half], tile[half:]
        if h % 2 == 0:
            second = pltpu.roll(second, HEAD_DIM, axis=1)
        else:
            first = pltpu.roll(first, HEAD_DIM, axis=1)
        kv_send[h, :half, :] = jnp.where(lane_at < HEAD_DIM, first, second).astype(BF16)
        value_rows = values_t[h * HEAD_DIM : (h + 1) * HEAD_DIM]
        kv_send[h, half : half + HEAD_DIM, :] = value_rows[:, :half]
        kv_send[h, half + HEAD_DIM :, :] = value_rows[:, half:]

    def kv_x(dx):
        hx = wrap(x + dx, NX)
        return remote(
            kv_send.at[hx], kv_all.at[z, x, c], kx_send.at[0], kx_recv.at[dx - 1],
            z, hx, c, tp,
        )

    for dx in range(1, NX):
        kv_x(dx).start()
    kv_all[z, x, c] = kv_send[x]

    def ring_enter(sub):
        for way in both:
            pl.when(sends(way, 1, sub))(
                lambda way=way: ring_hop(kv_all, kz_send, kz_recv, way, 1, sub).start()
            )
        twin(kv_all, kd_send, kd_recv, 0, 0, sub).start()

    ring_enter(0)

    def ring_poll(way, step, sub):
        @pl.when(receives(way, step, sub))
        def _():
            ring_wait(kv_all, kz_send, kz_recv, way, step, sub)

            @pl.when(sends(way, step + 1, sub))
            def _():
                ring_hop(kv_all, kz_send, kz_recv, way, step + 1, sub).start()

            @pl.when(reads(way, step))
            def _():
                twin(kv_all, kd_send, kd_recv, way, step, sub).start()

    def first_sub(step):
        for way in both:
            ring_poll(way, step, 0)

    @pl.loop(1, nz)
    def _(n):
        k = nearest(n)
        landed(w_q.at[0, :, c], wz_recv.at[1, k])
        w_twin(1, k).start()

    w_from_twin(1)
    queries_t = (project(w_q, 0).astype(BF16).astype(F32) * HEAD_DIM ** (-0.5)).T.astype(BF16)
    for h in range(heads):
        q_send[h] = queries_t[h * HEAD_DIM : (h + 1) * HEAD_DIM]

    def q_x(dx):
        hx = wrap(x + dx, NX)
        return remote(
            q_send.at[hx], q_recv.at[x], qx_send.at[0], qx_recv.at[0], z, hx, c, tp
        )

    for dx in range(1, NX):
        q_x(dx).start()
    q_recv[x] = q_send[x]

    landed(gates_all.at[0, pl.ds(0, NX - 1), 0], gx_recv.at[0])

    def gate_z(k):
        cc = c if k % NC == 0 else other
        place = gates_all.at[z, :, c]
        group = min(k - 1, 1)
        return remote(
            place, place, gz_send.at[group], gz_recv.at[group],
            wrap(z + k // NC, nz), x, cc, tp,
        )

    for k in range(1, nz * NC):
        gate_z(k).start()

    first_sub(1)
    for sub in (1, 3, 2):
        dx = NX - sub
        landed(kv_all.at[z, wrap(x + sub, NX), c], kx_recv.at[dx - 1])
        ring_enter(sub)

    landed(q_recv.at[pl.ds(0, NX - 1)], qx_recv.at[0])
    landed(wo_all.at[0, pl.ds(0, nz - 1), 0, 0], oz_recv.at[0])
    for dx in range(1, NX):
        wo_x(dx).start()
    ones_at = lax.broadcasted_iota(jnp.int32, (LANES, block), 0)
    no_rows = jnp.zeros((HEAD_DIM, block), BF16)
    for side in (0, 1):
        picks = ((ones_at // 8) % 2 == side) & (ones_at < 6 * 8)
        picks = jnp.where(picks, 1.0, 0.0).astype(BF16)
        for i in range(NX):
            parts = [q_recv[i], no_rows] if side == 0 else [no_rows, q_recv[i]]
            q_rhs[i, side] = jnp.concatenate(parts + [picks], axis=0)

    landed(gates_all.at[0, :, 0], gz_recv.at[0])
    landed(gates_all.at[pl.ds(0, nz - 1), :, :], gz_recv.at[1])

    n_blocks = nz * plane_blocks
    gate_rows = gates_all[...].reshape(n_blocks, block)
    mine = z * plane_blocks
    row_block = lax.broadcasted_iota(jnp.int32, (n_blocks, n_blocks), 0)
    col_block = lax.broadcasted_iota(jnp.int32, (n_blocks, n_blocks), 1)
    behind = (col_block >= row_block) & (col_block < mine)
    ahead = (col_block < row_block) & (col_block >= mine)
    steps_between = jnp.where(ahead, 1.0, 0.0) - jnp.where(behind, 1.0, 0.0)
    starts = jnp.dot(
        steps_between, gate_rows[:, half:], precision=lax.Precision.HIGHEST,
        preferred_element_type=F32,
    )[:, half - 1 :]
    bias = -(starts + gate_rows)
    bias_high = bias.astype(BF16).astype(F32)
    bias_rest = bias - bias_high
    bias_mid = bias_rest.astype(BF16).astype(F32)
    bias_low = bias_rest - bias_mid
    no_bias = jnp.zeros((LANES - 6 * plane_blocks, LANES), F32)
    for zz in range(nz):
        here = slice(zz * plane_blocks, (zz + 1) * plane_blocks)
        stack = []
        for part in (bias_high, bias_mid, bias_low):
            stack += [part[here, :half], part[here, half:]]
        bias_all[zz] = jnp.concatenate(stack + [no_bias], axis=0).T.astype(BF16)

    lane_block = lax.broadcasted_iota(jnp.int32, (8, LANES), 1) % 8
    ones_rows = jnp.ones((16, CHUNK * half), BF16)

    def attend(plane, own, core=None):
        if core is None:
            blocks = [(b // NC, b % NC) for b in range(plane_blocks)]
            key_rows = kv_all[plane, :, :, :half, :].reshape(plane_blocks * half, LANES)
        else:
            blocks = [(b, core) for b in range(NX)]
            key_rows = kv_all[plane, :, core, :half, :].reshape(NX * half, LANES)
        bias_cols = bias_all[plane]
        masks = [
            jnp.where(lane_block == xx * NC + cc, 1.0, 0.0)[:1].astype(BF16)
            for xx, cc in blocks
        ]
        bias_tiles = jnp.concatenate([bias_cols * mask for mask in masks], axis=0)
        key_side[: len(blocks) * half, :] = jnp.concatenate([key_rows, bias_tiles], axis=1)

        def score(i, side, b0):
            span = slice(b0 * half, (b0 + CHUNK) * half)
            s = jnp.dot(key_side[span, :], q_rhs[i, side], preferred_element_type=F32)
            if own and b0 == i * NC:
                row = lax.broadcasted_iota(jnp.int32, s.shape, 0)
                key_at = (b0 + row // half) * block + side * half + row % half
                query_at = lax.broadcasted_iota(jnp.int32, s.shape, 1) + (
                    (i * NC + c) * block
                )
                s = jnp.where(key_at <= query_at, s, -1e30)
            scores[i, side, span, :] = s
            return jnp.max(s, axis=0, keepdims=True)

        def absorb(i, side, b0, top):
            if own and side == 0 and b0 == 0:
                total = jnp.zeros((HEAD_DIM + 16, block), F32)
            else:
                old = run_max[i]
                top = jnp.maximum(old, top)
                total = run_acc[i] * jnp.exp(old - top)
            run_max[i] = top
            span = slice(b0 * half, (b0 + CHUNK) * half)
            weights = jnp.exp(scores[i, side, span, :] - top).astype(BF16)
            lo = half + side * HEAD_DIM
            value_cols = jnp.concatenate(
                [
                    kv_all[plane, xx, cc, lo : lo + HEAD_DIM, :]
                    for xx, cc in blocks[b0 : b0 + CHUNK]
                ],
                axis=1,
            )
            value_cols = jnp.concatenate([value_cols, ones_rows], axis=0)
            run_acc[i] = total + jnp.dot(value_cols, weights, preferred_element_type=F32)

        chunks = [
            (i, side, b0)
            for side in (0, 1) for b0 in range(0, len(blocks), CHUNK) for i in range(NX)
            if not own or b0 <= i * NC
        ]
        tops = []
        for n in range(len(chunks) + LAG):
            if n < len(chunks):
                tops.append(score(*chunks[n]))
            if n >= LAG:
                absorb(*chunks[n - LAG], tops[n - LAG])

    landed(kv_all.at[z, :, other], kd_recv.at[0, 0])
    attend(z, True)
    first_sub(2)

    def wo_along_y():
        landed(wo_all.at[tp, :, pl.ds(0, NX - 1), c], ox_recv.at[0])
        for dy in range(1, n_tp):
            wo_y(dy).start()
        wo_twin(0).start()

    def kv_step(step, subs):
        for sub in subs:
            for way in both:
                ring_poll(way, step, sub)

    def twin_step(step):
        for way in both:

            @pl.when(reads(way, step) & (step < far))
            def _():
                landed(kv_all.at[plane_at(way, step), :, other], kd_recv.at[way, step])

            @pl.when(reads(way, step) & (step == far))
            def _():
                landed(
                    kv_all.at[plane_at(way, step), pl.ds(0, NX // 2), other],
                    kd_recv.at[way, step],
                )

    def maybe_attend(plane, extra, core=None):
        @pl.when((plane < z) & extra)
        def _():
            attend(plane, False, core)

    @pl.loop(1, far + 1)
    def _(step):
        kv_step(step, (1,))
        pl.when(step == 2)(lambda: first_sub(3))
        pl.when(step == 3)(lambda: first_sub(4))
        maybe_attend(plane_at(1, step - 1), step > 1)
        kv_step(step, (2, 3))
        pl.when(step == 1)(wo_along_y)

        @pl.loop(0, NC)
        def _(part):
            pl.when(part == 1)(lambda: twin_step(step))
            maybe_attend(plane_at(0, step), True, lax.rem(c + part, NC))


    my_head = tp * NX + x
    quarter = rows // 2
    low_lane = lax.broadcasted_iota(jnp.int32, (quarter, LANES), 1) < HEAD_DIM

    def att_copy(rel, dy):
        i, yy = wrap(x + rel, NX), wrap(tp + dy, n_tp)
        return remote(
            att_send.at[i, yy], att_recv.at[my_head], at_send.at[0],
            at_recv.at[0], z, i, c, yy,
        )

    for rel in (2, 1, 3, 0):
        i = wrap(x + rel, NX)
        acc = run_acc[i]
        att = acc[:HEAD_DIM] / acc[HEAD_DIM : HEAD_DIM + 1]
        att = jnp.concatenate([att, att], axis=0).T
        for y in range(n_tp):
            first = att[y * rows : y * rows + quarter]
            second = att[y * rows + quarter : (y + 1) * rows]
            att_send[i, y] = jnp.where(low_lane, first, second).astype(BF16)
        for dy in (2, 1, 3, 0):
            if rel or dy:
                att_copy(rel, dy).start()
    att_recv[my_head] = att_send[x, tp]
    landed(wo_all.at[pl.ds(0, n_tp - 1), :, :, c], oy_recv.at[0])
    for dy in range(1, n_tp):
        wo_twin(dy).start()

    landed(wo_all.at[:, :, :, other], od_recv.at[0])
    landed(att_recv.at[pl.ds(0, NX * n_tp - 1)], at_recv.at[0])

    projected = jnp.zeros((rows, model), F32)
    for y in range(n_tp):
        pieces = []
        for pair in range(NX // 2):
            even = att_recv[y * NX + 2 * pair].astype(F32)
            odd = att_recv[y * NX + 2 * pair + 1].astype(F32)
            first = jnp.where(low_lane, even, pltpu.roll(odd, HEAD_DIM, axis=1))
            second = jnp.where(low_lane, pltpu.roll(even, HEAD_DIM, axis=1), odd)
            pieces.append(jnp.concatenate([first, second], axis=0).astype(BF16))
        columns = jnp.concatenate(pieces, axis=1)
        projected = projected + lax.dot_general(
            columns, wo_all[y].reshape(model, width), CONTRACT_LAST, preferred_element_type=F32
        )
    out_ref[...] = rms_norm(projected, out_gain_ref[...])

    left(w_kv.at[pl.ds(0, nz - 1), 0, 0], wz_send.at[0])
    left(w_kv.at[:, pl.ds(0, NX - 1), 0], wx_send.at[0])
    left(w_q.at[pl.ds(0, nz - 1), :, 0], wz_send.at[1])
    left(w_q.at[0, pl.ds(0, NX - 1), 0], wx_send.at[1])
    for a in (0, 1):
        left(weights[a].at[:, :, c], wd_send.at[a])
    left(normed.at[pl.ds(0, n_tp - 1)], tok_send.at[0])
    left(forget_all.at[pl.ds(0, nz - 1), 0, 0], fz_send.at[0])
    left(forget_all.at[:, pl.ds(0, NX - 1), 0], fx_send.at[0])
    forget_twin(c).wait_send()
    left(wo_all.at[0, pl.ds(0, nz - 1), 0, 0], oz_send.at[0])
    left(wo_all.at[0, :, pl.ds(0, NX - 1), 0], ox_send.at[0])
    left(wo_all.at[pl.ds(0, n_tp - 1), :, :, 0], oy_send.at[0])
    left(wo_all.at[:, :, :, 0], od_send.at[0])
    left(gates_all.at[0, pl.ds(0, NX - 1), 0], gx_send.at[0])
    left(gates_all.at[0, :, 0], gz_send.at[0])
    left(gates_all.at[pl.ds(0, nz - 1), :, :], gz_send.at[1])
    left(kv_send.at[pl.ds(0, NX - 1)], kx_send.at[0])
    left(q_send.at[pl.ds(0, NX - 1)], qx_send.at[0])
    left(kv_all.at[0, :, 0], kd_send.at[0, 0])
    for way in both:
        for step in range(1, far + 1):
            count = NX if step < far else NX // 2

            @pl.when(reads(way, step))
            def _():
                left(kv_all.at[0, pl.ds(0, count), 0], kd_send.at[way, step])

            for duo in (0, 1):
                if step <= steps_of(way, 2 * duo):

                    @pl.when(sends(way, step, 2 * duo))
                    def _():
                        left(kv_all.at[0, pl.ds(0, 2), 0], kz_send.at[way, step - 1, duo])
    left(att_recv.at[pl.ds(0, NX * n_tp - 1)], at_send.at[0])


def solution(mesh):
    n_sp, n_tp = mesh.shape["sp"], mesh.shape["tp"]
    nz = n_sp // (NX * NC)

    def on_device(
        tokens, norm_gain, w_query, w_key, w_value, w_forget, forget_offset, w_out_t, out_gain
    ):
        rows, model = tokens.shape
        w_rows, width = w_query.shape
        heads = w_forget.shape[1]
        block = rows * n_tp
        half = block // 2
        far = nz // 2
        vmem = pl.BlockSpec(memory_space=pltpu.VMEM)
        anywhere = pl.BlockSpec(memory_space=pl.ANY)
        dma = pltpu.SemaphoreType.DMA

        def pair(*shape):
            return [dma(shape), dma(shape)]

        return pl.pallas_call(
            functools.partial(layer_kernel, nz, n_tp),
            out_shape=jax.ShapeDtypeStruct((rows, model), BF16),
            in_specs=[
                vmem, vmem, anywhere, anywhere, anywhere, vmem,
                pl.BlockSpec(memory_space=pltpu.SMEM), anywhere, vmem,
            ],
            out_specs=vmem,
            scratch_shapes=[
                pltpu.VMEM((n_tp, rows, model), BF16),
                pltpu.VMEM((nz, NX, NC, w_rows, 2 * width), BF16),
                pltpu.VMEM((nz, NX, NC, w_rows, width), BF16),
                pltpu.VMEM((n_tp, nz, NX, NC, w_rows, width), BF16),
                pltpu.VMEM((nz, NX, NC, heads, LANES), F32),
                pltpu.VMEM((heads, 1, block), F32),
                pltpu.VMEM((nz, NX, NC, 1, block), F32),
                pltpu.VMEM((nz, LANES, LANES), BF16),
                pltpu.VMEM((heads, block, LANES), BF16),
                pltpu.VMEM((nz, NX, NC, block, LANES), BF16),
                pltpu.VMEM((heads, HEAD_DIM, block), BF16),
                pltpu.VMEM((NX, HEAD_DIM, block), BF16),
                pltpu.VMEM((NX, 2, block, block), BF16),
                pltpu.VMEM((NX * NC * half, 2 * LANES), BF16),
                pltpu.VMEM((NX, 2, NX * NC * half, block), F32),
                pltpu.VMEM((NX, 1, block), F32),
                pltpu.VMEM((NX, HEAD_DIM + 16, block), F32),
                pltpu.VMEM((NX, n_tp, rows // 2, LANES), BF16),
                pltpu.VMEM((NX * n_tp, rows // 2, LANES), BF16),
                dma((4,)),
                *pair(1),
                dma((2,)), dma((2, nz)),
                dma((2,)), dma((nz + 1,)),
                *pair(2),
                *pair(1),
                *pair(1),
                *pair(1),
                *pair(1),
                *pair(1),
                *pair(1),
                *pair(1),
                *pair(1),
                *pair(2),
                dma((1,)), dma((NX - 1,)),
                *pair(1),
                dma((2, far, 2)), dma((2, far, NX)),
                *pair(2, far + 1),
                *pair(1),
            ],
            compiler_params=pltpu.CompilerParams(collective_id=0, has_side_effects=True),
        )(
            tokens, norm_gain.reshape(1, model), w_query, w_key, w_value, w_forget.T,
            forget_offset, w_out_t, out_gain.reshape(1, model),
        )

    return jax.shard_map(
        on_device,
        mesh=mesh,
        in_specs=(
            P(("sp", "tp"), None),
            P(),
            P("sp", "tp"),
            P("sp", "tp"),
            P("sp", "tp"),
            P("sp", "tp"),
            P("tp"),
            P("sp", "tp"),
            P(),
        ),
        out_specs=P(("sp", "tp"), None),
        check_vma=False,
    )
```

```python
import functools

import jax
import jax.numpy as jnp
from jax import lax
from jax.experimental import pallas as pl
from jax.experimental.pallas import tpu as pltpu
from jax.sharding import PartitionSpec as P

HEAD_DIM = 64
LANES = 128
NORM_EPS = 1e-06
NX, NC = 4, 2
CHUNK, LAG = 2, 8
MESH = pl.DeviceIdType.MESH
F32 = jnp.float32
BF16 = jnp.bfloat16
CONTRACT_LAST = (((1,), (1,)), ((), ()))


def rms_norm(floats, gain_row):
    scale_col = lax.rsqrt(jnp.mean(floats * floats, axis=-1, keepdims=True) + NORM_EPS)
    return (floats * scale_col * gain_row).astype(BF16)


def layer_kernel(
    nz, n_tp,
    tokens_ref, gain_ref, wq_ref, wk_ref, wv_ref, wf_ref, offset_ref, wo_ref, out_gain_ref,
    out_ref,
    normed, w_kv, w_q, wo_all, forget_all, gates_send, gates_all, bias_all,
    kv_send, kv_all, q_send, q_recv, q_rhs, key_side, scores, run_max, run_acc, att_send, att_recv,
    local_sem, tok_send, tok_recv, wz_send, wz_recv, wx_send, wx_recv, wd_send, wd_recv,
    fz_send, fz_recv, fx_send, fx_recv, fd_send, fd_recv,
    oz_send, oz_recv, ox_send, ox_recv, oy_send, oy_recv, od_send, od_recv,
    gx_send, gx_recv, gz_send, gz_recv, kx_send, kx_recv, qx_send, qx_recv,
    kz_send, kz_recv, kd_send, kd_recv, at_send, at_recv,
):
    sp, tp = lax.axis_index("sp"), lax.axis_index("tp")
    z = lax.div(sp, NX * NC)
    x = lax.rem(lax.div(sp, NC), NX)
    c = lax.rem(sp, NC)
    rows = tokens_ref.shape[0]
    block = rows * n_tp
    half = block // 2
    model = tokens_ref.shape[1]
    width = wq_ref.shape[1]
    heads = NX
    plane_blocks = NX * NC
    far = nz // 2

    def wrap(value, size):
        return lax.rem(value + size, size)

    def at(zz, xx, cc):
        return (zz * NX + xx) * NC + cc

    def remote(src, dst, send, recv, zz, xx, cc, yy):
        return pltpu.make_async_remote_copy(
            src_ref=src, dst_ref=dst, send_sem=send, recv_sem=recv,
            device_id=(at(zz, xx, cc), yy), device_id_type=MESH,
        )

    def landed(view, sem):
        remote(view, view, sem, sem, z, x, 1 - c, tp).wait_recv()

    def left(view, sem):
        remote(view, view, sem, sem, z, x, 1 - c, tp).wait_send()

    up, down = wrap(z + 1, nz), wrap(z - 1, nz)
    other = 1 - c

    weights = (w_kv, w_q)
    local = [
        pltpu.make_async_copy(
            ref, place.at[z, x, c, :, pl.ds(i * width, width)], local_sem.at[n]
        )
        for n, (ref, place, i) in enumerate(
            ((wk_ref, w_kv, 0), (wv_ref, w_kv, 1), (wq_ref, w_q, 0))
        )
    ]
    local.append(pltpu.make_async_copy(wo_ref, wo_all.at[tp, z, x, c], local_sem.at[3]))
    for copy in local:
        copy.start()

    barrier = pltpu.get_barrier_semaphore()
    near = [(at(z, wrap(x + dx, NX), c), tp) for dx in range(1, NX)]
    near += [(sp, wrap(tp + dy, n_tp)) for dy in range(1, n_tp)]
    near += [(at(wrap(z + dz, nz), x, c), tp) for dz in range(1, nz)]
    near += [(at(z, x, other), tp)]
    for device in near:
        pl.semaphore_signal(barrier, inc=1, device_id_type=MESH, device_id=device)

    w_rows = wf_ref.shape[1]
    forget_all[z, x, c] = jnp.concatenate(
        [wf_ref[...].astype(F32), jnp.zeros((heads, LANES - w_rows), F32)], axis=1
    )
    normed[tp] = rms_norm(tokens_ref[...].astype(F32), gain_ref[...])
    for copy in local:
        copy.wait()
    pl.semaphore_wait(barrier, len(near))

    def w_place(a, k, dx, core):
        return weights[a].at[wrap(z - k, nz), wrap(x + dx, NX), core]

    def w_z(a, k):
        place = w_place(a, 0, 0, c)
        return remote(
            place, place, wz_send.at[a], wz_recv.at[a, k], wrap(z + k, nz), x, c, tp
        )

    def w_x(a, k, dx):
        place = w_place(a, k, 0, c)
        return remote(
            place, place, wx_send.at[a], wx_recv.at[a * nz + k],
            z, wrap(x + dx, NX), c, tp,
        )

    def w_twin(a, k):
        place = weights[a].at[wrap(z - k, nz), :, c]
        return remote(place, place, wd_send.at[a], wd_recv.at[a], z, x, other, tp)

    def w_group_z(k):
        place = w_q.at[z, :, c]
        return remote(
            place, place, wz_send.at[1], wz_recv.at[1, k], wrap(z + k, nz), x, c, tp
        )

    def w_onward(a, k):
        for dx in (2, 1, 3):
            w_x(a, k, dx).start()

    def nearest(n):
        return jnp.where(lax.rem(n, 2) == 1, lax.div(n + 1, 2), nz - lax.div(n, 2))

    def w_from_z(a, first, last):
        @pl.loop(first, last)
        def _(n):
            k = nearest(n)
            landed(w_place(a, k, 0, c), wz_recv.at[a, k])
            w_onward(a, k)

    def w_from_x(first, last):
        @pl.loop(first, last)
        def _(n):
            k = jnp.where(n == 0, 0, nearest(n))
            landed(w_kv.at[0, pl.ds(0, NX - 1), c], wx_recv.at[k])
            w_twin(0, k).start()

    def w_from_twin(a):
        landed(weights[a].at[:, :, other], wd_recv.at[a])

    def plane_at(way, step):
        return wrap(z - step, nz) if way == 0 else wrap(z + step, nz)

    def steps_of(way, sub):
        return far if (sub < NX // 2) == (way == 0) else far - 1

    def sends(way, step, sub):
        inside = step <= steps_of(way, sub)
        if way == 0:
            return inside & (z >= step - 1) & (z < nz - 1)
        return inside & (wrap(z + step - 1, nz) < steps_of(way, sub))

    def receives(way, step, sub):
        inside = step <= steps_of(way, sub)
        if way == 0:
            return inside & (z >= step)
        return inside & (wrap(z + step, nz) < steps_of(way, sub))

    def reads(way, step):
        return z >= step if way == 0 else z + step >= nz

    def ring_hop(ref, send, recv, way, step, sub):
        place = ref.at[plane_at(way, step - 1), wrap(x + sub, NX), c]
        return remote(
            place, place, send.at[way, step - 1, sub // 2], recv.at[way, step - 1, sub],
            (up, down)[way], x, c, tp,
        )

    def ring_wait(ref, send, recv, way, step, sub):
        landed(
            ref.at[plane_at(way, step), wrap(x + sub, NX), c], recv.at[way, step - 1, sub]
        )

    def twin(ref, send, recv, way, step, sub):
        place = ref.at[plane_at(way, step), wrap(x + sub, NX), c]
        return remote(place, place, send.at[way, step], recv.at[way, step], z, x, other, tp)

    def tok_copy(dy):
        return remote(
            normed.at[tp], normed.at[tp], tok_send.at[0], tok_recv.at[0],
            z, x, c, wrap(tp + dy, n_tp),
        )

    def forget_z(k):
        place = forget_all.at[z, x, c]
        return remote(
            place, place, fz_send.at[0], fz_recv.at[0], wrap(z + k, nz), x, c, tp
        )

    def forget_x(dx):
        place = forget_all.at[:, x, c]
        return remote(
            place, place, fx_send.at[0], fx_recv.at[0], z, wrap(x + dx, NX), c, tp
        )

    def forget_twin(core):
        place = forget_all.at[:, :, core]
        return remote(place, place, fd_send.at[0], fd_recv.at[0], z, x, other, tp)

    def wo_z(k):
        place = wo_all.at[tp, z, x, c]
        return remote(
            place, place, oz_send.at[0], oz_recv.at[0], wrap(z + k, nz), x, c, tp
        )

    def wo_x(dx):
        place = wo_all.at[tp, :, x, c]
        return remote(
            place, place, ox_send.at[0], ox_recv.at[0], z, wrap(x + dx, NX), c, tp
        )

    def wo_y(dy):
        place = wo_all.at[tp, :, :, c]
        return remote(
            place, place, oy_send.at[0], oy_recv.at[0], z, x, c, wrap(tp + dy, n_tp)
        )

    def wo_twin(dy):
        place = wo_all.at[wrap(tp + dy, n_tp), :, :, c]
        return remote(place, place, od_send.at[0], od_recv.at[0], z, x, other, tp)

    both = (0, 1)
    far_first = sorted(range(1, nz), key=lambda k: -min(k, nz - k))
    for k in far_first:
        forget_z(k).start()
    for k in far_first:
        w_z(0, k).start()
    for dx in (2, 1, 3):
        w_x(1, 0, dx).start()
    for dy in range(1, n_tp):
        tok_copy(dy).start()

    w_onward(0, 0)
    w_from_z(0, 1, 3)
    landed(w_q.at[0, pl.ds(0, NX - 1), c], wx_recv.at[nz])
    for k in far_first:
        w_group_z(k).start()
    for k in far_first:
        wo_z(k).start()
    w_twin(1, 0).start()
    w_from_z(0, 3, 5)
    landed(forget_all.at[pl.ds(0, nz - 1), 0, 0], fz_recv.at[0])
    for dx in range(1, NX):
        forget_x(dx).start()
    w_from_z(0, 5, nz)
    w_from_x(0, 5)
    landed(forget_all.at[:, pl.ds(0, NX - 1), 0], fx_recv.at[0])
    forget_twin(c).start()
    w_from_x(5, nz)
    landed(normed.at[pl.ds(0, n_tp - 1)], tok_recv.at[0])
    tokens_here = normed[...].reshape(block, model)
    forget_twin(other).wait_recv()
    forget_rows = jnp.concatenate(
        [
            forget_all[i // plane_blocks, (i // NC) % NX, i % NC][:, :w_rows]
            for i in range(nz * plane_blocks)
        ],
        axis=1,
    )
    forget_rows = jnp.concatenate(
        [forget_rows, jnp.zeros((8 - heads, model), F32)], axis=0
    ).astype(BF16)
    logits = lax.dot_general(
        forget_rows, tokens_here, CONTRACT_LAST, preferred_element_type=F32
    )
    head_row = lax.broadcasted_iota(jnp.int32, (8, block), 0)
    offsets = jnp.zeros((8, block), F32)
    for h in range(heads):
        offsets = jnp.where(head_row == h, offset_ref[h], offsets)
    n_tokens = nz * plane_blocks * block
    logits = logits + offsets + jnp.log(jnp.full((8, block), n_tokens, F32))
    log_gates = jnp.minimum(logits, 0.0) - jnp.log1p(jnp.exp(-jnp.abs(logits)))
    row_at = lax.broadcasted_iota(jnp.int32, (block, block), 0)
    col_at = lax.broadcasted_iota(jnp.int32, (block, block), 1)
    cum_here = jnp.dot(
        log_gates, jnp.where(row_at <= col_at, 1.0, 0.0).astype(F32),
        precision=lax.Precision.HIGHEST, preferred_element_type=F32,
    )
    for h in range(heads):
        gates_send[h] = cum_here[h : h + 1, :]
    gates_all[z, x, c] = gates_send[x]

    def gate_x(dx):
        hx = wrap(x + dx, NX)
        return remote(
            gates_send.at[hx], gates_all.at[z, x, c], gx_send.at[0], gx_recv.at[0],
            z, hx, c, tp,
        )

    for dx in range(1, NX):
        gate_x(dx).start()

    w_from_twin(0)

    def project(ref, i):
        columns = ref[:, :, :, :, i * width : (i + 1) * width].reshape(model, width)
        return jnp.dot(tokens_here, columns, preferred_element_type=F32)

    lane_at = lax.broadcasted_iota(jnp.int32, (half, LANES), 1)
    keys = project(w_kv, 0)
    values_t = project(w_kv, 1).T.astype(BF16)
    for h in range(heads):
        tile = keys[:, (h // 2) * LANES : (h // 2 + 1) * LANES]
        first, second = tile[:half], tile[half:]
        if h % 2 == 0:
            second = pltpu.roll(second, HEAD_DIM, axis=1)
        else:
            first = pltpu.roll(first, HEAD_DIM, axis=1)
        kv_send[h, :half, :] = jnp.where(lane_at < HEAD_DIM, first, second).astype(BF16)
        value_rows = values_t[h * HEAD_DIM : (h + 1) * HEAD_DIM]
        kv_send[h, half : half + HEAD_DIM, :] = value_rows[:, :half]
        kv_send[h, half + HEAD_DIM :, :] = value_rows[:, half:]

    def kv_x(dx):
        hx = wrap(x + dx, NX)
        return remote(
            kv_send.at[hx], kv_all.at[z, x, c], kx_send.at[0], kx_recv.at[dx - 1],
            z, hx, c, tp,
        )

    for dx in range(1, NX):
        kv_x(dx).start()
    kv_all[z, x, c] = kv_send[x]

    def ring_enter(sub):
        for way in both:
            pl.when(sends(way, 1, sub))(
                lambda way=way: ring_hop(kv_all, kz_send, kz_recv, way, 1, sub).start()
            )
        twin(kv_all, kd_send, kd_recv, 0, 0, sub).start()

    ring_enter(0)

    def ring_poll(way, step, sub):
        @pl.when(receives(way, step, sub))
        def _():
            ring_wait(kv_all, kz_send, kz_recv, way, step, sub)

            @pl.when(sends(way, step + 1, sub))
            def _():
                ring_hop(kv_all, kz_send, kz_recv, way, step + 1, sub).start()

            @pl.when(reads(way, step))
            def _():
                twin(kv_all, kd_send, kd_recv, way, step, sub).start()

    def first_sub(step):
        for way in both:
            ring_poll(way, step, 0)

    @pl.loop(1, nz)
    def _(n):
        k = nearest(n)
        landed(w_q.at[0, :, c], wz_recv.at[1, k])
        w_twin(1, k).start()

    w_from_twin(1)
    queries_t = (project(w_q, 0).astype(BF16).astype(F32) * HEAD_DIM ** (-0.5)).T.astype(BF16)
    for h in range(heads):
        q_send[h] = queries_t[h * HEAD_DIM : (h + 1) * HEAD_DIM]

    def q_x(dx):
        hx = wrap(x + dx, NX)
        return remote(
            q_send.at[hx], q_recv.at[x], qx_send.at[0], qx_recv.at[0], z, hx, c, tp
        )

    for dx in range(1, NX):
        q_x(dx).start()
    q_recv[x] = q_send[x]

    landed(gates_all.at[0, pl.ds(0, NX - 1), 0], gx_recv.at[0])

    def gate_z(k):
        cc = c if k % NC == 0 else other
        place = gates_all.at[z, :, c]
        group = min(k - 1, 1)
        return remote(
            place, place, gz_send.at[group], gz_recv.at[group],
            wrap(z + k // NC, nz), x, cc, tp,
        )

    for k in range(1, nz * NC):
        gate_z(k).start()

    first_sub(1)
    for sub in (1, 3, 2):
        dx = NX - sub
        landed(kv_all.at[z, wrap(x + sub, NX), c], kx_recv.at[dx - 1])
        ring_enter(sub)

    landed(q_recv.at[pl.ds(0, NX - 1)], qx_recv.at[0])
    landed(wo_all.at[0, pl.ds(0, nz - 1), 0, 0], oz_recv.at[0])
    for dx in range(1, NX):
        wo_x(dx).start()
    ones_at = lax.broadcasted_iota(jnp.int32, (LANES, block), 0)
    no_rows = jnp.zeros((HEAD_DIM, block), BF16)
    for side in (0, 1):
        picks = ((ones_at // 8) % 2 == side) & (ones_at < 6 * 8)
        picks = jnp.where(picks, 1.0, 0.0).astype(BF16)
        for i in range(NX):
            parts = [q_recv[i], no_rows] if side == 0 else [no_rows, q_recv[i]]
            q_rhs[i, side] = jnp.concatenate(parts + [picks], axis=0)

    landed(gates_all.at[0, :, 0], gz_recv.at[0])
    landed(gates_all.at[pl.ds(0, nz - 1), :, :], gz_recv.at[1])

    n_blocks = nz * plane_blocks
    gate_rows = gates_all[...].reshape(n_blocks, block)
    mine = z * plane_blocks
    row_block = lax.broadcasted_iota(jnp.int32, (n_blocks, n_blocks), 0)
    col_block = lax.broadcasted_iota(jnp.int32, (n_blocks, n_blocks), 1)
    behind = (col_block >= row_block) & (col_block < mine)
    ahead = (col_block < row_block) & (col_block >= mine)
    steps_between = jnp.where(ahead, 1.0, 0.0) - jnp.where(behind, 1.0, 0.0)
    starts = jnp.dot(
        steps_between, gate_rows[:, half:], precision=lax.Precision.HIGHEST,
        preferred_element_type=F32,
    )[:, half - 1 :]
    bias = -(starts + gate_rows)
    bias_high = bias.astype(BF16).astype(F32)
    bias_rest = bias - bias_high
    bias_mid = bias_rest.astype(BF16).astype(F32)
    bias_low = bias_rest - bias_mid
    no_bias = jnp.zeros((LANES - 6 * plane_blocks, LANES), F32)
    for zz in range(nz):
        here = slice(zz * plane_blocks, (zz + 1) * plane_blocks)
        stack = []
        for part in (bias_high, bias_mid, bias_low):
            stack += [part[here, :half], part[here, half:]]
        bias_all[zz] = jnp.concatenate(stack + [no_bias], axis=0).T.astype(BF16)

    lane_block = lax.broadcasted_iota(jnp.int32, (8, LANES), 1) % 8
    ones_rows = jnp.ones((16, CHUNK * half), BF16)

    def attend(plane, own, core=None):
        if core is None:
            blocks = [(b // NC, b % NC) for b in range(plane_blocks)]
            key_rows = kv_all[plane, :, :, :half, :].reshape(plane_blocks * half, LANES)
        else:
            blocks = [(b, core) for b in range(NX)]
            key_rows = kv_all[plane, :, core, :half, :].reshape(NX * half, LANES)
        bias_cols = bias_all[plane]
        masks = [
            jnp.where(lane_block == xx * NC + cc, 1.0, 0.0)[:1].astype(BF16)
            for xx, cc in blocks
        ]
        bias_tiles = jnp.concatenate([bias_cols * mask for mask in masks], axis=0)
        key_side[: len(blocks) * half, :] = jnp.concatenate([key_rows, bias_tiles], axis=1)

        def score(i, side, b0):
            span = slice(b0 * half, (b0 + CHUNK) * half)
            s = jnp.dot(key_side[span, :], q_rhs[i, side], preferred_element_type=F32)
            if own and b0 == i * NC:
                row = lax.broadcasted_iota(jnp.int32, s.shape, 0)
                key_at = (b0 + row // half) * block + side * half + row % half
                query_at = lax.broadcasted_iota(jnp.int32, s.shape, 1) + (
                    (i * NC + c) * block
                )
                s = jnp.where(key_at <= query_at, s, -1e30)
            scores[i, side, span, :] = s
            return jnp.max(s, axis=0, keepdims=True)

        def absorb(i, side, b0, top):
            if own and side == 0 and b0 == 0:
                total = jnp.zeros((HEAD_DIM + 16, block), F32)
            else:
                old = run_max[i]
                top = jnp.maximum(old, top)
                total = run_acc[i] * jnp.exp(old - top)
            run_max[i] = top
            span = slice(b0 * half, (b0 + CHUNK) * half)
            weights = jnp.exp(scores[i, side, span, :] - top).astype(BF16)
            lo = half + side * HEAD_DIM
            value_cols = jnp.concatenate(
                [
                    kv_all[plane, xx, cc, lo : lo + HEAD_DIM, :]
                    for xx, cc in blocks[b0 : b0 + CHUNK]
                ],
                axis=1,
            )
            value_cols = jnp.concatenate([value_cols, ones_rows], axis=0)
            run_acc[i] = total + jnp.dot(value_cols, weights, preferred_element_type=F32)

        chunks = [
            (i, side, b0)
            for side in (0, 1) for b0 in range(0, len(blocks), CHUNK) for i in range(NX)
            if not own or b0 <= i * NC
        ]
        tops = []
        for n in range(len(chunks) + LAG):
            if n < len(chunks):
                tops.append(score(*chunks[n]))
            if n >= LAG:
                absorb(*chunks[n - LAG], tops[n - LAG])

    landed(kv_all.at[z, :, other], kd_recv.at[0, 0])
    attend(z, True)
    first_sub(2)

    def wo_along_y():
        landed(wo_all.at[tp, :, pl.ds(0, NX - 1), c], ox_recv.at[0])
        for dy in range(1, n_tp):
            wo_y(dy).start()
        wo_twin(0).start()

    def kv_step(step, subs):
        for sub in subs:
            for way in both:
                ring_poll(way, step, sub)

    def twin_step(step):
        for way in both:

            @pl.when(reads(way, step) & (step < far))
            def _():
                landed(kv_all.at[plane_at(way, step), :, other], kd_recv.at[way, step])

            @pl.when(reads(way, step) & (step == far))
            def _():
                landed(
                    kv_all.at[plane_at(way, step), pl.ds(0, NX // 2), other],
                    kd_recv.at[way, step],
                )

    def maybe_attend(plane, extra, core=None):
        @pl.when((plane < z) & extra)
        def _():
            attend(plane, False, core)

    @pl.loop(1, far + 1)
    def _(step):
        kv_step(step, (1, 2))
        pl.when(step == 2)(lambda: first_sub(3))
        pl.when(step == 3)(lambda: first_sub(4))
        maybe_attend(plane_at(1, step - 1), step > 1)
        kv_step(step, (3,))
        pl.when(step == 1)(wo_along_y)

        @pl.loop(0, NC)
        def _(part):
            pl.when(part == 1)(lambda: twin_step(step))
            maybe_attend(plane_at(0, step), True, lax.rem(c + part, NC))


    my_head = tp * NX + x
    quarter = rows // 2
    low_lane = lax.broadcasted_iota(jnp.int32, (quarter, LANES), 1) < HEAD_DIM

    def att_copy(rel, dy):
        i, yy = wrap(x + rel, NX), wrap(tp + dy, n_tp)
        return remote(
            att_send.at[i, yy], att_recv.at[my_head], at_send.at[0],
            at_recv.at[0], z, i, c, yy,
        )

    for rel in (2, 1, 3, 0):
        i = wrap(x + rel, NX)
        acc = run_acc[i]
        att = acc[:HEAD_DIM] / acc[HEAD_DIM : HEAD_DIM + 1]
        att = jnp.concatenate([att, att], axis=0).T
        for y in range(n_tp):
            first = att[y * rows : y * rows + quarter]
            second = att[y * rows + quarter : (y + 1) * rows]
            att_send[i, y] = jnp.where(low_lane, first, second).astype(BF16)
        for dy in (2, 1, 3, 0):
            if rel or dy:
                att_copy(rel, dy).start()
    att_recv[my_head] = att_send[x, tp]
    landed(wo_all.at[pl.ds(0, n_tp - 1), :, :, c], oy_recv.at[0])
    for dy in range(1, n_tp):
        wo_twin(dy).start()

    landed(wo_all.at[:, :, :, other], od_recv.at[0])
    landed(att_recv.at[pl.ds(0, NX * n_tp - 1)], at_recv.at[0])

    projected = jnp.zeros((rows, model), F32)
    for y in range(n_tp):
        pieces = []
        for pair in range(NX // 2):
            even = att_recv[y * NX + 2 * pair].astype(F32)
            odd = att_recv[y * NX + 2 * pair + 1].astype(F32)
            first = jnp.where(low_lane, even, pltpu.roll(odd, HEAD_DIM, axis=1))
            second = jnp.where(low_lane, pltpu.roll(even, HEAD_DIM, axis=1), odd)
            pieces.append(jnp.concatenate([first, second], axis=0).astype(BF16))
        columns = jnp.concatenate(pieces, axis=1)
        projected = projected + lax.dot_general(
            columns, wo_all[y].reshape(model, width), CONTRACT_LAST, preferred_element_type=F32
        )
    out_ref[...] = rms_norm(projected, out_gain_ref[...])

    left(w_kv.at[pl.ds(0, nz - 1), 0, 0], wz_send.at[0])
    left(w_kv.at[:, pl.ds(0, NX - 1), 0], wx_send.at[0])
    left(w_q.at[pl.ds(0, nz - 1), :, 0], wz_send.at[1])
    left(w_q.at[0, pl.ds(0, NX - 1), 0], wx_send.at[1])
    for a in (0, 1):
        left(weights[a].at[:, :, c], wd_send.at[a])
    left(normed.at[pl.ds(0, n_tp - 1)], tok_send.at[0])
    left(forget_all.at[pl.ds(0, nz - 1), 0, 0], fz_send.at[0])
    left(forget_all.at[:, pl.ds(0, NX - 1), 0], fx_send.at[0])
    forget_twin(c).wait_send()
    left(wo_all.at[0, pl.ds(0, nz - 1), 0, 0], oz_send.at[0])
    left(wo_all.at[0, :, pl.ds(0, NX - 1), 0], ox_send.at[0])
    left(wo_all.at[pl.ds(0, n_tp - 1), :, :, 0], oy_send.at[0])
    left(wo_all.at[:, :, :, 0], od_send.at[0])
    left(gates_all.at[0, pl.ds(0, NX - 1), 0], gx_send.at[0])
    left(gates_all.at[0, :, 0], gz_send.at[0])
    left(gates_all.at[pl.ds(0, nz - 1), :, :], gz_send.at[1])
    left(kv_send.at[pl.ds(0, NX - 1)], kx_send.at[0])
    left(q_send.at[pl.ds(0, NX - 1)], qx_send.at[0])
    left(kv_all.at[0, :, 0], kd_send.at[0, 0])
    for way in both:
        for step in range(1, far + 1):
            count = NX if step < far else NX // 2

            @pl.when(reads(way, step))
            def _():
                left(kv_all.at[0, pl.ds(0, count), 0], kd_send.at[way, step])

            for duo in (0, 1):
                if step <= steps_of(way, 2 * duo):

                    @pl.when(sends(way, step, 2 * duo))
                    def _():
                        left(kv_all.at[0, pl.ds(0, 2), 0], kz_send.at[way, step - 1, duo])
    left(att_recv.at[pl.ds(0, NX * n_tp - 1)], at_send.at[0])


def solution(mesh):
    n_sp, n_tp = mesh.shape["sp"], mesh.shape["tp"]
    nz = n_sp // (NX * NC)

    def on_device(
        tokens, norm_gain, w_query, w_key, w_value, w_forget, forget_offset, w_out_t, out_gain
    ):
        rows, model = tokens.shape
        w_rows, width = w_query.shape
        heads = w_forget.shape[1]
        block = rows * n_tp
        half = block // 2
        far = nz // 2
        vmem = pl.BlockSpec(memory_space=pltpu.VMEM)
        anywhere = pl.BlockSpec(memory_space=pl.ANY)
        dma = pltpu.SemaphoreType.DMA

        def pair(*shape):
            return [dma(shape), dma(shape)]

        return pl.pallas_call(
            functools.partial(layer_kernel, nz, n_tp),
            out_shape=jax.ShapeDtypeStruct((rows, model), BF16),
            in_specs=[
                vmem, vmem, anywhere, anywhere, anywhere, vmem,
                pl.BlockSpec(memory_space=pltpu.SMEM), anywhere, vmem,
            ],
            out_specs=vmem,
            scratch_shapes=[
                pltpu.VMEM((n_tp, rows, model), BF16),
                pltpu.VMEM((nz, NX, NC, w_rows, 2 * width), BF16),
                pltpu.VMEM((nz, NX, NC, w_rows, width), BF16),
                pltpu.VMEM((n_tp, nz, NX, NC, w_rows, width), BF16),
                pltpu.VMEM((nz, NX, NC, heads, LANES), F32),
                pltpu.VMEM((heads, 1, block), F32),
                pltpu.VMEM((nz, NX, NC, 1, block), F32),
                pltpu.VMEM((nz, LANES, LANES), BF16),
                pltpu.VMEM((heads, block, LANES), BF16),
                pltpu.VMEM((nz, NX, NC, block, LANES), BF16),
                pltpu.VMEM((heads, HEAD_DIM, block), BF16),
                pltpu.VMEM((NX, HEAD_DIM, block), BF16),
                pltpu.VMEM((NX, 2, block, block), BF16),
                pltpu.VMEM((NX * NC * half, 2 * LANES), BF16),
                pltpu.VMEM((NX, 2, NX * NC * half, block), F32),
                pltpu.VMEM((NX, 1, block), F32),
                pltpu.VMEM((NX, HEAD_DIM + 16, block), F32),
                pltpu.VMEM((NX, n_tp, rows // 2, LANES), BF16),
                pltpu.VMEM((NX * n_tp, rows // 2, LANES), BF16),
                dma((4,)),
                *pair(1),
                dma((2,)), dma((2, nz)),
                dma((2,)), dma((nz + 1,)),
                *pair(2),
                *pair(1),
                *pair(1),
                *pair(1),
                *pair(1),
                *pair(1),
                *pair(1),
                *pair(1),
                *pair(1),
                *pair(2),
                dma((1,)), dma((NX - 1,)),
                *pair(1),
                dma((2, far, 2)), dma((2, far, NX)),
                *pair(2, far + 1),
                *pair(1),
            ],
            compiler_params=pltpu.CompilerParams(collective_id=0, has_side_effects=True),
        )(
            tokens, norm_gain.reshape(1, model), w_query, w_key, w_value, w_forget.T,
            forget_offset, w_out_t, out_gain.reshape(1, model),
        )

    return jax.shard_map(
        on_device,
        mesh=mesh,
        in_specs=(
            P(("sp", "tp"), None),
            P(),
            P("sp", "tp"),
            P("sp", "tp"),
            P("sp", "tp"),
            P("sp", "tp"),
            P("tp"),
            P("sp", "tp"),
            P(),
        ),
        out_specs=P(("sp", "tp"), None),
        check_vma=False,
    )
```

```python
import functools

import jax
import jax.numpy as jnp
from jax import lax
from jax.experimental import pallas as pl
from jax.experimental.pallas import tpu as pltpu
from jax.sharding import PartitionSpec as P

HEAD_DIM = 64
LANES = 128
NORM_EPS = 1e-06
NX, NC = 4, 2
CHUNK, LAG = 2, 8
MESH = pl.DeviceIdType.MESH
F32 = jnp.float32
BF16 = jnp.bfloat16
CONTRACT_LAST = (((1,), (1,)), ((), ()))


def rms_norm(floats, gain_row):
    scale_col = lax.rsqrt(jnp.mean(floats * floats, axis=-1, keepdims=True) + NORM_EPS)
    return (floats * scale_col * gain_row).astype(BF16)


def layer_kernel(
    nz, n_tp,
    tokens_ref, gain_ref, wq_ref, wk_ref, wv_ref, wf_ref, offset_ref, wo_ref, out_gain_ref,
    out_ref,
    normed, w_kv, w_q, wo_all, forget_all, gates_send, gates_all, bias_all,
    kv_send, kv_all, q_send, q_recv, q_rhs, key_side, scores, run_max, run_acc, att_send, att_recv,
    local_sem, tok_send, tok_recv, wz_send, wz_recv, wx_send, wx_recv, wd_send, wd_recv,
    fz_send, fz_recv, fx_send, fx_recv, fd_send, fd_recv,
    oz_send, oz_recv, ox_send, ox_recv, oy_send, oy_recv, od_send, od_recv,
    gx_send, gx_recv, gz_send, gz_recv, kx_send, kx_recv, qx_send, qx_recv,
    kz_send, kz_recv, kd_send, kd_recv, at_send, at_recv,
):
    sp, tp = lax.axis_index("sp"), lax.axis_index("tp")
    z = lax.div(sp, NX * NC)
    x = lax.rem(lax.div(sp, NC), NX)
    c = lax.rem(sp, NC)
    rows = tokens_ref.shape[0]
    block = rows * n_tp
    half = block // 2
    model = tokens_ref.shape[1]
    width = wq_ref.shape[1]
    heads = NX
    plane_blocks = NX * NC
    far = nz // 2

    def wrap(value, size):
        return lax.rem(value + size, size)

    def at(zz, xx, cc):
        return (zz * NX + xx) * NC + cc

    def remote(src, dst, send, recv, zz, xx, cc, yy):
        return pltpu.make_async_remote_copy(
            src_ref=src, dst_ref=dst, send_sem=send, recv_sem=recv,
            device_id=(at(zz, xx, cc), yy), device_id_type=MESH,
        )

    def landed(view, sem):
        remote(view, view, sem, sem, z, x, 1 - c, tp).wait_recv()

    def left(view, sem):
        remote(view, view, sem, sem, z, x, 1 - c, tp).wait_send()

    up, down = wrap(z + 1, nz), wrap(z - 1, nz)
    other = 1 - c

    weights = (w_kv, w_q)
    local = [
        pltpu.make_async_copy(
            ref, place.at[z, x, c, :, pl.ds(i * width, width)], local_sem.at[n]
        )
        for n, (ref, place, i) in enumerate(
            ((wk_ref, w_kv, 0), (wv_ref, w_kv, 1), (wq_ref, w_q, 0))
        )
    ]
    local.append(pltpu.make_async_copy(wo_ref, wo_all.at[tp, z, x, c], local_sem.at[3]))
    for copy in local:
        copy.start()

    barrier = pltpu.get_barrier_semaphore()
    near = [(at(z, wrap(x + dx, NX), c), tp) for dx in range(1, NX)]
    near += [(sp, wrap(tp + dy, n_tp)) for dy in range(1, n_tp)]
    near += [(at(wrap(z + dz, nz), x, c), tp) for dz in range(1, nz)]
    near += [(at(z, x, other), tp)]
    for device in near:
        pl.semaphore_signal(barrier, inc=1, device_id_type=MESH, device_id=device)

    w_rows = wf_ref.shape[1]
    forget_all[z, x, c] = jnp.concatenate(
        [wf_ref[...].astype(F32), jnp.zeros((heads, LANES - w_rows), F32)], axis=1
    )
    normed[tp] = rms_norm(tokens_ref[...].astype(F32), gain_ref[...])
    for copy in local:
        copy.wait()
    pl.semaphore_wait(barrier, len(near))

    def w_place(a, k, dx, core):
        return weights[a].at[wrap(z - k, nz), wrap(x + dx, NX), core]

    def w_z(a, k):
        place = w_place(a, 0, 0, c)
        return remote(
            place, place, wz_send.at[a], wz_recv.at[a, k], wrap(z + k, nz), x, c, tp
        )

    def w_x(a, k, dx):
        place = w_place(a, k, 0, c)
        return remote(
            place, place, wx_send.at[a], wx_recv.at[a * nz + k],
            z, wrap(x + dx, NX), c, tp,
        )

    def w_twin(a, k):
        place = weights[a].at[wrap(z - k, nz), :, c]
        return remote(place, place, wd_send.at[a], wd_recv.at[a], z, x, other, tp)

    def w_group_z(k):
        place = w_q.at[z, :, c]
        return remote(
            place, place, wz_send.at[1], wz_recv.at[1, k], wrap(z + k, nz), x, c, tp
        )

    def w_onward(a, k):
        for dx in (2, 1, 3):
            w_x(a, k, dx).start()

    def nearest(n):
        return jnp.where(lax.rem(n, 2) == 1, lax.div(n + 1, 2), nz - lax.div(n, 2))

    def w_from_z(a, first, last):
        @pl.loop(first, last)
        def _(n):
            k = nearest(n)
            landed(w_place(a, k, 0, c), wz_recv.at[a, k])
            w_onward(a, k)

    def w_from_x(first, last):
        @pl.loop(first, last)
        def _(n):
            k = jnp.where(n == 0, 0, nearest(n))
            landed(w_kv.at[0, pl.ds(0, NX - 1), c], wx_recv.at[k])
            w_twin(0, k).start()

    def w_from_twin(a):
        landed(weights[a].at[:, :, other], wd_recv.at[a])

    def plane_at(way, step):
        return wrap(z - step, nz) if way == 0 else wrap(z + step, nz)

    def steps_of(way, sub):
        return far if (sub < NX // 2) == (way == 0) else far - 1

    def sends(way, step, sub):
        inside = step <= steps_of(way, sub)
        if way == 0:
            return inside & (z >= step - 1) & (z < nz - 1)
        return inside & (wrap(z + step - 1, nz) < steps_of(way, sub))

    def receives(way, step, sub):
        inside = step <= steps_of(way, sub)
        if way == 0:
            return inside & (z >= step)
        return inside & (wrap(z + step, nz) < steps_of(way, sub))

    def reads(way, step):
        return z >= step if way == 0 else z + step >= nz

    def ring_hop(ref, send, recv, way, step, sub):
        place = ref.at[plane_at(way, step - 1), wrap(x + sub, NX), c]
        return remote(
            place, place, send.at[way, step - 1, sub // 2], recv.at[way, step - 1, sub],
            (up, down)[way], x, c, tp,
        )

    def ring_wait(ref, send, recv, way, step, sub):
        landed(
            ref.at[plane_at(way, step), wrap(x + sub, NX), c], recv.at[way, step - 1, sub]
        )

    def twin(ref, send, recv, way, step, sub):
        place = ref.at[plane_at(way, step), wrap(x + sub, NX), c]
        return remote(place, place, send.at[way, step], recv.at[way, step], z, x, other, tp)

    def tok_copy(dy):
        return remote(
            normed.at[tp], normed.at[tp], tok_send.at[0], tok_recv.at[0],
            z, x, c, wrap(tp + dy, n_tp),
        )

    def forget_z(k):
        place = forget_all.at[z, x, c]
        return remote(
            place, place, fz_send.at[0], fz_recv.at[0], wrap(z + k, nz), x, c, tp
        )

    def forget_x(dx):
        place = forget_all.at[:, x, c]
        return remote(
            place, place, fx_send.at[0], fx_recv.at[0], z, wrap(x + dx, NX), c, tp
        )

    def forget_twin(core):
        place = forget_all.at[:, :, core]
        return remote(place, place, fd_send.at[0], fd_recv.at[0], z, x, other, tp)

    def wo_z(k):
        place = wo_all.at[tp, z, x, c]
        return remote(
            place, place, oz_send.at[0], oz_recv.at[0], wrap(z + k, nz), x, c, tp
        )

    def wo_x(dx):
        place = wo_all.at[tp, :, x, c]
        return remote(
            place, place, ox_send.at[0], ox_recv.at[0], z, wrap(x + dx, NX), c, tp
        )

    def wo_y(dy):
        place = wo_all.at[tp, :, :, c]
        return remote(
            place, place, oy_send.at[0], oy_recv.at[0], z, x, c, wrap(tp + dy, n_tp)
        )

    def wo_twin(dy):
        place = wo_all.at[wrap(tp + dy, n_tp), :, :, c]
        return remote(place, place, od_send.at[0], od_recv.at[0], z, x, other, tp)

    both = (0, 1)
    far_first = sorted(range(1, nz), key=lambda k: -min(k, nz - k))
    for k in far_first:
        forget_z(k).start()
    for k in far_first:
        w_z(0, k).start()
    for dx in (2, 1, 3):
        w_x(1, 0, dx).start()
    for dy in range(1, n_tp):
        tok_copy(dy).start()

    w_onward(0, 0)
    w_from_z(0, 1, 3)
    landed(w_q.at[0, pl.ds(0, NX - 1), c], wx_recv.at[nz])
    for k in far_first:
        w_group_z(k).start()
    for k in far_first:
        wo_z(k).start()
    w_twin(1, 0).start()
    w_from_z(0, 3, 5)
    landed(forget_all.at[pl.ds(0, nz - 1), 0, 0], fz_recv.at[0])
    for dx in range(1, NX):
        forget_x(dx).start()
    w_from_z(0, 5, nz)
    w_from_x(0, 5)
    landed(forget_all.at[:, pl.ds(0, NX - 1), 0], fx_recv.at[0])
    forget_twin(c).start()
    w_from_x(5, nz)
    landed(normed.at[pl.ds(0, n_tp - 1)], tok_recv.at[0])
    tokens_here = normed[...].reshape(block, model)
    forget_twin(other).wait_recv()
    forget_rows = jnp.concatenate(
        [
            forget_all[i // plane_blocks, (i // NC) % NX, i % NC][:, :w_rows]
            for i in range(nz * plane_blocks)
        ],
        axis=1,
    )
    forget_rows = jnp.concatenate(
        [forget_rows, jnp.zeros((8 - heads, model), F32)], axis=0
    ).astype(BF16)
    logits = lax.dot_general(
        forget_rows, tokens_here, CONTRACT_LAST, preferred_element_type=F32
    )
    head_row = lax.broadcasted_iota(jnp.int32, (8, block), 0)
    offsets = jnp.zeros((8, block), F32)
    for h in range(heads):
        offsets = jnp.where(head_row == h, offset_ref[h], offsets)
    n_tokens = nz * plane_blocks * block
    logits = logits + offsets + jnp.log(jnp.full((8, block), n_tokens, F32))
    log_gates = jnp.minimum(logits, 0.0) - jnp.log1p(jnp.exp(-jnp.abs(logits)))
    row_at = lax.broadcasted_iota(jnp.int32, (block, block), 0)
    col_at = lax.broadcasted_iota(jnp.int32, (block, block), 1)
    cum_here = jnp.dot(
        log_gates, jnp.where(row_at <= col_at, 1.0, 0.0).astype(F32),
        precision=lax.Precision.HIGHEST, preferred_element_type=F32,
    )
    for h in range(heads):
        gates_send[h] = cum_here[h : h + 1, :]
    gates_all[z, x, c] = gates_send[x]

    def gate_x(dx):
        hx = wrap(x + dx, NX)
        return remote(
            gates_send.at[hx], gates_all.at[z, x, c], gx_send.at[0], gx_recv.at[0],
            z, hx, c, tp,
        )

    for dx in range(1, NX):
        gate_x(dx).start()

    w_from_twin(0)

    def project(ref, i):
        columns = ref[:, :, :, :, i * width : (i + 1) * width].reshape(model, width)
        return jnp.dot(tokens_here, columns, preferred_element_type=F32)

    lane_at = lax.broadcasted_iota(jnp.int32, (half, LANES), 1)
    keys = project(w_kv, 0)
    values_t = project(w_kv, 1).T.astype(BF16)
    for h in range(heads):
        tile = keys[:, (h // 2) * LANES : (h // 2 + 1) * LANES]
        first, second = tile[:half], tile[half:]
        if h % 2 == 0:
            second = pltpu.roll(second, HEAD_DIM, axis=1)
        else:
            first = pltpu.roll(first, HEAD_DIM, axis=1)
        kv_send[h, :half, :] = jnp.where(lane_at < HEAD_DIM, first, second).astype(BF16)
        value_rows = values_t[h * HEAD_DIM : (h + 1) * HEAD_DIM]
        kv_send[h, half : half + HEAD_DIM, :] = value_rows[:, :half]
        kv_send[h, half + HEAD_DIM :, :] = value_rows[:, half:]

    def kv_x(dx):
        hx = wrap(x + dx, NX)
        return remote(
            kv_send.at[hx], kv_all.at[z, x, c], kx_send.at[0], kx_recv.at[dx - 1],
            z, hx, c, tp,
        )

    for dx in range(1, NX):
        kv_x(dx).start()
    kv_all[z, x, c] = kv_send[x]

    def ring_enter(sub):
        for way in both:
            pl.when(sends(way, 1, sub))(
                lambda way=way: ring_hop(kv_all, kz_send, kz_recv, way, 1, sub).start()
            )
        twin(kv_all, kd_send, kd_recv, 0, 0, sub).start()

    ring_enter(0)

    def ring_poll(way, step, sub):
        @pl.when(receives(way, step, sub))
        def _():
            ring_wait(kv_all, kz_send, kz_recv, way, step, sub)

            @pl.when(sends(way, step + 1, sub))
            def _():
                ring_hop(kv_all, kz_send, kz_recv, way, step + 1, sub).start()

            @pl.when(reads(way, step))
            def _():
                twin(kv_all, kd_send, kd_recv, way, step, sub).start()

    def first_sub(step):
        for way in both:
            ring_poll(way, step, 0)

    @pl.loop(1, nz)
    def _(n):
        k = nearest(n)
        landed(w_q.at[0, :, c], wz_recv.at[1, k])
        w_twin(1, k).start()

    w_from_twin(1)
    queries_t = (project(w_q, 0).astype(BF16).astype(F32) * HEAD_DIM ** (-0.5)).T.astype(BF16)
    for h in range(heads):
        q_send[h] = queries_t[h * HEAD_DIM : (h + 1) * HEAD_DIM]

    def q_x(dx):
        hx = wrap(x + dx, NX)
        return remote(
            q_send.at[hx], q_recv.at[x], qx_send.at[0], qx_recv.at[0], z, hx, c, tp
        )

    for dx in range(1, NX):
        q_x(dx).start()
    q_recv[x] = q_send[x]

    landed(gates_all.at[0, pl.ds(0, NX - 1), 0], gx_recv.at[0])

    def gate_z(k):
        cc = c if k % NC == 0 else other
        place = gates_all.at[z, :, c]
        group = min(k - 1, 1)
        return remote(
            place, place, gz_send.at[group], gz_recv.at[group],
            wrap(z + k // NC, nz), x, cc, tp,
        )

    for k in range(1, nz * NC):
        gate_z(k).start()

    first_sub(1)
    for sub in (1, 3, 2):
        dx = NX - sub
        landed(kv_all.at[z, wrap(x + sub, NX), c], kx_recv.at[dx - 1])
        ring_enter(sub)

    landed(q_recv.at[pl.ds(0, NX - 1)], qx_recv.at[0])
    landed(wo_all.at[0, pl.ds(0, nz - 1), 0, 0], oz_recv.at[0])
    for dx in range(1, NX):
        wo_x(dx).start()
    ones_at = lax.broadcasted_iota(jnp.int32, (LANES, block), 0)
    no_rows = jnp.zeros((HEAD_DIM, block), BF16)
    for side in (0, 1):
        picks = ((ones_at // 8) % 2 == side) & (ones_at < 6 * 8)
        picks = jnp.where(picks, 1.0, 0.0).astype(BF16)
        for i in range(NX):
            parts = [q_recv[i], no_rows] if side == 0 else [no_rows, q_recv[i]]
            q_rhs[i, side] = jnp.concatenate(parts + [picks], axis=0)

    landed(gates_all.at[0, :, 0], gz_recv.at[0])
    landed(gates_all.at[pl.ds(0, nz - 1), :, :], gz_recv.at[1])

    n_blocks = nz * plane_blocks
    gate_rows = gates_all[...].reshape(n_blocks, block)
    mine = z * plane_blocks
    row_block = lax.broadcasted_iota(jnp.int32, (n_blocks, n_blocks), 0)
    col_block = lax.broadcasted_iota(jnp.int32, (n_blocks, n_blocks), 1)
    behind = (col_block >= row_block) & (col_block < mine)
    ahead = (col_block < row_block) & (col_block >= mine)
    steps_between = jnp.where(ahead, 1.0, 0.0) - jnp.where(behind, 1.0, 0.0)
    starts = jnp.dot(
        steps_between, gate_rows[:, half:], precision=lax.Precision.HIGHEST,
        preferred_element_type=F32,
    )[:, half - 1 :]
    bias = -(starts + gate_rows)
    bias_high = bias.astype(BF16).astype(F32)
    bias_rest = bias - bias_high
    bias_mid = bias_rest.astype(BF16).astype(F32)
    bias_low = bias_rest - bias_mid
    no_bias = jnp.zeros((LANES - 6 * plane_blocks, LANES), F32)
    for zz in range(nz):
        here = slice(zz * plane_blocks, (zz + 1) * plane_blocks)
        stack = []
        for part in (bias_high, bias_mid, bias_low):
            stack += [part[here, :half], part[here, half:]]
        bias_all[zz] = jnp.concatenate(stack + [no_bias], axis=0).T.astype(BF16)

    lane_block = lax.broadcasted_iota(jnp.int32, (8, LANES), 1) % 8
    ones_rows = jnp.ones((16, CHUNK * half), BF16)

    def attend(plane, own, core=None):
        if core is None:
            blocks = [(b // NC, b % NC) for b in range(plane_blocks)]
            key_rows = kv_all[plane, :, :, :half, :].reshape(plane_blocks * half, LANES)
        else:
            blocks = [(b, core) for b in range(NX)]
            key_rows = kv_all[plane, :, core, :half, :].reshape(NX * half, LANES)
        bias_cols = bias_all[plane]
        masks = [
            jnp.where(lane_block == xx * NC + cc, 1.0, 0.0)[:1].astype(BF16)
            for xx, cc in blocks
        ]
        bias_tiles = jnp.concatenate([bias_cols * mask for mask in masks], axis=0)
        key_side[: len(blocks) * half, :] = jnp.concatenate([key_rows, bias_tiles], axis=1)

        def score(i, side, b0):
            span = slice(b0 * half, (b0 + CHUNK) * half)
            s = jnp.dot(key_side[span, :], q_rhs[i, side], preferred_element_type=F32)
            if own and b0 == i * NC:
                row = lax.broadcasted_iota(jnp.int32, s.shape, 0)
                key_at = (b0 + row // half) * block + side * half + row % half
                query_at = lax.broadcasted_iota(jnp.int32, s.shape, 1) + (
                    (i * NC + c) * block
                )
                s = jnp.where(key_at <= query_at, s, -1e30)
            scores[i, side, span, :] = s
            return jnp.max(s, axis=0, keepdims=True)

        def absorb(i, side, b0, top):
            if own and side == 0 and b0 == 0:
                total = jnp.zeros((HEAD_DIM + 16, block), F32)
            else:
                old = run_max[i]
                top = jnp.maximum(old, top)
                total = run_acc[i] * jnp.exp(old - top)
            run_max[i] = top
            span = slice(b0 * half, (b0 + CHUNK) * half)
            weights = jnp.exp(scores[i, side, span, :] - top).astype(BF16)
            lo = half + side * HEAD_DIM
            value_cols = jnp.concatenate(
                [
                    kv_all[plane, xx, cc, lo : lo + HEAD_DIM, :]
                    for xx, cc in blocks[b0 : b0 + CHUNK]
                ],
                axis=1,
            )
            value_cols = jnp.concatenate([value_cols, ones_rows], axis=0)
            run_acc[i] = total + jnp.dot(value_cols, weights, preferred_element_type=F32)

        chunks = [
            (i, side, b0)
            for side in (0, 1) for b0 in range(0, len(blocks), CHUNK) for i in range(NX)
            if not own or b0 <= i * NC
        ]
        tops = []
        for n in range(len(chunks) + LAG):
            if n < len(chunks):
                tops.append(score(*chunks[n]))
            if n >= LAG:
                absorb(*chunks[n - LAG], tops[n - LAG])

    landed(kv_all.at[z, :, other], kd_recv.at[0, 0])
    attend(z, True)
    first_sub(2)

    def wo_along_y():
        landed(wo_all.at[tp, :, pl.ds(0, NX - 1), c], ox_recv.at[0])
        for dy in range(1, n_tp):
            wo_y(dy).start()
        wo_twin(0).start()

    def kv_step(step, subs):
        for sub in subs:
            for way in both:
                ring_poll(way, step, sub)

    def twin_step(step):
        for way in both:

            @pl.when(reads(way, step) & (step < far))
            def _():
                landed(kv_all.at[plane_at(way, step), :, other], kd_recv.at[way, step])

            @pl.when(reads(way, step) & (step == far))
            def _():
                landed(
                    kv_all.at[plane_at(way, step), pl.ds(0, NX // 2), other],
                    kd_recv.at[way, step],
                )

    def maybe_attend(plane, extra, core=None):
        @pl.when((plane < z) & extra)
        def _():
            attend(plane, False, core)

    @pl.loop(1, far + 1)
    def _(step):
        kv_step(step, (1,))
        pl.when(step == 2)(lambda: first_sub(3))
        pl.when(step == 3)(lambda: first_sub(4))
        maybe_attend(plane_at(1, step - 1), step > 1)
        kv_step(step, (3, 2))
        pl.when(step == 1)(wo_along_y)

        @pl.loop(0, NC)
        def _(part):
            pl.when(part == 1)(lambda: twin_step(step))
            maybe_attend(plane_at(0, step), True, lax.rem(c + part, NC))


    my_head = tp * NX + x
    quarter = rows // 2
    low_lane = lax.broadcasted_iota(jnp.int32, (quarter, LANES), 1) < HEAD_DIM

    def att_copy(rel, dy):
        i, yy = wrap(x + rel, NX), wrap(tp + dy, n_tp)
        return remote(
            att_send.at[i, yy], att_recv.at[my_head], at_send.at[0],
            at_recv.at[0], z, i, c, yy,
        )

    for rel in (2, 1, 3, 0):
        i = wrap(x + rel, NX)
        acc = run_acc[i]
        att = acc[:HEAD_DIM] / acc[HEAD_DIM : HEAD_DIM + 1]
        att = jnp.concatenate([att, att], axis=0).T
        for y in range(n_tp):
            first = att[y * rows : y * rows + quarter]
            second = att[y * rows + quarter : (y + 1) * rows]
            att_send[i, y] = jnp.where(low_lane, first, second).astype(BF16)
        for dy in (2, 1, 3, 0):
            if rel or dy:
                att_copy(rel, dy).start()
    att_recv[my_head] = att_send[x, tp]
    landed(wo_all.at[pl.ds(0, n_tp - 1), :, :, c], oy_recv.at[0])
    for dy in range(1, n_tp):
        wo_twin(dy).start()

    landed(wo_all.at[:, :, :, other], od_recv.at[0])
    landed(att_recv.at[pl.ds(0, NX * n_tp - 1)], at_recv.at[0])

    projected = jnp.zeros((rows, model), F32)
    for y in range(n_tp):
        pieces = []
        for pair in range(NX // 2):
            even = att_recv[y * NX + 2 * pair].astype(F32)
            odd = att_recv[y * NX + 2 * pair + 1].astype(F32)
            first = jnp.where(low_lane, even, pltpu.roll(odd, HEAD_DIM, axis=1))
            second = jnp.where(low_lane, pltpu.roll(even, HEAD_DIM, axis=1), odd)
            pieces.append(jnp.concatenate([first, second], axis=0).astype(BF16))
        columns = jnp.concatenate(pieces, axis=1)
        projected = projected + lax.dot_general(
            columns, wo_all[y].reshape(model, width), CONTRACT_LAST, preferred_element_type=F32
        )
    out_ref[...] = rms_norm(projected, out_gain_ref[...])

    left(w_kv.at[pl.ds(0, nz - 1), 0, 0], wz_send.at[0])
    left(w_kv.at[:, pl.ds(0, NX - 1), 0], wx_send.at[0])
    left(w_q.at[pl.ds(0, nz - 1), :, 0], wz_send.at[1])
    left(w_q.at[0, pl.ds(0, NX - 1), 0], wx_send.at[1])
    for a in (0, 1):
        left(weights[a].at[:, :, c], wd_send.at[a])
    left(normed.at[pl.ds(0, n_tp - 1)], tok_send.at[0])
    left(forget_all.at[pl.ds(0, nz - 1), 0, 0], fz_send.at[0])
    left(forget_all.at[:, pl.ds(0, NX - 1), 0], fx_send.at[0])
    forget_twin(c).wait_send()
    left(wo_all.at[0, pl.ds(0, nz - 1), 0, 0], oz_send.at[0])
    left(wo_all.at[0, :, pl.ds(0, NX - 1), 0], ox_send.at[0])
    left(wo_all.at[pl.ds(0, n_tp - 1), :, :, 0], oy_send.at[0])
    left(wo_all.at[:, :, :, 0], od_send.at[0])
    left(gates_all.at[0, pl.ds(0, NX - 1), 0], gx_send.at[0])
    left(gates_all.at[0, :, 0], gz_send.at[0])
    left(gates_all.at[pl.ds(0, nz - 1), :, :], gz_send.at[1])
    left(kv_send.at[pl.ds(0, NX - 1)], kx_send.at[0])
    left(q_send.at[pl.ds(0, NX - 1)], qx_send.at[0])
    left(kv_all.at[0, :, 0], kd_send.at[0, 0])
    for way in both:
        for step in range(1, far + 1):
            count = NX if step < far else NX // 2

            @pl.when(reads(way, step))
            def _():
                left(kv_all.at[0, pl.ds(0, count), 0], kd_send.at[way, step])

            for duo in (0, 1):
                if step <= steps_of(way, 2 * duo):

                    @pl.when(sends(way, step, 2 * duo))
                    def _():
                        left(kv_all.at[0, pl.ds(0, 2), 0], kz_send.at[way, step - 1, duo])
    left(att_recv.at[pl.ds(0, NX * n_tp - 1)], at_send.at[0])


def solution(mesh):
    n_sp, n_tp = mesh.shape["sp"], mesh.shape["tp"]
    nz = n_sp // (NX * NC)

    def on_device(
        tokens, norm_gain, w_query, w_key, w_value, w_forget, forget_offset, w_out_t, out_gain
    ):
        rows, model = tokens.shape
        w_rows, width = w_query.shape
        heads = w_forget.shape[1]
        block = rows * n_tp
        half = block // 2
        far = nz // 2
        vmem = pl.BlockSpec(memory_space=pltpu.VMEM)
        anywhere = pl.BlockSpec(memory_space=pl.ANY)
        dma = pltpu.SemaphoreType.DMA

        def pair(*shape):
            return [dma(shape), dma(shape)]

        return pl.pallas_call(
            functools.partial(layer_kernel, nz, n_tp),
            out_shape=jax.ShapeDtypeStruct((rows, model), BF16),
            in_specs=[
                vmem, vmem, anywhere, anywhere, anywhere, vmem,
                pl.BlockSpec(memory_space=pltpu.SMEM), anywhere, vmem,
            ],
            out_specs=vmem,
            scratch_shapes=[
                pltpu.VMEM((n_tp, rows, model), BF16),
                pltpu.VMEM((nz, NX, NC, w_rows, 2 * width), BF16),
                pltpu.VMEM((nz, NX, NC, w_rows, width), BF16),
                pltpu.VMEM((n_tp, nz, NX, NC, w_rows, width), BF16),
                pltpu.VMEM((nz, NX, NC, heads, LANES), F32),
                pltpu.VMEM((heads, 1, block), F32),
                pltpu.VMEM((nz, NX, NC, 1, block), F32),
                pltpu.VMEM((nz, LANES, LANES), BF16),
                pltpu.VMEM((heads, block, LANES), BF16),
                pltpu.VMEM((nz, NX, NC, block, LANES), BF16),
                pltpu.VMEM((heads, HEAD_DIM, block), BF16),
                pltpu.VMEM((NX, HEAD_DIM, block), BF16),
                pltpu.VMEM((NX, 2, block, block), BF16),
                pltpu.VMEM((NX * NC * half, 2 * LANES), BF16),
                pltpu.VMEM((NX, 2, NX * NC * half, block), F32),
                pltpu.VMEM((NX, 1, block), F32),
                pltpu.VMEM((NX, HEAD_DIM + 16, block), F32),
                pltpu.VMEM((NX, n_tp, rows // 2, LANES), BF16),
                pltpu.VMEM((NX * n_tp, rows // 2, LANES), BF16),
                dma((4,)),
                *pair(1),
                dma((2,)), dma((2, nz)),
                dma((2,)), dma((nz + 1,)),
                *pair(2),
                *pair(1),
                *pair(1),
                *pair(1),
                *pair(1),
                *pair(1),
                *pair(1),
                *pair(1),
                *pair(1),
                *pair(2),
                dma((1,)), dma((NX - 1,)),
                *pair(1),
                dma((2, far, 2)), dma((2, far, NX)),
                *pair(2, far + 1),
                *pair(1),
            ],
            compiler_params=pltpu.CompilerParams(collective_id=0, has_side_effects=True),
        )(
            tokens, norm_gain.reshape(1, model), w_query, w_key, w_value, w_forget.T,
            forget_offset, w_out_t, out_gain.reshape(1, model),
        )

    return jax.shard_map(
        on_device,
        mesh=mesh,
        in_specs=(
            P(("sp", "tp"), None),
            P(),
            P("sp", "tp"),
            P("sp", "tp"),
            P("sp", "tp"),
            P("sp", "tp"),
            P("tp"),
            P("sp", "tp"),
            P(),
        ),
        out_specs=P(("sp", "tp"), None),
        check_vma=False,
    )
```
